32 devices in a mesh: sp: 8 (over z, x), tp: 4 (over y, core).
Axes of the slice: x: 2, y: 2, z: 4, core: 2. Of those that a mesh axis runs over, the one named last changes fastest.
Arguments:
- probe_vectors: bfloat16 [1024, 2048], P('sp', 'tp'), may hold values from -6 to 6
- address_vectors: bfloat16 [1024, 2048], P('sp', 'tp'), may hold values from -6 to 6
- content_vectors: bfloat16 [1024, 2048], P('sp', 'tp'), may hold values from -6 to 6
- storage_raw_signal: float32 [16, 1024], P('tp', 'sp'), may hold values from -8 to 4
- fade_raw_signal: float32 [16, 1024], P('tp', 'sp'), may hold values from -6 to 6
- channel_fade_exponent: float32 [16], P('tp'), may hold values from -9 to 0
- extra_fade_amount: float32 [16, 1024], P('tp', 'sp'), may hold values from -1 to 0
- sequence_label: int32 [1024], P('sp'), may hold values from 0 to 2, never falling along the last dimension, each value on 1 to 768 neighbouring positions
- exit_valve_raw_signal: bfloat16 [1024, 2048], P('sp', 'tp'), may hold values from -6 to 6
- final_projection_matrix: bfloat16 [2048, 2048], P('tp'), may hold values from -0.125 to 0.125
- incoming_rows_matrix: bfloat16 [1024, 2048], P('sp', 'tp'), may hold values from -48 to 48
- initial_rescale_factor: float32 [2048], P('tp'), may hold values from 0 to 3
- specialist_picks: int32 [1024, 2], P('sp'), may hold values from 0 to 7, all different within a row; in each aligned block of 128 rows (0 to 127, 128 to 255, ...) at most 36 rows name the same one
- picked_specialist_share: bfloat16 [1024, 2], P('sp'), may hold values from 0.29882812 to 1.1953125
- specialist_valve_matrix: bfloat16 [8, 2048, 4096], P('sp', None, 'tp'), may hold values from -0.125 to 0.125
- specialist_raising_matrix: bfloat16 [8, 2048, 4096], P('sp', None, 'tp'), may hold values from -0.125 to 0.125
- specialist_lowering_matrix: bfloat16 [8, 4096, 2048], P('sp', 'tp'), may hold values from -0.09375 to 0.09375
- common_valve_matrix: bfloat16 [2048, 512], P(None, 'tp'), may hold values from -0.125 to 0.125
- common_raising_matrix: bfloat16 [2048, 512], P(None, 'tp'), may hold values from -0.125 to 0.125
- common_lowering_matrix: bfloat16 [512, 2048], P('tp'), may hold values from -0.25 to 0.25
- latter_rescale_factor: float32 [2048], P('tp'), may hold values from 0.1 to 1.9
Outputs:
- result: bfloat16 [1024, 2048], P('sp', 'tp')
The draws below stay inside these ranges and needn't reach their ends.
Inputs may be any that keep to these rules, and one draw needn't show every extreme that they name: `sequence_label`: document numbers never fall; a document has 1 to 768 positions, one exactly 768. `specialist_picks`: each row names 2 different experts; among the rows of one index of sp no expert is named more than 36 times, a bound that some block reaches.
All inputs are finite; a program needn't handle non-finite values.
Results may differ from the reference program's by a relative error of at most 0.018.
Values may be sent and summed in bfloat16 or wider, within the bound.
No kernel may reach another device: no remote copies, remote signals or barrier semaphores. Data moves between devices by JAX's collectives and lax.ppermute only.
A program may use at most 64 MiB of HBM per device.

```python
import math
import jax
import jax.numpy as jnp
import numpy as np
from jax import lax

D = 2048
H = 16
DK = 128
DV = 128
BLOCK = 64
FF = 4096
SF = 512
TOP = 2
TOK_DEV = 128
TOKENS = 1024
EXPERTS = 8
CAP = 36
DOC_SPAN = 768
DOCS = 3
N_SP = 8
N_TP = 4


def slow_heads(key):
    share = 0.5
    return jax.random.bernoulli(jax.random.fold_in(key, 11), share, (H,))


def draw_channel_fade_exponent(key, part):
    slower = slow_heads(key)
    jitter = jax.random.uniform(jax.random.fold_in(key, 12), (H,), jnp.float32, -0.3, 0.3)
    slow_rate = math.log(0.6 / DOC_SPAN)
    fast_rate = math.log(2.0 / BLOCK)
    return jnp.where(slower, slow_rate, fast_rate) + jitter


def draw_storage_raw_signal(key, part):
    slower = slow_heads(key)
    base_level = jnp.where(slower, math.log(0.3 * DK / DOC_SPAN), 0.0)
    noise = jnp.clip(jax.random.normal(jax.random.fold_in(key, 13), (H, TOKENS), jnp.float32), -4.0, 4.0)
    return base_level[:, None] + noise


def draw_fade_raw_signal(key, part):
    offsets = jax.random.uniform(jax.random.fold_in(key, 14), (TOKENS // TOK_DEV,), jnp.float32, -1.2, 1.2)
    spread_out = jnp.repeat(offsets, TOK_DEV)
    noise = jnp.clip(jax.random.normal(jax.random.fold_in(key, 15), (H, TOKENS), jnp.float32), -4.0, 4.0)
    return noise + spread_out[None, :]


def draw_extra_fade_amount(key, part):
    places = jax.random.randint(jax.random.fold_in(key, 16), (H, 12), 0, TOKENS)
    depths = jax.random.uniform(jax.random.fold_in(key, 17), (H, 12), jnp.float32, math.log(0.5), math.log(0.6))
    positions = jnp.arange(TOKENS, dtype=jnp.int32)
    hits = (positions[None, None, :] == places[:, :, None]).astype(jnp.float32)
    return jnp.min(hits * depths[:, :, None], 1)


def draw_incoming_rows_matrix(key, part):
    ramp = jnp.exp(jnp.linspace(math.log(0.5), math.log(1.5), D)) * jax.random.uniform(jax.random.fold_in(key, 18), (D,), jnp.float32, 0.7, 1.3)
    row_scale = jnp.exp(jax.random.uniform(jax.random.fold_in(key, 19), (TOKENS, 1), jnp.float32, 0.0, math.log(4.0)))
    base_draw = jnp.clip(jax.random.normal(jax.random.fold_in(key, 21), (TOKENS, D), jnp.float32), -5.0, 5.0)
    return (base_draw * ramp[None, :] * row_scale).astype(jnp.bfloat16)


def draw_initial_rescale_factor(key, part):
    ramp = jnp.exp(jnp.linspace(math.log(0.6), math.log(1.8), D))
    noise = jax.random.uniform(jax.random.fold_in(key, 22), (D,), jnp.float32, 0.8, 1.2)
    return ramp * noise


def block_levels(rng, extent, pieces, smallest, top_value):
    level = 1.0
    for dim, shards_of in pieces:
        draws = jax.random.uniform(jax.random.fold_in(jax.random.fold_in(rng, 6), dim), (shards_of,), jnp.float32, smallest / len(pieces), top_value / len(pieces))
        level = level * jnp.repeat(jnp.exp(draws), extent[dim] // shards_of).reshape((-1,) + (1,) * (len(extent) - 1 - dim))
    return level


def length_profile(number_of, total, limit, skew):
    portions = [(1 << 20) // math.isqrt(grade ** skew) + 1 for grade in range(2, number_of + 1)]
    spare, counts = total - limit - (number_of - 1), [1] * (number_of - 1)
    while spare > 0:
        candidates = [i for i in range(number_of - 1) if counts[i] < limit]
        whole, left = sum([portions[i] for i in candidates]), spare
        for i in candidates:
            extra = min(limit - counts[i], max(1, left * portions[i] // whole), spare)
            counts[i] = counts[i] + extra
            spare = spare - extra
    return np.array([limit] + counts)


def uneven(own_key, amount, total, most, skew):
    if amount == 2:
        one = jax.random.randint(own_key, (), max(1, total - most), min(most, total - 1) + 1)
        return jnp.stack([one, total - one])
    lengths = jnp.asarray(length_profile(amount, total, most, skew), jnp.int32)
    pairs = (amount - 1) // 2
    donor, sink = lengths[1:1 + 2 * pairs:2], lengths[2:2 + 2 * pairs:2]
    room = jnp.minimum(donor - 1, most - sink)
    shifted = jax.random.randint(jax.random.fold_in(own_key, 1), (pairs,), 0, 1 << 20) % (room + 1)
    lengths = lengths.at[1:1 + 2 * pairs:2].set(donor - shifted).at[2:2 + 2 * pairs:2].set(sink + shifted)
    return lengths[jax.random.permutation(jax.random.fold_in(own_key, 2), amount)]


def assign_block(own_key, own, number, rows, count, top, reach, skew):
    sequence = jax.random.permutation(own_key, count)
    packed, usual = load_shares(count, rows * top, reach, skew, True), load_shares(count, rows * top, reach, skew, False)
    places = jnp.arange(count)

    def named(tallies, turn):
        used = int((tallies > 0).sum())
        fixed = max(1, used // 4)
        shifted = fixed + (places - fixed + turn * (used - fixed)) % max(1, count - fixed)
        return jnp.zeros((count,), jnp.int32).at[sequence[jnp.where(places < fixed, places, shifted)]].set(jnp.asarray(tallies, jnp.int32))

    tallies = jnp.where(number % 4 == 0, named(packed, number // 4), named(usual, number - number // 4 - 1))
    mixed = jax.random.permutation(jax.random.fold_in(own, 3), count)
    donor, sink = mixed[0:count // 2 * 2:2], mixed[1:count // 2 * 2:2]
    slack = jnp.minimum(tallies[donor] - 1, reach - tallies[sink]) // 2
    slack = jnp.where((donor == sequence[0]) | (sink == sequence[0]) | (tallies[sink] == 0), 0, jnp.maximum(slack, 0))
    shifted = jax.random.randint(jax.random.fold_in(own, 4), (count // 2,), 0, 1 << 20) % (slack + 1)
    tallies = tallies.at[donor].add(-shifted).at[sink].add(shifted)
    members = jnp.searchsorted(jnp.cumsum(tallies), jnp.arange(rows * top), side="right").astype(jnp.int32)
    table = members.reshape(top, rows).T
    table = table[jax.random.permutation(jax.random.fold_in(own, 1), rows)]
    turn = jax.random.randint(jax.random.fold_in(own, 2), (rows, 1), 0, top)
    return jnp.take_along_axis(table, (jnp.arange(top)[None, :] + turn) % top, axis=1)


def load_shares(count, total, limit, lean, full):
    weights = [(1 << 20) // math.isqrt(grade ** lean) + 1 for grade in range(1, count + 1)]
    largest = limit if full else min(limit, max(-(-total // count), total * weights[0] // sum(weights)))
    least = 1 if total - largest >= count - 1 else 0
    holding, rest = [largest] + [least] * (count - 1), total - largest - least * (count - 1)
    while rest > 0:
        free = [i for i in range(1, count) if holding[i] < largest] or [i for i in range(1, count) if holding[i] < limit]
        pool, remaining = sum([weights[i] for i in free]), rest
        for i in free:
            addition = min(limit - holding[i], max(1, remaining * weights[i] // pool), rest)
            holding[i] = holding[i] + addition
            rest = rest - addition
    return np.array(holding)


def scatter_about(key, shape, width, most, shards=(), kind=jnp.bfloat16):
    drawn = width * jax.random.normal(key, shape, jnp.float32)
    if shards:
        drawn = drawn * block_levels(key, shape, shards, -0.22, 0.18)
    return jnp.clip(drawn, -most, most).astype(kind)


def setup_inputs(seed: int = 0) -> dict:
    splits = jax.random.split(jax.random.key(seed), 22)
    probe_vectors = scatter_about(splits[0], (TOKENS, H * DK), 1.0, 6.0, ((0, 8), (1, 4)))
    address_vectors = scatter_about(splits[1], (TOKENS, H * DK), 1.0, 6.0, ((0, 8), (1, 4)))
    content_vectors = scatter_about(splits[2], (TOKENS, H * DV), 1.0, 6.0, ((0, 8), (1, 4)))
    storage_raw_signal = draw_storage_raw_signal(jax.random.fold_in(splits[21], 71), 0)
    fade_raw_signal = draw_fade_raw_signal(jax.random.fold_in(splits[21], 71), 0)
    channel_fade_exponent = draw_channel_fade_exponent(jax.random.fold_in(splits[21], 71), 0)
    extra_fade_amount = draw_extra_fade_amount(jax.random.fold_in(splits[21], 71), 0)
    sequence_label = jnp.searchsorted(jnp.cumsum(uneven(splits[7], DOCS, TOKENS, DOC_SPAN, 1)), jnp.arange(TOKENS), side="right").astype(jnp.int32)
    exit_valve_raw_signal = scatter_about(splits[8], (TOKENS, H * DV), 1.0, 6.0, ((0, 8), (1, 4)))
    final_projection_matrix = scatter_about(splits[9], (H * DV, D), (H * DV) ** -0.5, 0.125, ((0, 4),))
    incoming_rows_matrix = draw_incoming_rows_matrix(jax.random.fold_in(splits[21], 71), 0)
    initial_rescale_factor = draw_initial_rescale_factor(jax.random.fold_in(splits[21], 71), 0)
    specialist_picks_keys = jax.random.split(jax.random.fold_in(splits[12], 1), TOKENS // TOK_DEV)
    specialist_picks_turns = jax.random.permutation(jax.random.fold_in(splits[12], 3), TOKENS // TOK_DEV)
    specialist_picks = jax.vmap(lambda own, number: assign_block(jax.random.fold_in(splits[12], 2), own, number, TOK_DEV, EXPERTS, TOP, CAP, 1))(specialist_picks_keys, specialist_picks_turns).reshape((TOKENS, TOP))
    picked_specialist_share = jnp.clip(0.29882812 + 0.8964844 * jax.random.uniform(splits[13], (TOKENS, TOP), jnp.float32) ** block_levels(splits[13], (TOKENS, TOP), ((0, 8),), -0.2, 0.2), 0.29882812, 1.1953125).astype(jnp.bfloat16)
    specialist_valve_matrix = scatter_about(splits[14], (EXPERTS, D, FF), D ** -0.5, 0.125, ((0, 8), (2, 4)))
    specialist_raising_matrix = scatter_about(splits[15], (EXPERTS, D, FF), D ** -0.5, 0.125, ((0, 8), (2, 4)))
    specialist_lowering_matrix = scatter_about(splits[16], (EXPERTS, FF, D), FF ** -0.5, 0.09375, ((0, 8), (1, 4)))
    common_valve_matrix = scatter_about(splits[17], (D, SF), D ** -0.5, 0.125, ((1, 4),))
    common_raising_matrix = scatter_about(splits[18], (D, SF), D ** -0.5, 0.125, ((1, 4),))
    common_lowering_matrix = scatter_about(splits[19], (SF, D), SF ** -0.5, 0.25, ((0, 4),))
    latter_rescale_factor = jnp.clip(1.0 + 0.18 * jax.random.normal(splits[20], (D,), jnp.float32), 0.1, 1.9)
    return dict(probe_vectors=probe_vectors, address_vectors=address_vectors, content_vectors=content_vectors, storage_raw_signal=storage_raw_signal, fade_raw_signal=fade_raw_signal, channel_fade_exponent=channel_fade_exponent, extra_fade_amount=extra_fade_amount, sequence_label=sequence_label, exit_valve_raw_signal=exit_valve_raw_signal, final_projection_matrix=final_projection_matrix, incoming_rows_matrix=incoming_rows_matrix, initial_rescale_factor=initial_rescale_factor, specialist_picks=specialist_picks, picked_specialist_share=picked_specialist_share, specialist_valve_matrix=specialist_valve_matrix, specialist_raising_matrix=specialist_raising_matrix, specialist_lowering_matrix=specialist_lowering_matrix, common_valve_matrix=common_valve_matrix, common_raising_matrix=common_raising_matrix, common_lowering_matrix=common_lowering_matrix, latter_rescale_factor=latter_rescale_factor)


HIGH = lax.Precision.HIGHEST
ALPHA = 2.0 ** 0.25

def stored_value(array):
    return lax.optimization_barrier(array.astype(jnp.bfloat16)).astype(jnp.float32)

def unit_rows(array):
    return array * lax.rsqrt(lax.optimization_barrier(jnp.sum(array * array, -1, keepdims=True)) + 1e-06)

def layer_norm(summed, gain):
    row_mean = lax.optimization_barrier(jnp.mean(summed, -1, keepdims=True))
    centred = summed - row_mean
    row_var = lax.optimization_barrier(jnp.mean(centred * centred, -1, keepdims=True))
    return centred * lax.rsqrt(row_var + 1e-05) * gain

def correction_memory_layer(probe_vectors, address_vectors, content_vectors, storage_raw_signal, fade_raw_signal, channel_fade_exponent, extra_fade_amount, sequence_label):
    query_unit = unit_rows(probe_vectors.astype(jnp.float32).reshape(TOKENS, H, DK)) * DK ** (-0.5)
    key_unit = unit_rows(address_vectors.astype(jnp.float32).reshape(TOKENS, H, DK))
    value_rows = content_vectors.astype(jnp.float32).reshape(TOKENS, H, DV)
    write_gate = jax.nn.sigmoid(storage_raw_signal).T
    fade_factor = jnp.exp(extra_fade_amount - jnp.exp(channel_fade_exponent)[:, None] * jax.nn.softplus(fade_raw_signal)).T
    prior = jnp.concatenate([sequence_label[:1], sequence_label[:-1]])
    keep_state = (sequence_label == prior).astype(jnp.float32)

    def advance(carry_state, inputs):
        query_t, key_t, value_t, write_t, decay_t, keep_t = inputs
        carry_state = carry_state * keep_t
        read_back = jnp.einsum('hd,hde->he', key_t, carry_state, precision=HIGH)
        erased = carry_state - write_t[:, None, None] * key_t[:, :, None] * read_back[:, None, :]
        carry_state = decay_t[:, None, None] * erased + write_t[:, None, None] * key_t[:, :, None] * value_t[:, None, :]
        output_t = jnp.einsum('hd,hde->he', query_t, carry_state, precision=HIGH)
        return (carry_state, output_t)
    initial = jnp.zeros((H, DK, DV), jnp.float32)
    unused, memory_layer_result = lax.scan(advance, initial, (query_unit, key_unit, value_rows, write_gate, fade_factor, keep_state))
    return memory_layer_result

def expert_layer(middle, specialist_picks, picked_specialist_share, specialist_valve_matrix, specialist_raising_matrix, specialist_lowering_matrix, common_valve_matrix, common_raising_matrix, common_lowering_matrix):
    picks = TOKENS * TOP
    slots = N_SP * CAP
    flat_routes = specialist_picks.reshape(picks)
    flat_weights = picked_specialist_share.reshape(picks).astype(jnp.float32)
    group_ff = FF // N_TP
    group_sf = SF // N_TP

    def visit(total, expert):
        chosen = flat_routes == expert
        rank_in = jnp.cumsum(chosen.astype(jnp.int32)) - 1
        target = jnp.where(chosen, rank_in, slots)
        owner = jnp.full((slots,), picks, jnp.int32).at[target].set(jnp.arange(picks, dtype=jnp.int32), mode='drop')
        live = (owner < picks).astype(jnp.float32)
        safe_owner = jnp.minimum(owner, picks - 1)
        source_row = safe_owner // TOP
        shared_flag = (safe_owner % TOP == 0).astype(jnp.float32) * live
        weight_e = flat_weights[safe_owner] * live
        inputs_e = middle[source_row]
        gate_e = jnp.dot(inputs_e, specialist_valve_matrix[expert], preferred_element_type=jnp.float32)
        up_e = jnp.dot(inputs_e, specialist_raising_matrix[expert], preferred_element_type=jnp.float32)
        hidden_e = (jax.nn.silu(gate_e) * up_e * weight_e[:, None]).astype(jnp.bfloat16)
        shared_g = jnp.dot(inputs_e, common_valve_matrix, preferred_element_type=jnp.float32)
        shared_u = jnp.dot(inputs_e, common_raising_matrix, preferred_element_type=jnp.float32)
        shared_hidden = (jax.nn.silu(shared_g) * shared_u * shared_flag[:, None]).astype(jnp.bfloat16)
        down_e = specialist_lowering_matrix[expert]
        summed = jnp.zeros((slots, D), jnp.float32)
        for group in range(N_TP):
            term = jnp.dot(hidden_e[:, group * group_ff:(group + 1) * group_ff], down_e[group * group_ff:(group + 1) * group_ff], preferred_element_type=jnp.float32)
            term = term + jnp.dot(shared_hidden[:, group * group_sf:(group + 1) * group_sf], common_lowering_matrix[group * group_sf:(group + 1) * group_sf], preferred_element_type=jnp.float32)
            summed = summed + stored_value(term)
        route_out = stored_value(summed)
        total = total.at[source_row].add(route_out * live[:, None])
        return (total, None)
    start = jnp.zeros((TOKENS, D), jnp.float32)
    mixture, unused = lax.scan(visit, start, jnp.arange(EXPERTS, dtype=jnp.int32))
    return mixture

def reference(probe_vectors, address_vectors, content_vectors, storage_raw_signal, fade_raw_signal, channel_fade_exponent, extra_fade_amount, sequence_label, exit_valve_raw_signal, final_projection_matrix, incoming_rows_matrix, initial_rescale_factor, specialist_picks, picked_specialist_share, specialist_valve_matrix, specialist_raising_matrix, specialist_lowering_matrix, common_valve_matrix, common_raising_matrix, common_lowering_matrix, latter_rescale_factor):
    memory_layer_result = correction_memory_layer(probe_vectors, address_vectors, content_vectors, storage_raw_signal, fade_raw_signal, channel_fade_exponent, extra_fade_amount, sequence_label)
    scaled = memory_layer_result * lax.rsqrt(lax.optimization_barrier(jnp.mean(memory_layer_result * memory_layer_result, -1, keepdims=True)) + 1e-06)
    heads_out = (scaled.reshape(TOKENS, H * DV) * jax.nn.silu(exit_valve_raw_signal.astype(jnp.float32))).astype(jnp.bfloat16)
    group_rows = H * DV // N_TP
    projected = jnp.zeros((TOKENS, D), jnp.float32)
    for group in range(N_TP):
        term = jnp.dot(heads_out[:, group * group_rows:(group + 1) * group_rows], final_projection_matrix[group * group_rows:(group + 1) * group_rows], preferred_element_type=jnp.float32)
        projected = projected + stored_value(term)
    first_sum = ALPHA * incoming_rows_matrix.astype(jnp.float32) + projected
    middle = layer_norm(first_sum, initial_rescale_factor).astype(jnp.bfloat16)
    mixture = expert_layer(middle, specialist_picks, picked_specialist_share, specialist_valve_matrix, specialist_raising_matrix, specialist_lowering_matrix, common_valve_matrix, common_raising_matrix, common_lowering_matrix)
    second_sum = ALPHA * middle.astype(jnp.float32) + mixture
    return layer_norm(second_sum, latter_rescale_factor).astype(jnp.bfloat16)
```

```python
import functools

import jax
import jax.numpy as jnp
from jax import lax
from jax.experimental import pallas as pl
from jax.experimental.pallas import tpu as pltpu
from jax.sharding import PartitionSpec as P

DK = 128
DV = 128
ALPHA = 2.0**0.25
F32 = jnp.float32
BF16 = jnp.bfloat16


def dot(left, right, contract=((1,), (0,))):
    return lax.dot_general(left, right, (contract, ((), ())), preferred_element_type=F32)


def split(array):
    high = array.astype(BF16)
    return high, (array - high.astype(F32)).astype(BF16)


def dot3(left, right):
    left_high, left_low = split(left)
    right_high, right_low = split(right)
    return dot(left_high, right_high) + (dot(left_high, right_low) + dot(left_low, right_high))


def dot_left(left, right):
    high, low = split(left)
    return dot(high, right) + dot(low, right)


def triangular_inverse(lower, rows, cols):
    size = lower.shape[0]
    inverse = jnp.where(rows == cols, 1.0, 0.0)
    block = 1
    while block < size:
        ratio = min(8, size // block)
        wide = block * ratio
        inside = rows // wide == cols // wide
        if block > 1:
            inside = inside & (rows // block != cols // block)
        part = jnp.where(inside, lower, 0.0)
        if block == 1:
            power = part
            inverse = inverse - part
        else:
            power = dot3(inverse, part)
            if ratio == 2:
                inverse = inverse - dot3(power, inverse)
        reach = 2
        if ratio > 2:
            if block == 1:
                power = dot3(power, power)
            else:
                both = dot3(power, jnp.concatenate([power, inverse], 1))
                power = both[:, :size]
                inverse = inverse - both[:, size:]
            while 2 * reach < ratio:
                both = dot3(power, jnp.concatenate([power, inverse], 1))
                power = both[:, :size]
                inverse = inverse + both[:, size:]
                reach *= 2
            inverse = inverse + dot3(power, inverse)
        block = wide
    return inverse


def delta_kernel(q_ref, k_ref, v_ref, store_ref, fade_ref, extra_ref, rate_ref, label_ref, ms_ref, local_ref, query_ref):
    length = q_ref.shape[0]
    heads = store_ref.shape[0]
    rows = lax.broadcasted_iota(jnp.int32, (length, length), 0)
    cols = lax.broadcasted_iota(jnp.int32, (length, length), 1)
    diagonal = rows == cols
    lower = rows >= cols
    strict = rows > cols
    identity = jnp.where(diagonal, 1.0, 0.0)

    def to_col(row):
        return jnp.sum(jnp.where(diagonal, row, 0.0), 1, keepdims=True)

    def to_row(col):
        return jnp.sum(jnp.where(diagonal, col, 0.0), 0, keepdims=True)

    label_row = label_ref[...].astype(F32)
    label_col = to_col(label_row)
    first = label_col[:1]
    last = label_col[length - 1 :]
    same = label_col == label_row
    carried = jnp.where(label_col == first, 1.0, 0.0)
    closing = jnp.where(label_col == last, 1.0, 0.0)
    through = jnp.where(first == last, 1.0, 0.0)
    fade = fade_ref[...]
    soft = jnp.maximum(fade, 0.0) + jnp.log(1.0 + jnp.exp(-jnp.abs(fade)))
    gates = 1.0 / (1.0 + jnp.exp(-store_ref[...]))
    extra = extra_ref[...]
    for h in range(heads):
        at = slice(h * DK, (h + 1) * DK)
        query = q_ref[:, at]
        key = k_ref[:, at]
        value = v_ref[:, at]
        query_f = query.astype(F32)
        key_f = key.astype(F32)
        query_scale = lax.rsqrt(jnp.sum(query_f * query_f, 1, keepdims=True) + 1e-06) * DK ** (-0.5)
        key_scale = lax.rsqrt(jnp.sum(key_f * key_f, 1, keepdims=True) + 1e-06)
        key_scale_row = to_row(key_scale)
        rate = jnp.exp(jnp.full((1, length), rate_ref[h], F32))
        decay = extra[h : h + 1] - rate * soft[h : h + 1]
        gate_row = gates[h : h + 1]
        gate = to_col(gate_row)
        total = jnp.sum(jnp.where(lower, decay, 0.0), 1, keepdims=True)
        total_row = to_row(total)
        end = total[length - 1 :]
        reach = jnp.where(lower & same, jnp.exp(jnp.where(lower, total - total_row, 0.0)), 0.0)
        growth = jnp.exp(total) * carried
        coupling = dot(key, key, ((1,), (1,))) * (key_scale * gate) * key_scale_row * reach
        coupling = jnp.where(strict, coupling, 0.0)
        scores = dot(query, key, ((1,), (1,))) * query_scale * key_scale_row * reach
        inverse = triangular_inverse(coupling, rows, cols)
        fresh = dot_left(inverse * gate_row, value)
        erase = dot_left(inverse * to_row(gate * key_scale * growth), key)
        both = jnp.concatenate([fresh, erase], 1)
        tail = key_scale * jnp.exp(end - total) * closing
        high, low = split(both * tail)
        over = ((0,), (0,))
        carry = dot(key, high, over) + dot(key, low, over)
        seen = dot3(scores, both)
        final = jnp.exp(end) * through
        ms_ref[h, :DK] = (final * identity[:DK, :DK] - carry[:, DV:]).astype(BF16)
        ms_ref[h, DK:] = carry[:, :DV].astype(BF16)
        local_ref[:, at] = seen[:, :DV]
        query_ref[:, at] = query_f * (query_scale * growth) - seen[:, DV:]


def fold_kernel(ms_ref, state_ref, entering_ref, leaving_ref):
    state = state_ref[...].astype(F32)
    for j in range(ms_ref.shape[0]):
        entering_ref[j] = state.astype(BF16)
        high, low = split(state)
        moved = dot(ms_ref[j, :DK], jnp.concatenate([high, low], 1))
        state = moved[:, :DV] + moved[:, DV:] + ms_ref[j, DK:].astype(F32)
    leaving_ref[...] = state.astype(BF16)


def project_kernel(match_ref, local_ref, query_ref, state_ref, valve_ref, weight_ref, out_ref):
    heads = state_ref.shape[0]
    pieces = []
    for h in range(heads):
        at = slice(h * DV, (h + 1) * DV)
        mixed = local_ref[:, at] + match_ref[0] * dot_left(query_ref[:, at], state_ref[h])
        scaled = mixed * lax.rsqrt(jnp.mean(mixed * mixed, 1, keepdims=True) + 1e-06)
        valve = valve_ref[:, at].astype(F32)
        pieces.append((scaled * (valve / (1.0 + jnp.exp(-valve)))).astype(BF16))
    heads_out = jnp.concatenate(pieces, 1) if heads > 1 else pieces[0]
    width = out_ref.shape[2]
    for b in range(out_ref.shape[0]):
        out_ref[b] = dot(heads_out, weight_ref[:, b * width : (b + 1) * width]).astype(BF16)


def expert_kernel(offsets, slots, capacity, *refs):
    count = len(offsets)
    place_ref = refs[0]
    piece_refs = refs[1 : 1 + count]
    valve_ref, raise_ref, lower_ref, cv_ref, cr_ref, cl_ref, out_ref, sum_ref, share_ref = refs[1 + count :]
    step = pl.program_id(0)
    width = piece_refs[0].shape[1]
    total = piece_refs[0].shape[0]

    def starts():
        return [pl.multiple_of((place_ref[0] ^ offset) * width, width) for offset in offsets]

    def product(weights):
        result = None
        for piece, start in zip(piece_refs, starts()):
            term = dot(piece[...], weights(start))
            result = term if result is None else result + term
        return result

    @pl.when(step == 0)
    def _():
        own = piece_refs[0]
        rows = lax.broadcasted_iota(jnp.int32, (slots, 128), 0)
        cols = lax.broadcasted_iota(jnp.int32, (slots, 128), 1)
        pick = rows == cols
        base = capacity // 8 * 8
        shares, flags = [], []
        for source in range(total // slots):
            info = own[source * slots + base : source * slots + base + 8, :].astype(F32)
            info = info[capacity - base : capacity - base + 1]
            shares.append(jnp.sum(jnp.where(pick, info[:, :128], 0.0), 1, keepdims=True))
        share_ref[...] = jnp.concatenate(shares, 0)
        flag = jnp.where(share_ref[...] < 0.0, 1.0, 0.0)
        gate = product(lambda start: cv_ref[pl.ds(start, width), :])
        lift = product(lambda start: cr_ref[pl.ds(start, width), :])
        hidden = (gate / (1.0 + jnp.exp(-gate)) * lift * flag).astype(BF16)
        sum_ref[...] = dot(hidden, cl_ref[...])

    gate = product(lambda start: valve_ref[0, pl.ds(start, width), :])
    lift = product(lambda start: raise_ref[0, pl.ds(start, width), :])
    hidden = (gate / (1.0 + jnp.exp(-gate)) * lift * jnp.abs(share_ref[...])).astype(BF16)
    sum_ref[...] += dot(hidden, lower_ref[0])

    @pl.when(step == pl.num_programs(0) - 1)
    def _():
        for b in range(out_ref.shape[0]):
            out_ref[b] = sum_ref[:, b * width : (b + 1) * width].astype(BF16)


def swap(array, axis, bit):
    size = lax.axis_size(axis)
    return lax.ppermute(array, axis, [(i, i ^ bit) for i in range(size)])


def scatter_sum(blocks, axis):
    place = lax.axis_index(axis)
    bit = 1
    while blocks.shape[0] > 1:
        pairs = blocks.reshape((blocks.shape[0] // 2, 2) + blocks.shape[1:])
        side = (place // bit) % 2
        keep = lax.dynamic_index_in_dim(pairs, side, 1, False)
        send = lax.dynamic_index_in_dim(pairs, 1 - side, 1, False)
        got = swap(send.astype(BF16), axis, bit)
        blocks = keep.astype(F32) + got.astype(F32)
        bit *= 2
    return blocks[0].astype(F32)


def sum_all(array, axis):
    bit = 1
    while bit < lax.axis_size(axis):
        array = array + swap(array, axis, bit)
        bit *= 2
    return array


def gather_pieces(array, axis):
    size = lax.axis_size(axis)
    pieces, offsets = [array], [0]
    bit = size // 2
    while bit:
        pieces = pieces + [swap(piece, axis, bit) for piece in pieces]
        offsets = offsets + [offset ^ bit for offset in offsets]
        bit //= 2
    return pieces, offsets


def feature_norm(summed, gain):
    width = summed.shape[-1] * lax.axis_size("tp")
    sums = sum_all(jnp.stack([jnp.sum(summed, -1), jnp.sum(summed * summed, -1)]), "tp")
    row_mean = sums[0] / width
    row_var = sums[1] / width - row_mean * row_mean
    return (summed - row_mean[:, None]) * lax.rsqrt(row_var[:, None] + 1e-05) * gain


def call(kernel, outs, *args, **kw):
    shapes = [jax.ShapeDtypeStruct(shape, kind) for shape, kind in outs]
    return pl.pallas_call(kernel, out_shape=shapes, **kw)(*args)


def smem():
    return pl.BlockSpec(memory_space=pltpu.SMEM)


def vmem():
    return pl.BlockSpec(memory_space=pltpu.VMEM)


def shards(
    probe_vectors,
    address_vectors,
    content_vectors,
    storage_raw_signal,
    fade_raw_signal,
    channel_fade_exponent,
    extra_fade_amount,
    sequence_label,
    exit_valve_raw_signal,
    final_projection_matrix,
    incoming_rows_matrix,
    initial_rescale_factor,
    specialist_picks,
    picked_specialist_share,
    specialist_valve_matrix,
    specialist_raising_matrix,
    specialist_lowering_matrix,
    common_valve_matrix,
    common_raising_matrix,
    common_lowering_matrix,
    latter_rescale_factor,
):
    tokens, width = incoming_rows_matrix.shape
    heads = storage_raw_signal.shape[0]
    n_sp = lax.axis_size("sp")
    n_tp = lax.axis_size("tp")
    big = pltpu.CompilerParams(vmem_limit_bytes=40 * 1024 * 1024)

    before = lax.ppermute(sequence_label[-1:], "sp", [(i, i + 1) for i in range(n_sp - 1)])
    match = ((before == sequence_label[:1]) & (lax.axis_index("sp") > 0)).astype(F32)

    ms, local, query = call(
        delta_kernel,
        [((heads, DK + DK, DV), BF16), ((tokens, heads * DV), F32), ((tokens, heads * DK), F32)],
        probe_vectors,
        address_vectors,
        content_vectors,
        storage_raw_signal,
        fade_raw_signal,
        extra_fade_amount,
        channel_fade_exponent,
        sequence_label[None, :],
        in_specs=[vmem()] * 6 + [smem(), vmem()],
        compiler_params=big,
    )
    is_map = lax.broadcasted_iota(jnp.int32, (1, DK + DK, 1), 1) < DK
    ms = jnp.where(is_map, ms * match.astype(BF16), ms)

    groups = [[s * heads + i for i in range(heads)] for s in range(n_sp // heads)]

    def exchange(blocks):
        if heads == 1:
            return blocks
        return lax.all_to_all(blocks, "sp", 0, 0, axis_index_groups=groups, tiled=True)

    mine = exchange(ms)

    def fold(state):
        return call(fold_kernel, [((heads, DK, DV), BF16), ((DK, DV), BF16)], mine, state)

    onward = [(i, i + heads) for i in range(n_sp - heads)]

    def hop(_, leaving):
        return fold(lax.ppermute(leaving, "sp", onward))[1]

    leaving = fold(jnp.zeros((DK, DV), BF16))[1]
    segments = n_sp // heads
    if segments > 2:
        leaving = lax.fori_loop(0, segments - 2, hop, leaving)
    entering = exchange(fold(lax.ppermute(leaving, "sp", onward))[0])

    (partial,) = call(
        project_kernel,
        [((n_tp, tokens, width), BF16)],
        match,
        local,
        query,
        entering,
        exit_valve_raw_signal,
        final_projection_matrix,
        in_specs=[smem()] + [vmem()] * 5,
        compiler_params=big,
    )
    projected = scatter_sum(partial, "tp")
    middle = feature_norm(
        ALPHA * incoming_rows_matrix.astype(F32) + projected, initial_rescale_factor
    ).astype(BF16)

    top = specialist_picks.shape[1]
    experts = specialist_valve_matrix.shape[0] * n_sp
    capacity = max(2, 9 * tokens * top // (8 * experts))
    slots = (capacity + 8) // 8 * 8
    named = specialist_picks.T[:, None, :] == jnp.arange(experts, dtype=jnp.int32)[None, :, None]
    taken = jnp.any(named, 0)
    earlier = jnp.arange(tokens)[:, None] < jnp.arange(tokens)[None, :]
    rank = jnp.dot(taken.astype(BF16), earlier.astype(BF16), preferred_element_type=F32)
    slot_index = jnp.arange(slots, dtype=jnp.int32)
    chosen = taken[:, None, :] & (rank.astype(jnp.int32)[:, None, :] == slot_index[None, :, None])
    chosen = chosen & (slot_index < capacity)[None, :, None]
    pick = chosen.astype(BF16).reshape(experts * slots, tokens)
    share = picked_specialist_share.astype(F32).T[:, None, :]
    sign = jnp.where(jnp.arange(top) == 0, -1.0, 1.0)[:, None, None]
    signed = jnp.sum(jnp.where(named, share * sign, 0.0), 0)
    slot_share = jnp.sum(jnp.where(chosen, signed[:, None, :], 0.0), 2)
    lane = jnp.arange(width, dtype=jnp.int32)
    info = jnp.pad(slot_share, ((0, 0), (0, width - slots)))
    info = jnp.where((slot_index == capacity)[None, :, None], info[:, None, :], 0.0)
    sent = jnp.dot(pick, middle, preferred_element_type=F32).reshape(experts, slots, width)
    sent = (sent + info).astype(BF16)
    arrived = lax.all_to_all(sent, "sp", 0, 0, tiled=True).reshape(experts * slots, width)

    pieces, offsets = gather_pieces(arrived, "tp")
    hidden = specialist_valve_matrix.shape[2]
    step = min(hidden, 256)
    total = experts * slots

    def whole_block(shape):
        return pl.BlockSpec(shape, lambda i: (0,) * len(shape))

    shared = common_valve_matrix.shape[1]
    results = pl.pallas_call(
        functools.partial(expert_kernel, offsets, slots, capacity),
        grid=(hidden // step,),
        in_specs=[smem()]
        + [whole_block((total, width))] * n_tp
        + [
            pl.BlockSpec((1, n_tp * width, step), lambda i: (0, 0, i)),
            pl.BlockSpec((1, n_tp * width, step), lambda i: (0, 0, i)),
            pl.BlockSpec((1, step, n_tp * width), lambda i: (0, i, 0)),
            whole_block((n_tp * width, shared)),
            whole_block((n_tp * width, shared)),
            whole_block((shared, n_tp * width)),
        ],
        out_specs=whole_block((n_tp, total, width)),
        out_shape=jax.ShapeDtypeStruct((n_tp, total, width), BF16),
        scratch_shapes=[pltpu.VMEM((total, n_tp * width), F32), pltpu.VMEM((total, 1), F32)],
        compiler_params=pltpu.CompilerParams(
            dimension_semantics=("arbitrary",), vmem_limit_bytes=50 * 1024 * 1024
        ),
    )(
        lax.axis_index("tp").astype(jnp.int32)[None],
        *pieces,
        specialist_valve_matrix,
        specialist_raising_matrix,
        specialist_lowering_matrix,
        common_valve_matrix,
        common_raising_matrix,
        common_lowering_matrix,
    )
    summed = scatter_sum(results, "tp").astype(BF16).reshape(experts, slots, width)
    returned = lax.all_to_all(summed, "sp", 0, 0, tiled=True).reshape(total, width)
    mixture = lax.dot_general(
        pick, returned, (((0,), (0,)), ((), ())), preferred_element_type=F32
    )
    second_sum = ALPHA * middle.astype(F32) + mixture
    return feature_norm(second_sum, latter_rescale_factor).astype(BF16)


def solution(mesh):
    placed = (
        P("sp", "tp"),
        P("sp", "tp"),
        P("sp", "tp"),
        P("tp", "sp"),
        P("tp", "sp"),
        P("tp"),
        P("tp", "sp"),
        P("sp"),
        P("sp", "tp"),
        P("tp", None),
        P("sp", "tp"),
        P("tp"),
        P("sp", None),
        P("sp", None),
        P("sp", None, "tp"),
        P("sp", None, "tp"),
        P("sp", "tp", None),
        P(None, "tp"),
        P(None, "tp"),
        P("tp", None),
        P("tp"),
    )
    return jax.shard_map(
        shards, mesh=mesh, in_specs=placed, out_specs=P("sp", "tp"), check_vma=False
    )
```

```python
import functools

import jax
import jax.numpy as jnp
from jax import lax
from jax.experimental import pallas as pl
from jax.experimental.pallas import tpu as pltpu
from jax.sharding import PartitionSpec as P


DK = 128
DV = 128
ALPHA = 2.0**0.25
F32 = jnp.float32
BF16 = jnp.bfloat16


def dot(left, right, contract=((1,), (0,))):
    return lax.dot_general(left, right, (contract, ((), ())), preferred_element_type=F32)


def split(array):
    high = array.astype(BF16)
    return high, (array - high.astype(F32)).astype(BF16)


def dot3(left, right):
    left_high, left_low = split(left)
    right_high, right_low = split(right)
    return dot(left_high, right_high) + (dot(left_high, right_low) + dot(left_low, right_high))


def dot_left(left, right):
    high, low = split(left)
    return dot(high, right) + dot(low, right)


def triangular_inverses(lowers, rows, cols):
    size = lowers[0].shape[0]
    identity = jnp.where(rows == cols, 1.0, 0.0)

    def once(left, right):
        return dot(left.astype(BF16), right.astype(BF16))

    def solve(powers, inverses, ratio, block):
        if block == 1:
            inverses = [x - p for p, x in zip(powers, inverses)]
            if ratio > 2:
                powers = [once(p, p) for p in powers]
        elif ratio > 2:
            both = [once(p, jnp.concatenate([p, x], 1)) for p, x in zip(powers, inverses)]
            powers = [pair[:, :size] for pair in both]
            inverses = [x - pair[:, size:] for pair, x in zip(both, inverses)]
        else:
            return [x - once(p, x) for p, x in zip(powers, inverses)]
        if ratio > 2:
            inverses = [x + once(p, x) for p, x in zip(powers, inverses)]
        return inverses

    inverses = [identity for _ in lowers]
    block = 1
    while block < size:
        ratio = min(4, size // block)
        wide = block * ratio
        inside = (rows // wide == cols // wide) & (rows // block != cols // block)
        parts = [jnp.where(inside, lower, 0.0) for lower in lowers]
        if block > 1:
            parts = [once(x, part) for x, part in zip(inverses, parts)]
        inverses = solve(parts, inverses, ratio, block)
        block = wide
    errors = [(identity - x) - dot3(lower, x) for lower, x in zip(lowers, inverses)]
    return [x + once(x, error) for x, error in zip(inverses, errors)]


def delta_kernel(*refs):
    q_ref, k_ref, v_ref, store_ref, fade_ref, extra_ref, rate_ref, label_ref, ms_ref, local_ref, query_ref = refs
    length = q_ref.shape[0]
    heads = store_ref.shape[0]
    every = range(heads)
    rows = lax.broadcasted_iota(jnp.int32, (length, length), 0)
    cols = lax.broadcasted_iota(jnp.int32, (length, length), 1)
    diagonal = rows == cols
    lower = rows >= cols
    strict = rows > cols
    identity = jnp.where(diagonal, 1.0, 0.0)

    def to_col(row):
        return jnp.sum(jnp.where(diagonal, row, 0.0), 1, keepdims=True)

    def to_row(col):
        return jnp.sum(jnp.where(diagonal, col, 0.0), 0, keepdims=True)

    label_row = label_ref[...].astype(F32)
    label_col = to_col(label_row)
    first = label_col[:1]
    last = label_col[length - 1 :]
    same = lower & (label_col == label_row)
    carried = jnp.where(label_col == first, 1.0, 0.0)
    closing = jnp.where(label_col == last, 1.0, 0.0)
    through = jnp.where(first == last, 1.0, 0.0)
    fade = fade_ref[...]
    soft = jnp.maximum(fade, 0.0) + jnp.log(1.0 + jnp.exp(-jnp.abs(fade)))
    gates = 1.0 / (1.0 + jnp.exp(-store_ref[...]))
    extra = extra_ref[...]
    rates = rate_ref[...]
    at = [slice(h * DK, (h + 1) * DK) for h in every]
    queries = [q_ref[:, at[h]] for h in every]
    keys = [k_ref[:, at[h]] for h in every]
    values = [v_ref[:, at[h]] for h in every]

    def scale_of(array):
        wide = array.astype(F32)
        return lax.rsqrt(jnp.sum(wide * wide, 1, keepdims=True) + 1e-06)

    key_scales = [scale_of(key) for key in keys]
    query_scales = [scale_of(query) * DK ** (-0.5) for query in queries]
    products = [dot(key, key, ((1,), (1,))) for key in keys]
    scores = [dot(query, key, ((1,), (1,))) for query, key in zip(queries, keys)]
    gate_rows = [gates[h : h + 1] for h in every]
    gate_cols = [to_col(gate_rows[h]) for h in every]
    decays = [
        extra[h : h + 1] - jnp.exp(rates[:, h : h + 1]) * soft[h : h + 1] for h in every
    ]
    totals = [jnp.sum(jnp.where(lower, decay, 0.0), 1, keepdims=True) for decay in decays]
    ends = [total[length - 1 :] for total in totals]
    reaches = [
        jnp.where(same, jnp.exp(jnp.where(lower, total - to_row(total), 0.0)), 0.0) for total in totals
    ]
    growths = [jnp.exp(total) * carried for total in totals]
    reaches = [reaches[h] * to_row(key_scales[h]) for h in every]
    couplings = [
        jnp.where(strict, products[h] * (key_scales[h] * gate_cols[h]) * reaches[h], 0.0) for h in every
    ]
    scores = [(scores[h] * query_scales[h] * reaches[h]).astype(BF16) for h in every]
    inverses = triangular_inverses(couplings, rows, cols)
    fresh = [dot_left(inverses[h] * gate_rows[h], values[h]) for h in every]
    erase = [
        dot_left(inverses[h] * to_row(gate_cols[h] * key_scales[h] * growths[h]), keys[h]) for h in every
    ]
    both = [jnp.concatenate([fresh[h], erase[h]], 1) for h in every]
    tails = [key_scales[h] * jnp.exp(ends[h] - totals[h]) * closing for h in every]
    carries = [dot(keys[h], (both[h] * tails[h]).astype(BF16), ((0,), (0,))) for h in every]
    seen = [dot(scores[h], both[h].astype(BF16)) for h in every]
    for h in every:
        final = jnp.exp(ends[h]) * through
        ms_ref[h, :DK] = (final * identity[:DK, :DK] - carries[h][:, DV:]).astype(BF16)
        ms_ref[h, DK : DK + DK] = carries[h][:, :DV].astype(BF16)
        ms_ref[h, DK + DK : DK + DK + 8] = jnp.broadcast_to(first, (8, DV)).astype(BF16)
        ms_ref[h, DK + DK + 8 :] = jnp.broadcast_to(last, (8, DV)).astype(BF16)
        local_ref[:, at[h]] = seen[h][:, :DV]
        query_ref[:, at[h]] = queries[h].astype(F32) * (query_scales[h] * growths[h]) - seen[h][:, DV:]


def first_label(ms_ref, j):
    return ms_ref[j, DK + DK : DK + DK + 8].astype(F32)[:1]


def last_label(ms_ref, j):
    return ms_ref[j, DK + DK + 8 :].astype(F32)[:1]


def fold_kernel(ms_ref, state_ref, map_ref, leaving_ref):
    blocks = ms_ref.shape[0]
    for j in range(blocks):
        onto = ms_ref[j, :DK]
        add = ms_ref[j, DK : DK + DK].astype(F32)
        if j == 0:
            state = add
            reach = onto.astype(F32)
        else:
            joined = jnp.where(first_label(ms_ref, j) == last_label(ms_ref, j - 1), 1.0, 0.0)
            state = state * joined
            reach = (reach * joined).astype(BF16)
            state_ref[j - 1] = state
            map_ref[j - 1] = reach
            high, low = split(state)
            moved = dot(onto, jnp.concatenate([high, low, reach], 1))
            state = moved[:, :DV] + moved[:, DV : DV + DV] + add
            reach = moved[:, DV + DV :]
    state_ref[blocks - 1] = state
    map_ref[blocks - 1] = reach.astype(BF16)
    leaving_ref[:DK] = state.astype(BF16)
    leaving_ref[DK:] = ms_ref[blocks - 1, DK + DK :]


def enter_kernel(got_ref, ms_ref, state_ref, map_ref, entering_ref):
    blocks = ms_ref.shape[0]
    last = got_ref[DK + 8 :].astype(F32)[:1]
    joined = jnp.where(first_label(ms_ref, 0) == last, 1.0, 0.0)
    state = (got_ref[:DK].astype(F32) * joined).astype(BF16)
    entering_ref[0] = state
    for j in range(1, blocks):
        entering_ref[j] = (state_ref[j - 1] + dot(map_ref[j - 1], state)).astype(BF16)


def leave_kernel(got_ref, ms_ref, state_ref, map_ref, leaving_ref):
    blocks = ms_ref.shape[0]
    last = got_ref[DK + 8 :].astype(F32)[:1]
    joined = jnp.where(first_label(ms_ref, 0) == last, 1.0, 0.0)
    state = (got_ref[:DK].astype(F32) * joined).astype(BF16)
    leaving_ref[:DK] = (state_ref[blocks - 1] + dot(map_ref[blocks - 1], state)).astype(BF16)
    leaving_ref[DK:] = ms_ref[blocks - 1, DK + DK :]


def project_kernel(place_ref, local_ref, query_ref, state_ref, valve_ref, weight_ref, *out_refs):
    heads = state_ref.shape[0]
    pieces = []
    for h in range(heads):
        at = slice(h * DV, (h + 1) * DV)
        mixed = local_ref[:, at] + dot_left(query_ref[:, at], state_ref[h])
        scaled = mixed * lax.rsqrt(jnp.mean(mixed * mixed, 1, keepdims=True) + 1e-06)
        valve = valve_ref[:, at].astype(F32)
        pieces.append((scaled * (valve / (1.0 + jnp.exp(-valve)))).astype(BF16))
    heads_out = jnp.concatenate(pieces, 1) if heads > 1 else pieces[0]
    width = out_refs[0].shape[1]
    for offset in range(len(out_refs) - 1, -1, -1):
        start = pl.multiple_of((place_ref[0] ^ offset) * width, width)
        out_refs[offset][...] = dot(heads_out, weight_ref[:, pl.ds(start, width)]).astype(BF16)


def silu(array):
    return array / (1.0 + jnp.exp(-array))


def join_pairs(place_ref, piece_refs, row_refs):
    width = piece_refs[0].shape[1]
    odd = place_ref[0] & 1
    for pair, row_ref in enumerate(row_refs):
        row_ref[:, pl.ds(pl.multiple_of(odd * width, width), width)] = piece_refs[2 * pair][...]
        row_ref[:, pl.ds(pl.multiple_of((1 - odd) * width, width), width)] = piece_refs[2 * pair + 1][...]


def products(place_ref, offsets, row_refs, weights):
    result = None
    for pair, row_ref in enumerate(row_refs):
        wide = row_ref.shape[1]
        start = pl.multiple_of(((place_ref[0] ^ offsets[2 * pair]) // 2) * wide, wide)
        term = dot(row_ref[...], weights(pl.ds(start, wide)))
        result = term if result is None else result + term
    return result


def expert_kernel(offsets, others, step, slots, capacity, *refs):
    place_ref = refs[0]
    count = len(offsets)
    pairs = count // 2
    piece_refs = refs[1 : 1 + count]
    valve_ref, raise_ref, cv_ref, cr_ref = refs[1 + count : 5 + count]
    refs = refs[5 + count :]
    row_refs = refs[len(refs) - pairs :]
    join_pairs(place_ref, piece_refs, row_refs)
    first = others == 0
    if first:
        gate_ref, lift_ref, cgate_ref, clift_ref = refs[:4]
    else:
        own_ref, gate_ref, lift_ref, cgate_ref, clift_ref, lower_ref, cl_ref = refs[:7]
        out_refs = refs[7 : 7 + others]
        hidden_ref, shared_ref = refs[7 + others : 9 + others]
        rows = lax.broadcasted_iota(jnp.int32, (slots, 128), 0)
        cols = lax.broadcasted_iota(jnp.int32, (slots, 128), 1)
        base = capacity // 8 * 8
        shares = []
        for source in range(own_ref.shape[0] // slots):
            info = own_ref[source * slots + base : source * slots + base + 8, :].astype(F32)
            info = info[capacity - base : capacity - base + 1]
            shares.append(jnp.sum(jnp.where(rows == cols, info[:, :128], 0.0), 1, keepdims=True))
        share = jnp.concatenate(shares, 0)

    cgate = products(place_ref, offsets, row_refs, lambda at: cv_ref[at, :])
    clift = products(place_ref, offsets, row_refs, lambda at: cr_ref[at, :])
    if first:
        cgate_ref[...] = cgate
        clift_ref[...] = clift
    else:
        flag = jnp.where(share < 0.0, 1.0, 0.0)
        shared_ref[...] = (silu(cgate_ref[...] + cgate) * (clift_ref[...] + clift) * flag).astype(BF16)
        share = jnp.abs(share)

    def chunk(i, _):
        cut = pl.ds(pl.multiple_of(i * step, step), step)
        gate = products(place_ref, offsets, row_refs, lambda at: valve_ref[0, at, cut])
        lift = products(place_ref, offsets, row_refs, lambda at: raise_ref[0, at, cut])
        if first:
            gate_ref[:, cut] = gate
            lift_ref[:, cut] = lift
        else:
            hidden_ref[:, cut] = (silu(gate_ref[:, cut] + gate) * (lift_ref[:, cut] + lift) * share).astype(BF16)
        return 0

    lax.fori_loop(0, valve_ref.shape[2] // step, chunk, 0)
    if not first:
        width = piece_refs[0].shape[1]
        for offset in range(others - 1, -1, -1):
            cut = pl.ds(pl.multiple_of((place_ref[0] ^ offset) * width, width), width)
            term = dot(hidden_ref[...], lower_ref[0, :, cut]) + dot(shared_ref[...], cl_ref[:, cut])
            out_refs[offset][...] = term.astype(BF16)


def swap(array, axis, bit):
    size = lax.axis_size(axis)
    return lax.ppermute(array, axis, [(i, i ^ bit) for i in range(size)])


def scatter_sum(blocks, axis):
    bit = 1
    while len(blocks) > 1:
        kept = {}
        for k in range(len(blocks) - 1, 0, -2):
            got = swap(blocks[k].astype(BF16), axis, bit)
            kept[k // 2] = blocks[k - 1].astype(F32) + got.astype(F32)
        blocks = [kept[k] for k in range(len(blocks) // 2)]
        bit *= 2
    return blocks[0].astype(F32)


def sum_all(array, axis):
    bit = 1
    while bit < lax.axis_size(axis):
        array = array + swap(array, axis, bit)
        bit *= 2
    return array


def gather_pieces(array, axis):
    size = lax.axis_size(axis)
    pieces = {0: array}
    bit = size // 2
    while bit:
        for k, piece in list(pieces.items()):
            pieces[k ^ bit] = swap(piece, axis, bit)
        bit //= 2
    return pieces


def feature_norm(summed, gain):
    width = summed.shape[-1] * lax.axis_size("tp")
    sums = sum_all(jnp.stack([jnp.sum(summed, -1), jnp.sum(summed * summed, -1)]), "tp")
    row_mean = sums[0] / width
    row_var = sums[1] / width - row_mean * row_mean
    return (summed - row_mean[:, None]) * lax.rsqrt(row_var[:, None] + 1e-05) * gain


def call(kernel, outs, *args, in_specs=None, out_specs=None, limit=12, flops=4 * 10**9, **kw):
    shapes = [jax.ShapeDtypeStruct(shape, kind) for shape, kind in outs]
    moved = sum(array.size * array.dtype.itemsize for array in args)
    return pl.pallas_call(
        kernel,
        out_shape=shapes,
        in_specs=in_specs or [vmem()] * len(args),
        out_specs=out_specs or [vmem()] * len(outs),
        compiler_params=pltpu.CompilerParams(vmem_limit_bytes=limit * 1024 * 1024),
        cost_estimate=pl.CostEstimate(flops=flops, bytes_accessed=moved, transcendentals=0),
        **kw,
    )(*args)


def smem():
    return pl.BlockSpec(memory_space=pltpu.SMEM)


def vmem():
    return pl.BlockSpec(memory_space=pltpu.VMEM)


def shards(
    probe_vectors,
    address_vectors,
    content_vectors,
    storage_raw_signal,
    fade_raw_signal,
    channel_fade_exponent,
    extra_fade_amount,
    sequence_label,
    exit_valve_raw_signal,
    final_projection_matrix,
    incoming_rows_matrix,
    initial_rescale_factor,
    specialist_picks,
    picked_specialist_share,
    specialist_valve_matrix,
    specialist_raising_matrix,
    specialist_lowering_matrix,
    common_valve_matrix,
    common_raising_matrix,
    common_lowering_matrix,
    latter_rescale_factor,
):
    tokens, width = incoming_rows_matrix.shape
    heads = storage_raw_signal.shape[0]
    n_sp = lax.axis_size("sp")
    n_tp = lax.axis_size("tp")

    place = lax.axis_index("tp").astype(jnp.int32)[None]

    inputs = (
        probe_vectors,
        address_vectors,
        content_vectors,
        storage_raw_signal,
        fade_raw_signal,
        extra_fade_amount,
        channel_fade_exponent[None, :],
        sequence_label[None, :],
    )
    shapes = [((heads, DK + DK + 16, DV), BF16), ((tokens, heads * DV), F32), ((tokens, heads * DK), F32)]

    def one_step(shape):
        return pl.BlockSpec(shape, lambda i: (0,) * len(shape))

    ms, local, query = call(
        delta_kernel,
        shapes,
        *inputs,
        grid=(1,),
        in_specs=[one_step(array.shape) for array in inputs],
        out_specs=[one_step(shape) for shape, _ in shapes],
        limit=61,
        flops=2 * 10**9,
    )

    groups = [[s * heads + i for i in range(heads)] for s in range(n_sp // heads)]

    def exchange(blocks):
        if heads == 1:
            return blocks
        return lax.all_to_all(blocks, "sp", 0, 0, axis_index_groups=groups, tiled=True)

    mine = exchange(ms)
    states, maps, leaving = call(
        fold_kernel,
        [((heads, DK, DV), F32), ((heads, DK, DK), BF16), ((DK + 16, DV), BF16)],
        mine,
    )
    onward = [(i, i + heads) for i in range(n_sp - heads)]

    def hop(_, leaving):
        got = lax.ppermute(leaving, "sp", onward)
        return call(leave_kernel, [((DK + 16, DV), BF16)], got, mine, states, maps)[0]

    segments = n_sp // heads
    if segments > 2:
        leaving = lax.fori_loop(0, segments - 2, hop, leaving)
    got = lax.ppermute(leaving, "sp", onward)
    (entering,) = call(enter_kernel, [((heads, DK, DV), BF16)], got, mine, states, maps)
    entering = exchange(entering)

    partial = call(
        project_kernel,
        [((tokens, width), BF16)] * n_tp,
        place,
        local,
        query,
        entering,
        exit_valve_raw_signal,
        final_projection_matrix,
        in_specs=[smem()] + [vmem()] * 5,
    )
    projected = scatter_sum(partial, "tp")
    middle = feature_norm(
        ALPHA * incoming_rows_matrix.astype(F32) + projected, initial_rescale_factor
    ).astype(BF16)

    top = specialist_picks.shape[1]
    experts = specialist_valve_matrix.shape[0] * n_sp
    capacity = max(2, 9 * tokens * top // (8 * experts))
    slots = (capacity + 8) // 8 * 8
    named = specialist_picks.T[:, None, :] == jnp.arange(experts, dtype=jnp.int32)[None, :, None]
    taken = jnp.any(named, 0)
    earlier = jnp.arange(tokens)[:, None] < jnp.arange(tokens)[None, :]
    rank = jnp.dot(taken.astype(BF16), earlier.astype(BF16), preferred_element_type=F32)
    slot_index = jnp.arange(slots, dtype=jnp.int32)
    chosen = taken[:, None, :] & (rank.astype(jnp.int32)[:, None, :] == slot_index[None, :, None])
    chosen = chosen & (slot_index < capacity)[None, :, None]
    pick = chosen.astype(BF16).reshape(experts * slots, tokens)
    share = picked_specialist_share.astype(F32).T[:, None, :]
    sign = jnp.where(jnp.arange(top) == 0, -1.0, 1.0)[:, None, None]
    signed = jnp.sum(jnp.where(named, share * sign, 0.0), 0)
    slot_share = jnp.sum(jnp.where(chosen, signed[:, None, :], 0.0), 2)
    lane = jnp.arange(width, dtype=jnp.int32)
    info = jnp.pad(slot_share, ((0, 0), (0, width - slots)))
    info = jnp.where((slot_index == capacity)[None, :, None], info[:, None, :], 0.0)
    sent = jnp.dot(pick, middle, preferred_element_type=F32).reshape(experts, slots, width)
    sent = (sent + info).astype(BF16)
    arrived = lax.all_to_all(sent, "sp", 0, 0, tiled=True).reshape(experts * slots, width)

    by_offset = gather_pieces(arrived, "tp")
    hidden = specialist_valve_matrix.shape[2]
    shared = common_valve_matrix.shape[1]
    total = experts * slots
    step = min(hidden, 256)
    weights = (specialist_valve_matrix, specialist_raising_matrix, common_valve_matrix, common_raising_matrix)
    work = 4 * total * width * (hidden + shared)
    near, far = list(range(2)), list(range(2, n_tp))
    partial = call(
        functools.partial(expert_kernel, near, 0, step, slots, capacity),
        [((total, hidden), F32)] * 2 + [((total, shared), F32)] * 2,
        place,
        *[by_offset[k] for k in near],
        *weights,
        in_specs=[smem()] + [vmem()] * 6,
        scratch_shapes=[pltpu.VMEM((total, 2 * width), BF16)],
        flops=work * 2,
    )
    results = call(
        functools.partial(expert_kernel, far, n_tp, step, slots, capacity),
        [((total, width), BF16)] * n_tp,
        place,
        *[by_offset[k] for k in far],
        *weights,
        arrived,
        *partial,
        specialist_lowering_matrix,
        common_lowering_matrix,
        in_specs=[smem()] + [vmem()] * (n_tp + 9),
        scratch_shapes=[pltpu.VMEM((total, hidden), BF16), pltpu.VMEM((total, shared), BF16)]
        + [pltpu.VMEM((total, 2 * width), BF16)] * (n_tp // 2 - 1),
        flops=work * n_tp,
    )
    summed = scatter_sum(results, "tp").astype(BF16).reshape(experts, slots, width)
    returned = lax.all_to_all(summed, "sp", 0, 0, tiled=True).reshape(total, width)
    mixture = lax.dot_general(
        pick, returned, (((0,), (0,)), ((), ())), preferred_element_type=F32
    )
    second_sum = ALPHA * middle.astype(F32) + mixture
    return feature_norm(second_sum, latter_rescale_factor).astype(BF16)


def solution(mesh):
    placed = (
        P("sp", "tp"),
        P("sp", "tp"),
        P("sp", "tp"),
        P("tp", "sp"),
        P("tp", "sp"),
        P("tp"),
        P("tp", "sp"),
        P("sp"),
        P("sp", "tp"),
        P("tp", None),
        P("sp", "tp"),
        P("tp"),
        P("sp", None),
        P("sp", None),
        P("sp", None, "tp"),
        P("sp", None, "tp"),
        P("sp", "tp", None),
        P(None, "tp"),
        P(None, "tp"),
        P("tp", None),
        P("tp"),
    )

    return jax.shard_map(shards, mesh=mesh, in_specs=placed, out_specs=P("sp", "tp"), check_vma=False)
```

```python
import functools

import jax
import jax.numpy as jnp
from jax import lax
from jax.experimental import pallas as pl
from jax.experimental.pallas import tpu as pltpu
from jax.sharding import PartitionSpec as P


DK = 128
DV = 128
ALPHA = 2.0**0.25
F32 = jnp.float32
BF16 = jnp.bfloat16


def dot(left, right, contract=((1,), (0,))):
    return lax.dot_general(left, right, (contract, ((), ())), preferred_element_type=F32)


def split(array):
    high = array.astype(BF16)
    return high, (array - high.astype(F32)).astype(BF16)


def dot3(left, right):
    left_high, left_low = split(left)
    right_high, right_low = split(right)
    return dot(left_high, right_high) + (dot(left_high, right_low) + dot(left_low, right_high))


def dot_left(left, right):
    high, low = split(left)
    return dot(high, right) + dot(low, right)


def triangular_inverses(lowers, rows, cols):
    size = lowers[0].shape[0]
    identity = jnp.where(rows == cols, 1.0, 0.0)

    def once(left, right):
        return dot(left.astype(BF16), right.astype(BF16))

    def solve(powers, inverses, ratio, block):
        if block == 1:
            inverses = [x - p for p, x in zip(powers, inverses)]
            if ratio > 2:
                powers = [once(p, p) for p in powers]
        elif ratio > 2:
            both = [once(p, jnp.concatenate([p, x], 1)) for p, x in zip(powers, inverses)]
            powers = [pair[:, :size] for pair in both]
            inverses = [x - pair[:, size:] for pair, x in zip(both, inverses)]
        else:
            return [x - once(p, x) for p, x in zip(powers, inverses)]
        if ratio > 2:
            inverses = [x + once(p, x) for p, x in zip(powers, inverses)]
        return inverses

    inverses = [identity for _ in lowers]
    block = 1
    while block < size:
        ratio = min(4, size // block)
        wide = block * ratio
        inside = (rows // wide == cols // wide) & (rows // block != cols // block)
        parts = [jnp.where(inside, lower, 0.0) for lower in lowers]
        if block > 1:
            parts = [once(x, part) for x, part in zip(inverses, parts)]
        inverses = solve(parts, inverses, ratio, block)
        block = wide
    errors = [(identity - x) - dot3(lower, x) for lower, x in zip(lowers, inverses)]
    return [x + once(x, error) for x, error in zip(inverses, errors)]


def delta_kernel(*refs):
    place_ref, q_ref, k_ref, v_ref, store_ref, fade_ref, extra_ref, rate_ref, label_ref = refs[:9]
    ms_refs = refs[9:-2]
    local_ref, query_ref = refs[-2:]
    length = q_ref.shape[0]
    heads = store_ref.shape[0]
    every = range(heads)
    rows = lax.broadcasted_iota(jnp.int32, (length, length), 0)
    cols = lax.broadcasted_iota(jnp.int32, (length, length), 1)
    diagonal = rows == cols
    lower = rows >= cols
    strict = rows > cols
    identity = jnp.where(diagonal, 1.0, 0.0)

    def to_col(row):
        return jnp.sum(jnp.where(diagonal, row, 0.0), 1, keepdims=True)

    def to_row(col):
        return jnp.sum(jnp.where(diagonal, col, 0.0), 0, keepdims=True)

    label_row = label_ref[...].astype(F32)
    label_col = to_col(label_row)
    first = label_col[:1]
    last = label_col[length - 1 :]
    same = lower & (label_col == label_row)
    carried = jnp.where(label_col == first, 1.0, 0.0)
    closing = jnp.where(label_col == last, 1.0, 0.0)
    through = jnp.where(first == last, 1.0, 0.0)
    names = [place_ref[0] ^ k for k in every]
    at = [pl.ds(pl.multiple_of(name * DK, DK), DK) for name in names]
    queries = [q_ref[:, at[h]] for h in every]
    keys = [k_ref[:, at[h]] for h in every]
    values = [v_ref[:, at[h]] for h in every]
    row = [pl.ds(name, 1) for name in names]
    fades = [fade_ref[row[h], :] for h in every]
    softs = [jnp.maximum(fade, 0.0) + jnp.log(1.0 + jnp.exp(-jnp.abs(fade))) for fade in fades]
    rates = [jnp.exp(jnp.full((1, length), rate_ref[names[h]], F32)) for h in every]

    def scale_of(array):
        wide = array.astype(F32)
        return lax.rsqrt(jnp.sum(wide * wide, 1, keepdims=True) + 1e-06)

    key_scales = [scale_of(key) for key in keys]
    query_scales = [scale_of(query) * DK ** (-0.5) for query in queries]
    products = [dot(key, key, ((1,), (1,))) for key in keys]
    scores = [dot(query, key, ((1,), (1,))) for query, key in zip(queries, keys)]
    gate_rows = [1.0 / (1.0 + jnp.exp(-store_ref[row[h], :])) for h in every]
    gate_cols = [to_col(gate_rows[h]) for h in every]
    decays = [extra_ref[row[h], :] - rates[h] * softs[h] for h in every]
    totals = [jnp.sum(jnp.where(lower, decay, 0.0), 1, keepdims=True) for decay in decays]
    ends = [total[length - 1 :] for total in totals]
    reaches = [
        jnp.where(same, jnp.exp(jnp.where(lower, total - to_row(total), 0.0)), 0.0) for total in totals
    ]
    growths = [jnp.exp(total) * carried for total in totals]
    reaches = [reaches[h] * to_row(key_scales[h]) for h in every]
    couplings = [
        jnp.where(strict, products[h] * (key_scales[h] * gate_cols[h]) * reaches[h], 0.0) for h in every
    ]
    scores = [(scores[h] * query_scales[h] * reaches[h]).astype(BF16) for h in every]
    inverses = triangular_inverses(couplings, rows, cols)
    fresh = [dot_left(inverses[h] * gate_rows[h], values[h]) for h in every]
    erase = [
        dot_left(inverses[h] * to_row(gate_cols[h] * key_scales[h] * growths[h]), keys[h]) for h in every
    ]
    both = [jnp.concatenate([fresh[h], erase[h]], 1) for h in every]
    tails = [key_scales[h] * jnp.exp(ends[h] - totals[h]) * closing for h in every]
    carries = [dot(keys[h], (both[h] * tails[h]).astype(BF16), ((0,), (0,))) for h in every]
    seen = [dot(scores[h], both[h].astype(BF16)) for h in every]
    for h in every:
        final = jnp.exp(ends[h]) * through
        ms_refs[h][:DK] = (final * identity[:DK, :DK] - carries[h][:, DV:]).astype(BF16)
        ms_refs[h][DK : DK + DK] = carries[h][:, :DV].astype(BF16)
        ms_refs[h][DK + DK : DK + DK + 8] = jnp.broadcast_to(first, (8, DV)).astype(BF16)
        ms_refs[h][DK + DK + 8 :] = jnp.broadcast_to(last, (8, DV)).astype(BF16)
        local_ref[:, at[h]] = seen[h][:, :DV]
        query_ref[:, at[h]] = queries[h].astype(F32) * (query_scales[h] * growths[h]) - seen[h][:, DV:]


def first_label(ms_ref, j):
    return ms_ref[j, DK + DK : DK + DK + 8].astype(F32)[:1]


def last_label(ms_ref, j):
    return ms_ref[j, DK + DK + 8 :].astype(F32)[:1]


def fold_kernel(place_ref, *refs):
    ms_refs = refs[:-6]
    state_ref, map_ref, start_ref, leaving_ref, end_ref, ms_ref = refs[-6:]
    blocks = len(ms_refs)
    for k in range(blocks):
        ms_ref[place_ref[0] ^ k] = ms_refs[k][...]
    state = jnp.zeros((DK, DV), F32)
    reach = jnp.where(
        lax.broadcasted_iota(jnp.int32, (DK, DK), 0) == lax.broadcasted_iota(jnp.int32, (DK, DK), 1), 1.0, 0.0
    )
    for j in range(blocks):
        if j:
            joined = jnp.where(first_label(ms_ref, j) == last_label(ms_ref, j - 1), 1.0, 0.0)
            state = state * joined
            reach = reach * joined
        onto = ms_ref[j, :DK]
        reach = reach.astype(BF16)
        state_ref[j] = state
        map_ref[j] = reach
        add = ms_ref[j, DK : DK + DK].astype(F32)
        if j:
            high, low = split(state)
            moved = dot(onto, jnp.concatenate([high, low, reach], 1))
            state = moved[:, :DV] + moved[:, DV : DV + DV] + add
            reach = moved[:, DV + DV :]
        else:
            state = add
            reach = onto.astype(F32)
    start_ref[...] = ms_ref[0, DK + DK :]
    leaving_ref[:DK] = state.astype(BF16)
    leaving_ref[DK:] = ms_ref[blocks - 1, DK + DK :]
    end_ref[:DK] = state
    end_ref[DK:] = reach


def arriving(got_ref, start_ref):
    last = got_ref[DK + 8 :].astype(F32)[:1]
    joined = jnp.where(start_ref[:8].astype(F32)[:1] == last, 1.0, 0.0)
    return (got_ref[:DK].astype(F32) * joined).astype(BF16)


def enter_kernel(place_ref, got_ref, start_ref, state_ref, map_ref, *entering_refs):
    state = arriving(got_ref, start_ref)
    for k, entering_ref in enumerate(entering_refs):
        j = place_ref[0] ^ k
        entering_ref[...] = (state_ref[j] + dot(map_ref[j], state)).astype(BF16)


def leave_kernel(got_ref, start_ref, leaving_ref, end_ref, out_ref):
    state = arriving(got_ref, start_ref)
    out_ref[:DK] = (end_ref[:DK] + dot(end_ref[DK:].astype(BF16), state)).astype(BF16)
    out_ref[DK:] = leaving_ref[DK:]


def project_kernel(place_ref, group_ref, local_ref, query_ref, valve_ref, weight_ref, *refs):
    heads = local_ref.shape[1] // DV
    state_refs, out_refs, heads_ref = refs[:heads], refs[heads:-1], refs[-1]
    for k in range(heads):
        at = pl.ds(pl.multiple_of((group_ref[0] ^ k) * DV, DV), DV)
        mixed = local_ref[:, at] + dot_left(query_ref[:, at], state_refs[k][...])
        scaled = mixed * lax.rsqrt(jnp.mean(mixed * mixed, 1, keepdims=True) + 1e-06)
        heads_ref[:, at] = (scaled * silu(valve_ref[:, at].astype(F32))).astype(BF16)
    width = out_refs[0].shape[1]
    for offset in range(len(out_refs) - 1, -1, -1):
        start = pl.multiple_of((place_ref[0] ^ offset) * width, width)
        out_refs[offset][...] = dot(heads_ref[...], weight_ref[:, pl.ds(start, width)]).astype(BF16)


def spread(fields, width):
    rows = lax.broadcasted_iota(jnp.int32, (128, width), 0)
    lanes = lax.broadcasted_iota(jnp.int32, (128, width), 1)
    return jnp.where(lanes // (width // fields) == rows, 1.0, 0.0).astype(BF16)


def own_lane(fields, slots, width):
    rows = lax.broadcasted_iota(jnp.int32, (slots, width), 0)
    lanes = lax.broadcasted_iota(jnp.int32, (slots, width), 1)
    return rows == lanes % (width // fields)


def pack_kernel(capacity, fields, keep_ref, got_ref, row_ref, gain_ref, pick_ref, route_ref, out_ref):
    experts, slots, width = out_ref.shape
    summed = ALPHA * row_ref[...].astype(F32) + (keep_ref[...] + got_ref[...].astype(F32))
    tokens = summed.shape[0]
    mean = jnp.mean(summed, 1, keepdims=True)
    centred = summed - mean
    squares = jnp.sum(centred * centred, 1, keepdims=True)
    gain = gain_ref[...]
    lane = lax.broadcasted_iota(jnp.int32, (tokens, 128), 1)
    notes = jnp.zeros((tokens, 128), F32)
    for value, places in ((mean, (1, 2, 3)), (squares, (4, 5))):
        for place in places:
            piece = value.astype(BF16).astype(F32)
            notes = jnp.where(lane == place, piece, notes)
            value = value - piece
    pick = pick_ref[...]
    body = dot(pick, (centred * gain).astype(BF16))
    notes = dot(pick, notes.astype(BF16))
    routes = dot(pick, route_ref[...], ((1,), (1,)))
    expert = (lax.broadcasted_iota(jnp.int32, (experts * slots, 1), 0) // slots + 1).astype(F32)
    share = jnp.where(routes[:, 2:3] == expert, -routes[:, :1], routes[:, 1:2])
    lane = lax.broadcasted_iota(jnp.int32, (experts * slots, 128), 1)
    notes = jnp.where(lane == 0, share, notes).astype(BF16)
    notes = dot(notes, spread(fields, width))
    mine = own_lane(fields, slots, width)
    gain_high, gain_low = split(gain)
    rows = lax.broadcasted_iota(jnp.int32, (slots, width), 0)
    for e in range(experts):
        here = slice(e * slots, (e + 1) * slots)
        info = jnp.sum(jnp.where(mine, notes[here], 0.0), 0, keepdims=True)
        block = jnp.where(rows == capacity, info, body[here])
        block = jnp.where(rows == capacity + 1, gain_high.astype(F32), block)
        block = jnp.where(rows == capacity + 2, gain_low.astype(F32), block)
        out_ref[e] = block.astype(BF16)


def silu(array):
    return array / (1.0 + jnp.exp(-array))


def read_notes(piece_ref, capacity, slots, fields):
    width = piece_ref.shape[1]
    mine = own_lane(fields, slots, width)
    base = capacity // 8 * 8
    blocks = []
    for source in range(piece_ref.shape[0] // slots):
        info = piece_ref[source * slots + base : source * slots + base + 8, :].astype(F32)
        blocks.append(jnp.where(mine, info[capacity - base : capacity - base + 1], 0.0))
    return dot(jnp.concatenate(blocks, 0).astype(BF16), spread(fields, width), ((1,), (1,)))


def gain_row(array, capacity):
    return array[capacity + 1 : capacity + 2] + array[capacity + 2 : capacity + 3]


def near_kernel(step, slots, capacity, fields, *refs):
    place_ref, piece_refs = refs[0], refs[1:3]
    weight_refs, sum_refs, gain_refs, note_refs = refs[3:7], refs[7:11], refs[11:15], refs[15:17]
    width = piece_refs[0].shape[1]
    at = [pl.ds(pl.multiple_of((place_ref[0] ^ k) * width, width), width) for k in range(2)]

    def product(weight_ref, sum_ref, gain_ref, cut):
        total = None
        for k in range(2):
            weight = weight_ref[at[k], cut] if len(weight_ref.shape) == 2 else weight_ref[0, at[k], cut]
            term = dot(piece_refs[k][...], weight)
            gain_ref[k : k + 1, cut] = gain_row(term, capacity)
            total = term if total is None else total + term
        sum_ref[:, cut] = total

    for i in (2, 3):
        product(weight_refs[i], sum_refs[i], gain_refs[i], slice(None))

    def chunk(i, _):
        cut = pl.ds(pl.multiple_of(i * step, step), step)
        for j in (0, 1):
            product(weight_refs[j], sum_refs[j], gain_refs[j], cut)
        return 0

    lax.fori_loop(0, weight_refs[0].shape[2] // step, chunk, 0)
    for k in range(2):
        note_refs[k][...] = read_notes(piece_refs[k], capacity, slots, fields)


def far_kernel(count, half, step, slots, capacity, fields, *refs):
    place_ref, piece_refs = refs[0], refs[1 : count - 1]
    refs = refs[count - 1 :]
    weight_refs, sum_refs, gain_refs, note_refs = refs[:4], refs[4:8], refs[8:12], refs[12:14]
    own_ref, lower_ref, cl_ref = refs[14:17]
    out_refs = refs[17 : 17 + count]
    hidden_ref, shared_ref = refs[17 + count :]
    height, width = piece_refs[0].shape
    here = slice(half * height, (half + 1) * height)
    at = [pl.ds(pl.multiple_of((place_ref[0] ^ k) * width, width), width) for k in range(2, count)]
    notes = [note_ref[here] for note_ref in note_refs]
    notes = notes + [read_notes(piece_ref, capacity, slots, fields) for piece_ref in piece_refs]
    means = [note[:, 1:2] + note[:, 2:3] + note[:, 3:4] for note in notes]
    mean = sum(means) / count
    offsets = [own_mean - mean for own_mean in means]
    squares = sum(note[:, 4:5] + note[:, 5:6] + width * offset * offset for note, offset in zip(notes, offsets))
    scale = lax.rsqrt(squares / (count * width) + 1e-05)
    share = notes[0][:, :1]
    flag = jnp.where(share < 0.0, 1.0, 0.0)
    share = jnp.abs(share)

    def product(weight_ref, sum_ref, gain_ref, cut):
        total = sum_ref[here, cut]
        for k in range(2):
            total = total + offsets[k] * gain_ref[k : k + 1, cut]
        for k in range(2, count):
            weight = weight_ref[at[k - 2], cut] if len(weight_ref.shape) == 2 else weight_ref[0, at[k - 2], cut]
            term = dot(piece_refs[k - 2][...], weight)
            total = total + term + offsets[k] * gain_row(term, capacity)
        return total * scale

    every = slice(None)
    gate = product(weight_refs[2], sum_refs[2], gain_refs[2], every)
    lift = product(weight_refs[3], sum_refs[3], gain_refs[3], every)
    shared_ref[...] = (silu(gate) * lift * flag).astype(BF16)

    def chunk(i, _):
        cut = pl.ds(pl.multiple_of(i * step, step), step)
        gate = product(weight_refs[0], sum_refs[0], gain_refs[0], cut)
        lift = product(weight_refs[1], sum_refs[1], gain_refs[1], cut)
        hidden_ref[:, cut] = (silu(gate) * lift * share).astype(BF16)
        return 0

    lax.fori_loop(0, weight_refs[0].shape[2] // step, chunk, 0)
    for k in range(count - 1, -1, -1):
        cut = pl.ds(pl.multiple_of((place_ref[0] ^ k) * width, width), width)
        term = dot(hidden_ref[...], lower_ref[0, :, cut]) + dot(shared_ref[...], cl_ref[:, cut])
        if k == 0:
            own = own_ref[here, :].astype(F32)
            term = term + (own + offsets[0] * gain_row(own, capacity)) * (flag * scale * ALPHA)
        out_refs[k][...] = term.astype(out_refs[k].dtype)


def swap(array, axis, bit):
    size = lax.axis_size(axis)
    return lax.ppermute(array, axis, [(i, i ^ bit) for i in range(size)])


def scatter_sum(blocks, axis):
    bit = 1
    while len(blocks) > 1:
        kept = {}
        final = len(blocks) == 2
        for k in range(len(blocks) - 1, 0, -2):
            got = swap(blocks[k].astype(BF16), axis, bit)
            if final:
                return blocks[0].astype(F32), got
            kept[k // 2] = blocks[k - 1].astype(F32) + got.astype(F32)
        blocks = [kept[k] for k in range(len(blocks) // 2)]
        bit *= 2


def sum_all(array, axis):
    bit = 1
    while bit < lax.axis_size(axis):
        array = array + swap(array, axis, bit)
        bit *= 2
    return array


def gather_near(array, axis):
    return [array, swap(array, axis, 1)]


def gather_far(array, axis):
    size = lax.axis_size(axis)
    pieces = {0: array}
    bit = size // 2
    while bit:
        for k, piece in list(pieces.items()):
            if k ^ bit != 1:
                pieces[k ^ bit] = swap(piece, axis, bit)
        bit //= 2
    return [pieces[k] for k in range(2, size)]


def feature_norm(summed, gain):
    width = summed.shape[-1] * lax.axis_size("tp")
    sums = sum_all(jnp.stack([jnp.sum(summed, -1), jnp.sum(summed * summed, -1)]), "tp")
    row_mean = sums[0] / width
    row_var = sums[1] / width - row_mean * row_mean
    return (summed - row_mean[:, None]) * lax.rsqrt(row_var[:, None] + 1e-05) * gain


def call(kernel, outs, *args, in_specs=None, out_specs=None, limit=12, flops=4 * 10**9, **kw):
    shapes = [jax.ShapeDtypeStruct(shape, kind) for shape, kind in outs]
    moved = sum(array.size * array.dtype.itemsize for array in args)
    return pl.pallas_call(
        kernel,
        out_shape=shapes,
        in_specs=in_specs or [vmem()] * len(args),
        out_specs=out_specs or [vmem()] * len(outs),
        compiler_params=pltpu.CompilerParams(vmem_limit_bytes=limit * 1024 * 1024),
        cost_estimate=pl.CostEstimate(flops=flops, bytes_accessed=moved, transcendentals=0),
        **kw,
    )(*args)


def smem():
    return pl.BlockSpec(memory_space=pltpu.SMEM)


def vmem():
    return pl.BlockSpec(memory_space=pltpu.VMEM)


def shards(
    probe_vectors,
    address_vectors,
    content_vectors,
    storage_raw_signal,
    fade_raw_signal,
    channel_fade_exponent,
    extra_fade_amount,
    sequence_label,
    exit_valve_raw_signal,
    final_projection_matrix,
    incoming_rows_matrix,
    initial_rescale_factor,
    specialist_picks,
    picked_specialist_share,
    specialist_valve_matrix,
    specialist_raising_matrix,
    specialist_lowering_matrix,
    common_valve_matrix,
    common_raising_matrix,
    common_lowering_matrix,
    latter_rescale_factor,
):
    tokens, width = incoming_rows_matrix.shape
    heads = storage_raw_signal.shape[0]
    n_sp = lax.axis_size("sp")
    n_tp = lax.axis_size("tp")

    place = lax.axis_index("tp").astype(jnp.int32)[None]

    inputs = (
        probe_vectors,
        address_vectors,
        content_vectors,
        storage_raw_signal,
        fade_raw_signal,
        extra_fade_amount,
        channel_fade_exponent,
        sequence_label[None, :],
    )
    shapes = [((tokens, heads * DV), F32), ((tokens, heads * DK), F32)]

    def one_step(shape):
        return pl.BlockSpec(shape, lambda i: (0,) * len(shape))

    group = (lax.axis_index("sp").astype(jnp.int32) % heads)[None]
    *ms, local, query = call(
        delta_kernel,
        [((DK + DK + 16, DV), BF16)] * heads + shapes,
        group,
        *inputs,
        grid=(1,),
        in_specs=[smem()] + [one_step(array.shape) for array in inputs[:-2]] + [smem(), one_step(inputs[-1].shape)],
        out_specs=[one_step((DK + DK + 16, DV))] * heads + [one_step(shape) for shape, _ in shapes],
        limit=61,
        flops=2 * 10**9,
    )

    def exchange(blocks):
        return [blocks[0]] + [swap(blocks[k], "sp", k) for k in range(1, heads)]

    mine = exchange(ms)
    states, maps, start, leaving, end = call(
        fold_kernel,
        [
            ((heads, DK, DV), F32),
            ((heads, DK, DK), BF16),
            ((16, DV), BF16),
            ((DK + 16, DV), BF16),
            ((DK + DK, DV), F32),
        ],
        group,
        *mine,
        in_specs=[smem()] + [vmem()] * heads,
        scratch_shapes=[pltpu.VMEM((heads, DK + DK + 16, DV), BF16)],
    )
    onward = [(i, i + heads) for i in range(n_sp - heads)]

    def hop(_, leaving):
        got = lax.ppermute(leaving, "sp", onward)
        return call(leave_kernel, [((DK + 16, DV), BF16)], got, start, leaving, end)[0]

    segments = n_sp // heads
    if segments > 2:
        leaving = lax.fori_loop(0, segments - 2, hop, leaving)
    got = lax.ppermute(leaving, "sp", onward)
    entering = exchange(
        call(
            enter_kernel,
            [((DK, DV), BF16)] * heads,
            group,
            got,
            start,
            states,
            maps,
            in_specs=[smem()] + [vmem()] * 4,
        )
    )

    partial = call(
        project_kernel,
        [((tokens, width), BF16)] * n_tp,
        place,
        group,
        local,
        query,
        exit_valve_raw_signal,
        final_projection_matrix,
        *entering,
        in_specs=[smem()] * 2 + [vmem()] * (4 + heads),
        scratch_shapes=[pltpu.VMEM((tokens, heads * DV), BF16)],
    )
    keep, got = scatter_sum(partial, "tp")

    top = specialist_picks.shape[1]
    experts = specialist_valve_matrix.shape[0] * n_sp
    capacity = max(2, 9 * tokens * top // (8 * experts))
    slots = (capacity + 10) // 8 * 8
    named = specialist_picks.T[:, None, :] == jnp.arange(experts, dtype=jnp.int32)[None, :, None]
    taken = jnp.any(named, 0)
    earlier = jnp.arange(tokens)[:, None] < jnp.arange(tokens)[None, :]
    rank = jnp.dot(taken.astype(BF16), earlier.astype(BF16), preferred_element_type=F32)
    slot_index = jnp.arange(slots, dtype=jnp.int32)
    chosen = taken[:, None, :] & (rank.astype(jnp.int32)[:, None, :] == slot_index[None, :, None])
    chosen = chosen & (slot_index < capacity)[None, :, None]
    pick = chosen.astype(BF16).reshape(experts * slots, tokens)
    routes = jnp.concatenate(
        [picked_specialist_share.T.astype(F32), (specialist_picks.T[:1] + 1).astype(F32)], 0
    )
    routes = jnp.pad(routes, ((0, 13), (0, 0))).astype(BF16)
    fields = 8
    (sent,) = call(
        functools.partial(pack_kernel, capacity, fields),
        [((experts, slots, width), BF16)],
        keep,
        got,
        incoming_rows_matrix,
        initial_rescale_factor[None, :],
        pick,
        routes,
    )
    arrived = lax.all_to_all(sent, "sp", 0, 0, tiled=True).reshape(experts * slots, width)

    hidden = specialist_valve_matrix.shape[2]
    shared = common_valve_matrix.shape[1]
    total = experts * slots
    step = min(hidden, 256)
    weights = (specialist_valve_matrix, specialist_raising_matrix, common_valve_matrix, common_raising_matrix)
    work = 4 * total * width * (hidden + shared)
    parts = 2
    height = total // parts
    halves = [gather_far(arrived[i * height : (i + 1) * height], "tp") for i in range(parts)]
    near = gather_near(arrived, "tp")
    common = (step, slots, capacity, fields)
    partial = call(
        functools.partial(near_kernel, *common),
        [((total, hidden), F32)] * 2
        + [((total, shared), F32)] * 2
        + [((8, hidden), F32)] * 2
        + [((8, shared), F32)] * 2
        + [((total, 128), F32)] * 2,
        place,
        *near,
        *weights,
        in_specs=[smem()] + [vmem()] * 6,
        flops=work * 2,
    )
    sums = []
    for i in range(parts):
        results = call(
            functools.partial(far_kernel, n_tp, i, *common),
            [((height, width), F32)] + [((height, width), BF16)] * (n_tp - 1),
            place,
            *halves[i],
            *weights,
            *partial,
            arrived,
            specialist_lowering_matrix,
            common_lowering_matrix,
            in_specs=[smem()] + [vmem()] * (n_tp + 15),
            scratch_shapes=[pltpu.VMEM((height, hidden), BF16), pltpu.VMEM((height, shared), BF16)],
            flops=work * n_tp // parts,
        )
        sums.append(sum(term.astype(F32) for term in scatter_sum(results, "tp")).astype(BF16))
    summed = jnp.concatenate(sums, 0).reshape(experts, slots, width)
    returned = lax.all_to_all(summed, "sp", 0, 0, tiled=True).reshape(total, width)
    second_sum = lax.dot_general(
        pick, returned, (((0,), (0,)), ((), ())), preferred_element_type=F32
    )
    return feature_norm(second_sum, latter_rescale_factor).astype(BF16)


def solution(mesh):
    placed = (
        P("sp", "tp"),
        P("sp", "tp"),
        P("sp", "tp"),
        P("tp", "sp"),
        P("tp", "sp"),
        P("tp"),
        P("tp", "sp"),
        P("sp"),
        P("sp", "tp"),
        P("tp", None),
        P("sp", "tp"),
        P("tp"),
        P("sp", None),
        P("sp", None),
        P("sp", None, "tp"),
        P("sp", None, "tp"),
        P("sp", "tp", None),
        P(None, "tp"),
        P(None, "tp"),
        P("tp", None),
        P("tp"),
    )

    return jax.shard_map(shards, mesh=mesh, in_specs=placed, out_specs=P("sp", "tp"), check_vma=False)
```

```python
import functools

import jax
import jax.numpy as jnp
from jax import lax
from jax.experimental import pallas as pl
from jax.experimental.pallas import tpu as pltpu
from jax.sharding import PartitionSpec as P


DK = 128
DV = 128
ALPHA = 2.0**0.25
F32 = jnp.float32
BF16 = jnp.bfloat16


def dot(left, right, contract=((1,), (0,))):
    return lax.dot_general(left, right, (contract, ((), ())), preferred_element_type=F32)


def split(array):
    high = array.astype(BF16)
    return high, (array - high.astype(F32)).astype(BF16)


def dot3(left, right):
    left_high, left_low = split(left)
    right_high, right_low = split(right)
    return dot(left_high, right_high) + (dot(left_high, right_low) + dot(left_low, right_high))


def dot_left(left, right):
    high, low = split(left)
    return dot(high, right) + dot(low, right)


def triangular_inverses(lowers, rows, cols):
    size = lowers[0].shape[0]
    identity = jnp.where(rows == cols, 1.0, 0.0)

    def once(left, right):
        return dot(left.astype(BF16), right.astype(BF16))

    def solve(powers, inverses, ratio, block):
        if block == 1:
            inverses = [x - p for p, x in zip(powers, inverses)]
            if ratio > 2:
                powers = [once(p, p) for p in powers]
        elif ratio > 2:
            both = [once(p, jnp.concatenate([p, x], 1)) for p, x in zip(powers, inverses)]
            powers = [pair[:, :size] for pair in both]
            inverses = [x - pair[:, size:] for pair, x in zip(both, inverses)]
        else:
            return [x - once(p, x) for p, x in zip(powers, inverses)]
        if ratio > 2:
            inverses = [x + once(p, x) for p, x in zip(powers, inverses)]
        return inverses

    inverses = [identity for _ in lowers]
    block = 1
    while block < size:
        ratio = min(4, size // block)
        wide = block * ratio
        inside = (rows // wide == cols // wide) & (rows // block != cols // block)
        parts = [jnp.where(inside, lower, 0.0) for lower in lowers]
        if block > 1:
            parts = [once(x, part) for x, part in zip(inverses, parts)]
        inverses = solve(parts, inverses, ratio, block)
        block = wide
    errors = [(identity - x) - dot3(lower, x) for lower, x in zip(lowers, inverses)]
    return [x + once(x, error) for x, error in zip(inverses, errors)]


def delta_kernel(*refs):
    place_ref, q_ref, k_ref, v_ref, store_ref, fade_ref, extra_ref, rate_ref, label_ref = refs[:9]
    ms_refs = refs[9:-2]
    local_ref, query_ref = refs[-2:]
    length = q_ref.shape[0]
    heads = store_ref.shape[0]
    every = range(heads)
    rows = lax.broadcasted_iota(jnp.int32, (length, length), 0)
    cols = lax.broadcasted_iota(jnp.int32, (length, length), 1)
    diagonal = rows == cols
    lower = rows >= cols
    strict = rows > cols
    identity = jnp.where(diagonal, 1.0, 0.0)

    def to_col(row):
        return jnp.sum(jnp.where(diagonal, row, 0.0), 1, keepdims=True)

    def to_row(col):
        return jnp.sum(jnp.where(diagonal, col, 0.0), 0, keepdims=True)

    label_row = label_ref[...].astype(F32)
    label_col = to_col(label_row)
    first = label_col[:1]
    last = label_col[length - 1 :]
    same = lower & (label_col == label_row)
    carried = jnp.where(label_col == first, 1.0, 0.0)
    closing = jnp.where(label_col == last, 1.0, 0.0)
    through = jnp.where(first == last, 1.0, 0.0)
    names = [place_ref[0] ^ k for k in every]
    at = [pl.ds(pl.multiple_of(name * DK, DK), DK) for name in names]
    queries = [q_ref[:, at[h]] for h in every]
    keys = [k_ref[:, at[h]] for h in every]
    values = [v_ref[:, at[h]] for h in every]
    row = [pl.ds(name, 1) for name in names]
    fades = [fade_ref[row[h], :] for h in every]
    softs = [jnp.maximum(fade, 0.0) + jnp.log(1.0 + jnp.exp(-jnp.abs(fade))) for fade in fades]
    rates = [jnp.exp(jnp.full((1, length), rate_ref[names[h]], F32)) for h in every]

    def scale_of(array):
        wide = array.astype(F32)
        return lax.rsqrt(jnp.sum(wide * wide, 1, keepdims=True) + 1e-06)

    key_scales = [scale_of(key) for key in keys]
    query_scales = [scale_of(query) * DK ** (-0.5) for query in queries]
    products = [dot(key, key, ((1,), (1,))) for key in keys]
    scores = [dot(query, key, ((1,), (1,))) for query, key in zip(queries, keys)]
    gate_rows = [1.0 / (1.0 + jnp.exp(-store_ref[row[h], :])) for h in every]
    gate_cols = [to_col(gate_rows[h]) for h in every]
    decays = [extra_ref[row[h], :] - rates[h] * softs[h] for h in every]
    totals = [jnp.sum(jnp.where(lower, decay, 0.0), 1, keepdims=True) for decay in decays]
    ends = [total[length - 1 :] for total in totals]
    reaches = [
        jnp.where(same, jnp.exp(jnp.where(lower, total - to_row(total), 0.0)), 0.0) for total in totals
    ]
    growths = [jnp.exp(total) * carried for total in totals]
    reaches = [reaches[h] * to_row(key_scales[h]) for h in every]
    couplings = [
        jnp.where(strict, products[h] * (key_scales[h] * gate_cols[h]) * reaches[h], 0.0) for h in every
    ]
    scores = [(scores[h] * query_scales[h] * reaches[h]).astype(BF16) for h in every]
    inverses = triangular_inverses(couplings, rows, cols)
    fresh = [dot_left(inverses[h] * gate_rows[h], values[h]) for h in every]
    erase = [
        dot_left(inverses[h] * to_row(gate_cols[h] * key_scales[h] * growths[h]), keys[h]) for h in every
    ]
    both = [jnp.concatenate([fresh[h], erase[h]], 1) for h in every]
    tails = [key_scales[h] * jnp.exp(ends[h] - totals[h]) * closing for h in every]
    carries = [dot(keys[h], (both[h] * tails[h]).astype(BF16), ((0,), (0,))) for h in every]
    seen = [dot(scores[h], both[h].astype(BF16)) for h in every]
    for h in every:
        final = jnp.exp(ends[h]) * through
        ms_refs[h][:DK] = (final * identity[:DK, :DK] - carries[h][:, DV:]).astype(BF16)
        ms_refs[h][DK : DK + DK] = carries[h][:, :DV].astype(BF16)
        ms_refs[h][DK + DK : DK + DK + 8] = jnp.broadcast_to(first, (8, DV)).astype(BF16)
        ms_refs[h][DK + DK + 8 :] = jnp.broadcast_to(last, (8, DV)).astype(BF16)
        local_ref[:, at[h]] = seen[h][:, :DV]
        query_ref[:, at[h]] = queries[h].astype(F32) * (query_scales[h] * growths[h]) - seen[h][:, DV:]


def first_label(ms_ref, j):
    return ms_ref[j, DK + DK : DK + DK + 8].astype(F32)[:1]


def last_label(ms_ref, j):
    return ms_ref[j, DK + DK + 8 :].astype(F32)[:1]


def hold_kernel(array_ref, out_ref, done_ref):
    copy = pltpu.make_async_copy(array_ref, out_ref, done_ref)
    copy.start()
    copy.wait()


def fold_kernel(place_ref, *refs):
    ms_refs = refs[:-6]
    state_ref, map_ref, start_ref, leaving_ref, end_ref, ms_ref = refs[-6:]
    blocks = len(ms_refs)
    for k in range(blocks):
        ms_ref[place_ref[0] ^ k] = ms_refs[k][...]
    state = jnp.zeros((DK, DV), F32)
    reach = jnp.where(
        lax.broadcasted_iota(jnp.int32, (DK, DK), 0) == lax.broadcasted_iota(jnp.int32, (DK, DK), 1), 1.0, 0.0
    )
    for j in range(blocks):
        if j:
            joined = jnp.where(first_label(ms_ref, j) == last_label(ms_ref, j - 1), 1.0, 0.0)
            state = state * joined
            reach = reach * joined
        onto = ms_ref[j, :DK]
        reach = reach.astype(BF16)
        state_ref[j] = state
        map_ref[j] = reach
        add = ms_ref[j, DK : DK + DK].astype(F32)
        if j:
            high, low = split(state)
            moved = dot(onto, jnp.concatenate([high, low, reach], 1))
            state = moved[:, :DV] + moved[:, DV : DV + DV] + add
            reach = moved[:, DV + DV :]
        else:
            state = add
            reach = onto.astype(F32)
    start_ref[...] = ms_ref[0, DK + DK :]
    leaving_ref[:DK] = state.astype(BF16)
    leaving_ref[DK:] = ms_ref[blocks - 1, DK + DK :]
    end_ref[:DK] = state
    end_ref[DK:] = reach


def arriving(got_ref, start_ref):
    last = got_ref[DK + 8 :].astype(F32)[:1]
    joined = jnp.where(start_ref[:8].astype(F32)[:1] == last, 1.0, 0.0)
    return (got_ref[:DK].astype(F32) * joined).astype(BF16)


def enter_kernel(place_ref, got_ref, start_ref, state_ref, map_ref, *entering_refs):
    state = arriving(got_ref, start_ref)
    for k, entering_ref in enumerate(entering_refs):
        j = place_ref[0] ^ k
        entering_ref[...] = (state_ref[j] + dot(map_ref[j], state)).astype(BF16)


def leave_kernel(got_ref, start_ref, leaving_ref, end_ref, out_ref):
    state = arriving(got_ref, start_ref)
    out_ref[:DK] = (end_ref[:DK] + dot(end_ref[DK:].astype(BF16), state)).astype(BF16)
    out_ref[DK:] = leaving_ref[DK:]


def project_kernel(place_ref, group_ref, local_ref, query_ref, valve_ref, weight_ref, *refs):
    heads = local_ref.shape[1] // DV
    state_refs, out_refs, heads_ref = refs[:heads], refs[heads:-1], refs[-1]
    for k in range(heads):
        at = pl.ds(pl.multiple_of((group_ref[0] ^ k) * DV, DV), DV)
        mixed = local_ref[:, at] + dot_left(query_ref[:, at], state_refs[k][...])
        scaled = mixed * lax.rsqrt(jnp.mean(mixed * mixed, 1, keepdims=True) + 1e-06)
        heads_ref[:, at] = (scaled * silu(valve_ref[:, at].astype(F32))).astype(BF16)
    width = out_refs[0].shape[1]
    for offset in range(len(out_refs) - 1, -1, -1):
        start = pl.multiple_of((place_ref[0] ^ offset) * width, width)
        out_refs[offset][...] = dot(heads_ref[...], weight_ref[:, pl.ds(start, width)]).astype(BF16)


def spread(fields, width):
    rows = lax.broadcasted_iota(jnp.int32, (128, width), 0)
    lanes = lax.broadcasted_iota(jnp.int32, (128, width), 1)
    return jnp.where(lanes // (width // fields) == rows, 1.0, 0.0).astype(BF16)


def own_lane(fields, slots, width):
    rows = lax.broadcasted_iota(jnp.int32, (slots, width), 0)
    lanes = lax.broadcasted_iota(jnp.int32, (slots, width), 1)
    return rows == lanes % (width // fields)


def route_kernel(capacity, slots, place_ref, named_ref, share_ref, pick_ref, note_ref):
    top, tokens = named_ref.shape
    experts = pick_ref.shape[0] // slots
    named, share = named_ref[...], share_ref[...].astype(F32)
    taken, signed = [], []
    for k in range(experts):
        hit = jnp.where(named == (place_ref[0] ^ k), 1.0, 0.0)
        taken.append(sum(hit[j : j + 1] for j in range(top)))
        signed.append(sum(hit[j : j + 1] * share[j : j + 1] * (1.0 if j else -1.0) for j in range(top)))
    before = lax.broadcasted_iota(jnp.int32, (tokens, tokens), 0)
    after = lax.broadcasted_iota(jnp.int32, (tokens, tokens), 1)
    earlier = jnp.where(before < after, 1.0, 0.0).astype(BF16)
    rank = dot(jnp.concatenate(taken, 0).astype(BF16), earlier)
    slot = lax.broadcasted_iota(jnp.int32, (slots, tokens), 0).astype(F32)
    for k in range(experts):
        chosen = jnp.where(rank[k : k + 1] == slot, taken[k], 0.0)
        chosen = jnp.where(slot < capacity, chosen, 0.0)
        here = slice(k * slots, (k + 1) * slots)
        pick_ref[here] = chosen.astype(BF16)
        note_ref[here] = jnp.sum(chosen * signed[k], 1, keepdims=True)


def pack_kernel(capacity, fields, keep_ref, got_ref, row_ref, gain_ref, pick_ref, share_ref, *out_refs):
    experts = len(out_refs)
    slots, width = out_refs[0].shape
    summed = ALPHA * row_ref[...].astype(F32) + (keep_ref[...] + got_ref[...].astype(F32))
    tokens = summed.shape[0]
    mean = jnp.mean(summed, 1, keepdims=True)
    centred = summed - mean
    squares = jnp.sum(centred * centred, 1, keepdims=True)
    gain = gain_ref[...]
    lane = lax.broadcasted_iota(jnp.int32, (tokens, 128), 1)
    notes = jnp.zeros((tokens, 128), F32)
    for value, places in ((mean, (1, 2, 3)), (squares, (4, 5))):
        for place in places:
            piece = value.astype(BF16).astype(F32)
            notes = jnp.where(lane == place, piece, notes)
            value = value - piece
    pick = pick_ref[...]
    body = dot(pick, (centred * gain).astype(BF16))
    notes = dot(pick, notes.astype(BF16))
    lane = lax.broadcasted_iota(jnp.int32, (experts * slots, 128), 1)
    notes = jnp.where(lane == 0, share_ref[...], notes).astype(BF16)
    notes = dot(notes, spread(fields, width))
    mine = own_lane(fields, slots, width)
    gain_high, gain_low = split(gain)
    rows = lax.broadcasted_iota(jnp.int32, (slots, width), 0)
    for e in range(experts):
        here = slice(e * slots, (e + 1) * slots)
        info = jnp.sum(jnp.where(mine, notes[here], 0.0), 0, keepdims=True)
        block = jnp.where(rows == capacity, info, body[here])
        block = jnp.where(rows == capacity + 1, gain_high.astype(F32), block)
        block = jnp.where(rows == capacity + 2, gain_low.astype(F32), block)
        out_refs[e][...] = block.astype(BF16)


def silu(array):
    return array / (1.0 + jnp.exp(-array))


def read_notes(piece_ref, capacity, slots, fields):
    width = piece_ref.shape[1]
    mine = own_lane(fields, slots, width)
    base = capacity // 8 * 8
    blocks = []
    for source in range(piece_ref.shape[0] // slots):
        info = piece_ref[source * slots + base : source * slots + base + 8, :].astype(F32)
        blocks.append(jnp.where(mine, info[capacity - base : capacity - base + 1], 0.0))
    return dot(jnp.concatenate(blocks, 0).astype(BF16), spread(fields, width), ((1,), (1,)))


def gain_row(array, capacity):
    return array[capacity + 1 : capacity + 2] + array[capacity + 2 : capacity + 3]


def near_kernel(step, slots, capacity, fields, *refs):
    place_ref, piece_refs = refs[0], refs[1:3]
    weight_refs, sum_refs, gain_refs, note_refs = refs[3:7], refs[7:11], refs[11:15], refs[15:17]
    width = piece_refs[0].shape[1]
    at = [pl.ds(pl.multiple_of((place_ref[0] ^ k) * width, width), width) for k in range(2)]

    def product(weight_ref, sum_ref, gain_ref, cut):
        total = None
        for k in range(2):
            weight = weight_ref[at[k], cut] if len(weight_ref.shape) == 2 else weight_ref[0, at[k], cut]
            term = dot(piece_refs[k][...], weight)
            gain_ref[k : k + 1, cut] = gain_row(term, capacity)
            total = term if total is None else total + term
        sum_ref[:, cut] = total

    for i in (2, 3):
        product(weight_refs[i], sum_refs[i], gain_refs[i], slice(None))

    def chunk(i, _):
        cut = pl.ds(pl.multiple_of(i * step, step), step)
        for j in (0, 1):
            product(weight_refs[j], sum_refs[j], gain_refs[j], cut)
        return 0

    lax.fori_loop(0, weight_refs[0].shape[2] // step, chunk, 0)
    for k in range(2):
        note_refs[k][...] = read_notes(piece_refs[k], capacity, slots, fields)


def far_kernel(count, step, slots, capacity, fields, *refs):
    place_ref, piece_refs = refs[0], refs[1 : count - 1]
    refs = refs[count - 1 :]
    weight_refs, sum_refs, gain_refs, note_refs = refs[:4], refs[4:8], refs[8:12], refs[12:14]
    own_ref, lower_ref, cl_ref = refs[14:17]
    out_refs = refs[17 : 17 + count]
    hidden_ref, shared_ref = refs[17 + count :]
    _, width = piece_refs[0].shape
    at = [pl.ds(pl.multiple_of((place_ref[0] ^ k) * width, width), width) for k in range(2, count)]
    notes = [note_ref[...] for note_ref in note_refs]
    notes = notes + [read_notes(piece_ref, capacity, slots, fields) for piece_ref in piece_refs]
    means = [note[:, 1:2] + note[:, 2:3] + note[:, 3:4] for note in notes]
    mean = sum(means) / count
    offsets = [own_mean - mean for own_mean in means]
    squares = sum(note[:, 4:5] + note[:, 5:6] + width * offset * offset for note, offset in zip(notes, offsets))
    scale = lax.rsqrt(squares / (count * width) + 1e-05)
    share = notes[0][:, :1]
    flag = jnp.where(share < 0.0, 1.0, 0.0)
    share = jnp.abs(share)

    def product(weight_ref, sum_ref, gain_ref, cut):
        total = sum_ref[:, cut]
        for k in range(2):
            total = total + offsets[k] * gain_ref[k : k + 1, cut]
        for k in range(2, count):
            weight = weight_ref[at[k - 2], cut] if len(weight_ref.shape) == 2 else weight_ref[0, at[k - 2], cut]
            term = dot(piece_refs[k - 2][...], weight)
            total = total + term + offsets[k] * gain_row(term, capacity)
        return total * scale

    every = slice(None)
    gate = product(weight_refs[2], sum_refs[2], gain_refs[2], every)
    lift = product(weight_refs[3], sum_refs[3], gain_refs[3], every)
    shared_ref[...] = (silu(gate) * lift * flag).astype(BF16)

    def chunk(i, _):
        cut = pl.ds(pl.multiple_of(i * step, step), step)
        gate = product(weight_refs[0], sum_refs[0], gain_refs[0], cut)
        lift = product(weight_refs[1], sum_refs[1], gain_refs[1], cut)
        hidden_ref[:, cut] = (silu(gate) * lift * share).astype(BF16)
        return 0

    lax.fori_loop(0, weight_refs[0].shape[2] // step, chunk, 0)
    for k in range(count - 1, -1, -1):
        cut = pl.ds(pl.multiple_of((place_ref[0] ^ k) * width, width), width)
        term = dot(hidden_ref[...], lower_ref[0, :, cut]) + dot(shared_ref[...], cl_ref[:, cut])
        if k == 0:
            own = own_ref[...].astype(F32)
            term = term + (own + offsets[0] * gain_row(own, capacity)) * (flag * scale * ALPHA)
        out_refs[k][...] = term.astype(out_refs[k].dtype)


def swap(array, axis, bit):
    size = lax.axis_size(axis)
    return lax.ppermute(array, axis, [(i, i ^ bit) for i in range(size)])


def scatter_sum(blocks, axis):
    bit = 1
    while len(blocks) > 1:
        kept = {}
        final = len(blocks) == 2
        for k in range(len(blocks) - 1, 0, -2):
            got = swap(blocks[k].astype(BF16), axis, bit)
            if final:
                return blocks[0].astype(F32), got
            kept[k // 2] = blocks[k - 1].astype(F32) + got.astype(F32)
        blocks = [kept[k] for k in range(len(blocks) // 2)]
        bit *= 2


def sum_all(array, axis):
    bit = 1
    while bit < lax.axis_size(axis):
        array = array + swap(array, axis, bit)
        bit *= 2
    return array


def gather_near(array, axis):
    return [array, swap(array, axis, 1)]


def gather_far(array, axis):
    size = lax.axis_size(axis)
    pieces = {0: array}
    bit = size // 2
    while bit:
        for k, piece in list(pieces.items()):
            if k ^ bit != 1:
                pieces[k ^ bit] = swap(piece, axis, bit)
        bit //= 2
    return [pieces[k] for k in range(2, size)]


def feature_norm(summed, gain):
    width = summed.shape[-1] * lax.axis_size("tp")
    sums = sum_all(jnp.stack([jnp.sum(summed, -1), jnp.sum(summed * summed, -1)]), "tp")
    row_mean = sums[0] / width
    row_var = sums[1] / width - row_mean * row_mean
    return (summed - row_mean[:, None]) * lax.rsqrt(row_var[:, None] + 1e-05) * gain


def call(kernel, outs, *args, in_specs=None, out_specs=None, limit=12, flops=4 * 10**9, **kw):
    shapes = [jax.ShapeDtypeStruct(shape, kind) for shape, kind in outs]
    moved = sum(array.size * array.dtype.itemsize for array in args)
    return pl.pallas_call(
        kernel,
        out_shape=shapes,
        in_specs=in_specs or [vmem()] * len(args),
        out_specs=out_specs or [vmem()] * len(outs),
        compiler_params=pltpu.CompilerParams(vmem_limit_bytes=limit * 1024 * 1024),
        cost_estimate=pl.CostEstimate(flops=flops, bytes_accessed=moved, transcendentals=0),
        **kw,
    )(*args)


def smem():
    return pl.BlockSpec(memory_space=pltpu.SMEM)


def vmem():
    return pl.BlockSpec(memory_space=pltpu.VMEM)


def shards(
    probe_vectors,
    address_vectors,
    content_vectors,
    storage_raw_signal,
    fade_raw_signal,
    channel_fade_exponent,
    extra_fade_amount,
    sequence_label,
    exit_valve_raw_signal,
    final_projection_matrix,
    incoming_rows_matrix,
    initial_rescale_factor,
    specialist_picks,
    picked_specialist_share,
    specialist_valve_matrix,
    specialist_raising_matrix,
    specialist_lowering_matrix,
    common_valve_matrix,
    common_raising_matrix,
    common_lowering_matrix,
    latter_rescale_factor,
):
    tokens, width = incoming_rows_matrix.shape
    heads = storage_raw_signal.shape[0]
    n_sp = lax.axis_size("sp")
    n_tp = lax.axis_size("tp")

    place = lax.axis_index("tp").astype(jnp.int32)[None]

    inputs = (
        probe_vectors,
        address_vectors,
        content_vectors,
        storage_raw_signal,
        fade_raw_signal,
        extra_fade_amount,
        channel_fade_exponent,
        sequence_label[None, :],
    )
    shapes = [((tokens, heads * DV), F32), ((tokens, heads * DK), F32)]

    def one_step(shape):
        return pl.BlockSpec(shape, lambda i: (0,) * len(shape))

    group = (lax.axis_index("sp").astype(jnp.int32) % heads)[None]
    *ms, local, query = call(
        delta_kernel,
        [((DK + DK + 16, DV), BF16)] * heads + shapes,
        group,
        *inputs,
        grid=(1,),
        in_specs=[smem()] + [one_step(array.shape) for array in inputs[:-2]] + [smem(), one_step(inputs[-1].shape)],
        out_specs=[one_step((DK + DK + 16, DV))] * heads + [one_step(shape) for shape, _ in shapes],
        limit=61,
        flops=2 * 10**9,
    )

    def exchange(blocks):
        moved = []
        for k in range(1, heads):
            moved.append(swap(blocks[k], "sp", k))
        return [blocks[0]] + moved

    _, *others = exchange(ms)
    own = call(
        hold_kernel,
        [((DK + DK + 16, DV), BF16)],
        ms[0],
        in_specs=[pl.BlockSpec(memory_space=pl.ANY)],
        scratch_shapes=[pltpu.SemaphoreType.DMA(())],
    )
    mine = list(own) + others
    states, maps, start, leaving, end = call(
        fold_kernel,
        [
            ((heads, DK, DV), F32),
            ((heads, DK, DK), BF16),
            ((16, DV), BF16),
            ((DK + 16, DV), BF16),
            ((DK + DK, DV), F32),
        ],
        group,
        *mine,
        in_specs=[smem()] + [vmem()] * heads,
        scratch_shapes=[pltpu.VMEM((heads, DK + DK + 16, DV), BF16)],
    )
    onward = [(i, i + heads) for i in range(n_sp - heads)]

    def hop(_, leaving):
        got = lax.ppermute(leaving, "sp", onward)
        return call(leave_kernel, [((DK + 16, DV), BF16)], got, start, leaving, end)[0]

    segments = n_sp // heads
    if segments > 2:
        leaving = lax.fori_loop(0, segments - 2, hop, leaving)
    got = lax.ppermute(leaving, "sp", onward)
    entering = exchange(
        call(
            enter_kernel,
            [((DK, DV), BF16)] * heads,
            group,
            got,
            start,
            states,
            maps,
            in_specs=[smem()] + [vmem()] * 4,
        ),
    )

    partial = call(
        project_kernel,
        [((tokens, width), BF16)] * n_tp,
        place,
        group,
        local,
        query,
        exit_valve_raw_signal,
        final_projection_matrix,
        *entering,
        in_specs=[smem()] * 2 + [vmem()] * (4 + heads),
        scratch_shapes=[pltpu.VMEM((tokens, heads * DV), BF16)],
    )
    keep, got = scatter_sum(partial, "tp")

    top = specialist_picks.shape[1]
    experts = specialist_valve_matrix.shape[0] * n_sp
    capacity = max(2, 9 * tokens * top // (8 * experts))
    slots = (capacity + 10) // 8 * 8
    total = experts * slots
    pick, share = call(
        functools.partial(route_kernel, capacity, slots),
        [((total, tokens), BF16), ((total, 1), F32)],
        lax.axis_index("sp").astype(jnp.int32)[None],
        specialist_picks.T,
        picked_specialist_share.T,
        in_specs=[smem()] + [vmem()] * 2,
    )
    fields = 8
    sent = call(
        functools.partial(pack_kernel, capacity, fields),
        [((slots, width), BF16)] * experts,
        keep,
        got,
        incoming_rows_matrix,
        initial_rescale_factor[None, :],
        pick,
        share,
    )

    def trade(blocks, ks):
        moved = []
        for k in ks:
            moved.append(swap(blocks[k], "sp", k) if k else blocks[k])
        return moved

    parts = [range(experts // 2, experts), range(experts // 2)]
    arrived = []
    for ks in parts:
        moved = trade(sent, ks)
        arrived.append(jnp.concatenate(moved, 0))
    hidden = specialist_valve_matrix.shape[2]
    shared = common_valve_matrix.shape[1]
    step = min(hidden, 256)
    weights = (specialist_valve_matrix, specialist_raising_matrix, common_valve_matrix, common_raising_matrix)
    work = 4 * total * width * (hidden + shared)
    height = total // len(parts)
    common = (step, slots, capacity, fields)
    back = {}
    for i, ks in enumerate(parts):
        far = gather_far(arrived[i], "tp")
        near = gather_near(arrived[i], "tp")
        partial = call(
            functools.partial(near_kernel, *common),
            [((height, hidden), F32)] * 2
            + [((height, shared), F32)] * 2
            + [((8, hidden), F32)] * 2
            + [((8, shared), F32)] * 2
            + [((height, 128), F32)] * 2,
            place,
            *near,
            *weights,
            in_specs=[smem()] + [vmem()] * 6,
            flops=work,
        )
        results = call(
            functools.partial(far_kernel, n_tp, *common),
            [((height, width), F32)] + [((height, width), BF16)] * (n_tp - 1),
            place,
            *far,
            *weights,
            *partial,
            arrived[i],
            specialist_lowering_matrix,
            common_lowering_matrix,
            in_specs=[smem()] + [vmem()] * (n_tp + 15),
            scratch_shapes=[pltpu.VMEM((height, hidden), BF16), pltpu.VMEM((height, shared), BF16)],
            flops=work * n_tp // 2,
        )
        keep, got = scatter_sum(results, "tp")
        blocks = (keep + got.astype(F32)).astype(BF16).reshape(len(ks), slots, width)
        back.update(zip(ks, trade({k: blocks[j] for j, k in enumerate(ks)}, ks)))
    returned = jnp.concatenate([back[k] for k in range(experts)], 0)
    second_sum = lax.dot_general(
        pick, returned, (((0,), (0,)), ((), ())), preferred_element_type=F32
    )
    return feature_norm(second_sum, latter_rescale_factor).astype(BF16)


def solution(mesh):
    placed = (
        P("sp", "tp"),
        P("sp", "tp"),
        P("sp", "tp"),
        P("tp", "sp"),
        P("tp", "sp"),
        P("tp"),
        P("tp", "sp"),
        P("sp"),
        P("sp", "tp"),
        P("tp", None),
        P("sp", "tp"),
        P("tp"),
        P("sp", None),
        P("sp", None),
        P("sp", None, "tp"),
        P("sp", None, "tp"),
        P("sp", "tp", None),
        P(None, "tp"),
        P(None, "tp"),
        P("tp", None),
        P("tp"),
    )

    return jax.shard_map(shards, mesh=mesh, in_specs=placed, out_specs=P("sp", "tp"), check_vma=False)
```

```python
import functools

import jax
import jax.numpy as jnp
from jax import lax
from jax.experimental import pallas as pl
from jax.experimental.pallas import tpu as pltpu
from jax.sharding import PartitionSpec as P


DK = 128
DV = 128
ALPHA = 2.0**0.25
F32 = jnp.float32
BF16 = jnp.bfloat16


def dot(left, right, contract=((1,), (0,))):
    return lax.dot_general(left, right, (contract, ((), ())), preferred_element_type=F32)


def split(array):
    high = array.astype(BF16)
    return high, (array - high.astype(F32)).astype(BF16)


def dot3(left, right):
    left_high, left_low = split(left)
    right_high, right_low = split(right)
    return dot(left_high, right_high) + (dot(left_high, right_low) + dot(left_low, right_high))


def dot_left(left, right):
    high, low = split(left)
    return dot(high, right) + dot(low, right)


def triangular_inverses(lowers, rows, cols):
    size = lowers[0].shape[0]
    identity = jnp.where(rows == cols, 1.0, 0.0)

    def once(left, right):
        return dot(left.astype(BF16), right.astype(BF16))

    def solve(powers, inverses, ratio, block):
        if block == 1:
            inverses = [x - p for p, x in zip(powers, inverses)]
            if ratio > 2:
                powers = [once(p, p) for p in powers]
        elif ratio > 2:
            both = [once(p, jnp.concatenate([p, x], 1)) for p, x in zip(powers, inverses)]
            powers = [pair[:, :size] for pair in both]
            inverses = [x - pair[:, size:] for pair, x in zip(both, inverses)]
        else:
            return [x - once(p, x) for p, x in zip(powers, inverses)]
        if ratio > 2:
            inverses = [x + once(p, x) for p, x in zip(powers, inverses)]
        return inverses

    inverses = [identity for _ in lowers]
    block = 1
    while block < size:
        ratio = min(4, size // block)
        wide = block * ratio
        inside = (rows // wide == cols // wide) & (rows // block != cols // block)
        parts = [jnp.where(inside, lower, 0.0) for lower in lowers]
        if block > 1:
            parts = [once(x, part) for x, part in zip(inverses, parts)]
        inverses = solve(parts, inverses, ratio, block)
        block = wide
    errors = [(identity - x) - dot3(lower, x) for lower, x in zip(lowers, inverses)]
    return [x + once(x, error) for x, error in zip(inverses, errors)]


def delta_kernel(*refs):
    place_ref, q_ref, k_ref, v_ref, store_ref, fade_ref, extra_ref, rate_ref, label_ref = refs[:9]
    ms_refs = refs[9:-2]
    local_ref, query_ref = refs[-2:]
    length = q_ref.shape[0]
    heads = store_ref.shape[0]
    every = range(heads)
    rows = lax.broadcasted_iota(jnp.int32, (length, length), 0)
    cols = lax.broadcasted_iota(jnp.int32, (length, length), 1)
    diagonal = rows == cols
    lower = rows >= cols
    strict = rows > cols
    identity = jnp.where(diagonal, 1.0, 0.0)

    def to_col(row):
        return jnp.sum(jnp.where(diagonal, row, 0.0), 1, keepdims=True)

    def to_row(col):
        return jnp.sum(jnp.where(diagonal, col, 0.0), 0, keepdims=True)

    label_row = label_ref[...].astype(F32)
    label_col = to_col(label_row)
    first = label_col[:1]
    last = label_col[length - 1 :]
    same = lower & (label_col == label_row)
    carried = jnp.where(label_col == first, 1.0, 0.0)
    closing = jnp.where(label_col == last, 1.0, 0.0)
    through = jnp.where(first == last, 1.0, 0.0)
    names = [place_ref[0] ^ k for k in every]
    at = [pl.ds(pl.multiple_of(name * DK, DK), DK) for name in names]
    queries = [q_ref[:, at[h]] for h in every]
    keys = [k_ref[:, at[h]] for h in every]
    values = [v_ref[:, at[h]] for h in every]
    row = [pl.ds(name, 1) for name in names]
    fades = [fade_ref[row[h], :] for h in every]
    softs = [jnp.maximum(fade, 0.0) + jnp.log(1.0 + jnp.exp(-jnp.abs(fade))) for fade in fades]
    rates = [jnp.exp(jnp.full((1, length), rate_ref[names[h]], F32)) for h in every]

    def scale_of(array):
        wide = array.astype(F32)
        return lax.rsqrt(jnp.sum(wide * wide, 1, keepdims=True) + 1e-06)

    key_scales = [scale_of(key) for key in keys]
    query_scales = [scale_of(query) * DK ** (-0.5) for query in queries]
    products = [dot(key, key, ((1,), (1,))) for key in keys]
    scores = [dot(query, key, ((1,), (1,))) for query, key in zip(queries, keys)]
    gate_rows = [1.0 / (1.0 + jnp.exp(-store_ref[row[h], :])) for h in every]
    gate_cols = [to_col(gate_rows[h]) for h in every]
    decays = [extra_ref[row[h], :] - rates[h] * softs[h] for h in every]
    totals = [jnp.sum(jnp.where(lower, decay, 0.0), 1, keepdims=True) for decay in decays]
    ends = [total[length - 1 :] for total in totals]
    reaches = [
        jnp.where(same, jnp.exp(jnp.where(lower, total - to_row(total), 0.0)), 0.0) for total in totals
    ]
    growths = [jnp.exp(total) * carried for total in totals]
    reaches = [reaches[h] * to_row(key_scales[h]) for h in every]
    couplings = [
        jnp.where(strict, products[h] * (key_scales[h] * gate_cols[h]) * reaches[h], 0.0) for h in every
    ]
    scores = [(scores[h] * query_scales[h] * reaches[h]).astype(BF16) for h in every]
    inverses = triangular_inverses(couplings, rows, cols)
    fresh = [dot_left(inverses[h] * gate_rows[h], values[h]) for h in every]
    erase = [
        dot_left(inverses[h] * to_row(gate_cols[h] * key_scales[h] * growths[h]), keys[h]) for h in every
    ]
    both = [jnp.concatenate([fresh[h], erase[h]], 1) for h in every]
    tails = [key_scales[h] * jnp.exp(ends[h] - totals[h]) * closing for h in every]
    carries = [dot(keys[h], (both[h] * tails[h]).astype(BF16), ((0,), (0,))) for h in every]
    seen = [dot(scores[h], both[h].astype(BF16)) for h in every]
    for h in every:
        final = jnp.exp(ends[h]) * through
        ms_refs[h][:DK] = (final * identity[:DK, :DK] - carries[h][:, DV:]).astype(BF16)
        ms_refs[h][DK : DK + DK] = carries[h][:, :DV].astype(BF16)
        ms_refs[h][DK + DK : DK + DK + 8] = jnp.broadcast_to(first, (8, DV)).astype(BF16)
        ms_refs[h][DK + DK + 8 :] = jnp.broadcast_to(last, (8, DV)).astype(BF16)
        local_ref[:, at[h]] = seen[h][:, :DV]
        query_ref[:, at[h]] = queries[h].astype(F32) * (query_scales[h] * growths[h]) - seen[h][:, DV:]


def first_label(ms_ref, j):
    return ms_ref[j, DK + DK : DK + DK + 8].astype(F32)[:1]


def last_label(ms_ref, j):
    return ms_ref[j, DK + DK + 8 :].astype(F32)[:1]


def hold_kernel(array_ref, out_ref, done_ref):
    copy = pltpu.make_async_copy(array_ref, out_ref, done_ref)
    copy.start()
    copy.wait()


def fold_kernel(place_ref, *refs):
    ms_refs = refs[:-6]
    state_ref, map_ref, start_ref, leaving_ref, end_ref, ms_ref = refs[-6:]
    blocks = len(ms_refs)
    for k in range(blocks):
        ms_ref[place_ref[0] ^ k] = ms_refs[k][...]
    state = jnp.zeros((DK, DV), F32)
    reach = jnp.where(
        lax.broadcasted_iota(jnp.int32, (DK, DK), 0) == lax.broadcasted_iota(jnp.int32, (DK, DK), 1), 1.0, 0.0
    )
    for j in range(blocks):
        if j:
            joined = jnp.where(first_label(ms_ref, j) == last_label(ms_ref, j - 1), 1.0, 0.0)
            state = state * joined
            reach = reach * joined
        onto = ms_ref[j, :DK]
        reach = reach.astype(BF16)
        state_ref[j] = state
        map_ref[j] = reach
        add = ms_ref[j, DK : DK + DK].astype(F32)
        if j:
            high, low = split(state)
            moved = dot(onto, jnp.concatenate([high, low, reach], 1))
            state = moved[:, :DV] + moved[:, DV : DV + DV] + add
            reach = moved[:, DV + DV :]
        else:
            state = add
            reach = onto.astype(F32)
    start_ref[...] = ms_ref[0, DK + DK :]
    leaving_ref[:DK] = state.astype(BF16)
    leaving_ref[DK:] = ms_ref[blocks - 1, DK + DK :]
    end_ref[:DK] = state
    end_ref[DK:] = reach


def arriving(got_ref, start_ref):
    last = got_ref[DK + 8 :].astype(F32)[:1]
    joined = jnp.where(start_ref[:8].astype(F32)[:1] == last, 1.0, 0.0)
    return (got_ref[:DK].astype(F32) * joined).astype(BF16)


def enter_kernel(place_ref, got_ref, start_ref, state_ref, map_ref, *entering_refs):
    state = arriving(got_ref, start_ref)
    for k, entering_ref in enumerate(entering_refs):
        j = place_ref[0] ^ k
        entering_ref[...] = (state_ref[j] + dot(map_ref[j], state)).astype(BF16)


def leave_kernel(got_ref, start_ref, leaving_ref, end_ref, out_ref):
    state = arriving(got_ref, start_ref)
    out_ref[:DK] = (end_ref[:DK] + dot(end_ref[DK:].astype(BF16), state)).astype(BF16)
    out_ref[DK:] = leaving_ref[DK:]


def project_kernel(place_ref, group_ref, local_ref, query_ref, valve_ref, weight_ref, *refs):
    heads = local_ref.shape[1] // DV
    state_refs, out_refs, heads_ref = refs[:heads], refs[heads:-1], refs[-1]
    for k in range(heads):
        at = pl.ds(pl.multiple_of((group_ref[0] ^ k) * DV, DV), DV)
        mixed = local_ref[:, at] + dot_left(query_ref[:, at], state_refs[k][...])
        scaled = mixed * lax.rsqrt(jnp.mean(mixed * mixed, 1, keepdims=True) + 1e-06)
        heads_ref[:, at] = (scaled * silu(valve_ref[:, at].astype(F32))).astype(BF16)
    width = out_refs[0].shape[1]
    for offset in range(len(out_refs) - 1, -1, -1):
        start = pl.multiple_of((place_ref[0] ^ offset) * width, width)
        out_refs[offset][...] = dot(heads_ref[...], weight_ref[:, pl.ds(start, width)]).astype(BF16)


def spread(fields, width):
    rows = lax.broadcasted_iota(jnp.int32, (128, width), 0)
    lanes = lax.broadcasted_iota(jnp.int32, (128, width), 1)
    return jnp.where(lanes // (width // fields) == rows, 1.0, 0.0).astype(BF16)


def own_lane(fields, slots, width):
    rows = lax.broadcasted_iota(jnp.int32, (slots, width), 0)
    lanes = lax.broadcasted_iota(jnp.int32, (slots, width), 1)
    return rows == lanes % (width // fields)


def route_kernel(capacity, slots, place_ref, named_ref, share_ref, pick_ref, note_ref):
    top, tokens = named_ref.shape
    experts = pick_ref.shape[0] // slots
    named, share = named_ref[...], share_ref[...].astype(F32)
    taken, signed = [], []
    for k in range(experts):
        hit = jnp.where(named == (place_ref[0] ^ k), 1.0, 0.0)
        taken.append(sum(hit[j : j + 1] for j in range(top)))
        signed.append(sum(hit[j : j + 1] * share[j : j + 1] * (1.0 if j else -1.0) for j in range(top)))
    before = lax.broadcasted_iota(jnp.int32, (tokens, tokens), 0)
    after = lax.broadcasted_iota(jnp.int32, (tokens, tokens), 1)
    earlier = jnp.where(before < after, 1.0, 0.0).astype(BF16)
    rank = dot(jnp.concatenate(taken, 0).astype(BF16), earlier)
    slot = lax.broadcasted_iota(jnp.int32, (slots, tokens), 0).astype(F32)
    for k in range(experts):
        chosen = jnp.where(rank[k : k + 1] == slot, taken[k], 0.0)
        chosen = jnp.where(slot < capacity, chosen, 0.0)
        here = slice(k * slots, (k + 1) * slots)
        pick_ref[here] = chosen.astype(BF16)
        note_ref[here] = jnp.sum(chosen * signed[k], 1, keepdims=True)


def pack_kernel(capacity, fields, keep_ref, got_ref, row_ref, gain_ref, pick_ref, share_ref, *out_refs):
    experts = len(out_refs)
    slots, width = out_refs[0].shape
    summed = ALPHA * row_ref[...].astype(F32) + (keep_ref[...] + got_ref[...].astype(F32))
    tokens = summed.shape[0]
    mean = jnp.mean(summed, 1, keepdims=True)
    centred = summed - mean
    squares = jnp.sum(centred * centred, 1, keepdims=True)
    gain = gain_ref[...]
    lane = lax.broadcasted_iota(jnp.int32, (tokens, 128), 1)
    notes = jnp.zeros((tokens, 128), F32)
    for value, places in ((mean, (1, 2, 3)), (squares, (4, 5))):
        for place in places:
            piece = value.astype(BF16).astype(F32)
            notes = jnp.where(lane == place, piece, notes)
            value = value - piece
    pick = pick_ref[...]
    body = dot(pick, (centred * gain).astype(BF16))
    notes = dot(pick, notes.astype(BF16))
    lane = lax.broadcasted_iota(jnp.int32, (experts * slots, 128), 1)
    notes = jnp.where(lane == 0, share_ref[...], notes).astype(BF16)
    notes = dot(notes, spread(fields, width))
    mine = own_lane(fields, slots, width)
    gain_high, gain_low = split(gain)
    rows = lax.broadcasted_iota(jnp.int32, (slots, width), 0)
    for e in range(experts):
        here = slice(e * slots, (e + 1) * slots)
        info = jnp.sum(jnp.where(mine, notes[here], 0.0), 0, keepdims=True)
        block = jnp.where(rows == capacity, info, body[here])
        block = jnp.where(rows == capacity + 1, gain_high.astype(F32), block)
        block = jnp.where(rows == capacity + 2, gain_low.astype(F32), block)
        out_refs[e][...] = block.astype(BF16)


def silu(array):
    return array / (1.0 + jnp.exp(-array))


def read_notes(piece_ref, capacity, slots, fields):
    width = piece_ref.shape[1]
    mine = own_lane(fields, slots, width)
    base = capacity // 8 * 8
    blocks = []
    for source in range(piece_ref.shape[0] // slots):
        info = piece_ref[source * slots + base : source * slots + base + 8, :].astype(F32)
        blocks.append(jnp.where(mine, info[capacity - base : capacity - base + 1], 0.0))
    return dot(jnp.concatenate(blocks, 0).astype(BF16), spread(fields, width), ((1,), (1,)))


def gain_row(array, capacity):
    return array[capacity + 1 : capacity + 2] + array[capacity + 2 : capacity + 3]


def near_kernel(step, slots, capacity, fields, *refs):
    place_ref, piece_refs = refs[0], refs[1:3]
    weight_refs, sum_refs, gain_refs, note_refs = refs[3:7], refs[7:11], refs[11:15], refs[15:17]
    width = piece_refs[0].shape[1]
    at = [pl.ds(pl.multiple_of((place_ref[0] ^ k) * width, width), width) for k in range(2)]

    def product(weight_ref, sum_ref, gain_ref, cut):
        total = None
        for k in range(2):
            weight = weight_ref[at[k], cut] if len(weight_ref.shape) == 2 else weight_ref[0, at[k], cut]
            term = dot(piece_refs[k][...], weight)
            gain_ref[k : k + 1, cut] = gain_row(term, capacity)
            total = term if total is None else total + term
        sum_ref[:, cut] = total

    for i in (2, 3):
        product(weight_refs[i], sum_refs[i], gain_refs[i], slice(None))

    def chunk(i, _):
        cut = pl.ds(pl.multiple_of(i * step, step), step)
        for j in (0, 1):
            product(weight_refs[j], sum_refs[j], gain_refs[j], cut)
        return 0

    lax.fori_loop(0, weight_refs[0].shape[2] // step, chunk, 0)
    for k in range(2):
        note_refs[k][...] = read_notes(piece_refs[k], capacity, slots, fields)


def far_kernel(count, step, slots, capacity, fields, *refs):
    place_ref, piece_refs = refs[0], refs[1 : count - 1]
    refs = refs[count - 1 :]
    weight_refs, sum_refs, gain_refs, note_refs = refs[:4], refs[4:8], refs[8:12], refs[12:14]
    lower_ref, cl_ref = refs[14:16]
    out_refs = refs[16 : 16 + count // 2]
    hidden_ref, shared_ref, row_ref = refs[16 + count // 2 :]
    height, width = piece_refs[0].shape
    at = [pl.ds(pl.multiple_of((place_ref[0] ^ k) * width, width), width) for k in range(2, count)]
    notes = [note_ref[...] for note_ref in note_refs]
    notes = notes + [read_notes(piece_ref, capacity, slots, fields) for piece_ref in piece_refs]
    means = [note[:, 1:2] + note[:, 2:3] + note[:, 3:4] for note in notes]
    mean = sum(means) / count
    offsets = [own_mean - mean for own_mean in means]
    squares = sum(note[:, 4:5] + note[:, 5:6] + width * offset * offset for note, offset in zip(notes, offsets))
    scale = lax.rsqrt(squares / (count * width) + 1e-05)
    share = notes[0][:, :1]
    flag = jnp.where(share < 0.0, 1.0, 0.0)
    share = jnp.abs(share)

    def product(weight_ref, sum_ref, gain_ref, cut):
        total = sum_ref[:, cut]
        for k in range(2):
            total = total + offsets[k] * gain_ref[k : k + 1, cut]
        for k in range(2, count):
            weight = weight_ref[at[k - 2], cut] if len(weight_ref.shape) == 2 else weight_ref[0, at[k - 2], cut]
            term = dot(piece_refs[k - 2][...], weight)
            total = total + term + offsets[k] * gain_row(term, capacity)
        return total * scale

    every = slice(None)
    gate = product(weight_refs[2], sum_refs[2], gain_refs[2], every)
    lift = product(weight_refs[3], sum_refs[3], gain_refs[3], every)
    shared_ref[...] = (silu(gate) * lift * flag).astype(BF16)

    def chunk(i, _):
        cut = pl.ds(pl.multiple_of(i * step, step), step)
        gate = product(weight_refs[0], sum_refs[0], gain_refs[0], cut)
        lift = product(weight_refs[1], sum_refs[1], gain_refs[1], cut)
        hidden_ref[:, cut] = (silu(gate) * lift * share).astype(BF16)
        return 0

    lax.fori_loop(0, weight_refs[0].shape[2] // step, chunk, 0)
    lane = lax.broadcasted_iota(jnp.int32, (height, 128), 1)
    row_ref[...] = jnp.where(lane == 0, offsets[0], flag * scale * ALPHA)
    for k in range(count - 1, 0, -2):
        out_refs[k // 2][...] = lowered(place_ref, k, width, hidden_ref, shared_ref, lower_ref, cl_ref).astype(BF16)


def lowered(place_ref, k, width, hidden_ref, shared_ref, lower_ref, cl_ref):
    cut = pl.ds(pl.multiple_of((place_ref[0] ^ k) * width, width), width)
    return dot(hidden_ref[...], lower_ref[0, :, cut]) + dot(shared_ref[...], cl_ref[:, cut])


def tail_kernel(capacity, place_ref, own_ref, hidden_ref, shared_ref, row_ref, lower_ref, cl_ref, *out_refs):
    width = own_ref.shape[1]
    for k in range(2 * len(out_refs) - 2, -1, -2):
        term = lowered(place_ref, k, width, hidden_ref, shared_ref, lower_ref, cl_ref)
        if k == 0:
            own = own_ref[...].astype(F32)
            term = term + (own + row_ref[:, :1] * gain_row(own, capacity)) * row_ref[:, 1:2]
        out_refs[k // 2][...] = term.astype(out_refs[k // 2].dtype)


def swap(array, axis, bit):
    size = lax.axis_size(axis)
    return lax.ppermute(array, axis, [(i, i ^ bit) for i in range(size)])


def scatter_sum(blocks, axis):
    bit = 1
    while len(blocks) > 1:
        kept = {}
        final = len(blocks) == 2
        for k in range(len(blocks) - 1, 0, -2):
            got = swap(blocks[k].astype(BF16), axis, bit)
            if final:
                return blocks[0].astype(F32), got
            kept[k // 2] = blocks[k - 1].astype(F32) + got.astype(F32)
        blocks = [kept[k] for k in range(len(blocks) // 2)]
        bit *= 2


def sum_all(array, axis):
    bit = 1
    while bit < lax.axis_size(axis):
        array = array + swap(array, axis, bit)
        bit *= 2
    return array


def gather_near(array, axis):
    return [array, swap(array, axis, 1)]


def gather_far(array, axis):
    size = lax.axis_size(axis)
    pieces = {0: array}
    bit = size // 2
    while bit:
        for k, piece in list(pieces.items()):
            if k ^ bit != 1:
                pieces[k ^ bit] = swap(piece, axis, bit)
        bit //= 2
    return [pieces[k] for k in range(2, size)]


def feature_norm(summed, gain):
    width = summed.shape[-1] * lax.axis_size("tp")
    sums = sum_all(jnp.stack([jnp.sum(summed, -1), jnp.sum(summed * summed, -1)]), "tp")
    row_mean = sums[0] / width
    row_var = sums[1] / width - row_mean * row_mean
    return (summed - row_mean[:, None]) * lax.rsqrt(row_var[:, None] + 1e-05) * gain


def call(kernel, outs, *args, in_specs=None, out_specs=None, limit=12, flops=4 * 10**9, **kw):
    shapes = [jax.ShapeDtypeStruct(shape, kind) for shape, kind in outs]
    moved = sum(array.size * array.dtype.itemsize for array in args)
    return pl.pallas_call(
        kernel,
        out_shape=shapes,
        in_specs=in_specs or [vmem()] * len(args),
        out_specs=out_specs or [vmem()] * len(outs),
        compiler_params=pltpu.CompilerParams(vmem_limit_bytes=limit * 1024 * 1024),
        cost_estimate=pl.CostEstimate(flops=flops, bytes_accessed=moved, transcendentals=0),
        **kw,
    )(*args)


def smem():
    return pl.BlockSpec(memory_space=pltpu.SMEM)


def vmem():
    return pl.BlockSpec(memory_space=pltpu.VMEM)


def shards(
    probe_vectors,
    address_vectors,
    content_vectors,
    storage_raw_signal,
    fade_raw_signal,
    channel_fade_exponent,
    extra_fade_amount,
    sequence_label,
    exit_valve_raw_signal,
    final_projection_matrix,
    incoming_rows_matrix,
    initial_rescale_factor,
    specialist_picks,
    picked_specialist_share,
    specialist_valve_matrix,
    specialist_raising_matrix,
    specialist_lowering_matrix,
    common_valve_matrix,
    common_raising_matrix,
    common_lowering_matrix,
    latter_rescale_factor,
):
    tokens, width = incoming_rows_matrix.shape
    heads = storage_raw_signal.shape[0]
    n_sp = lax.axis_size("sp")
    n_tp = lax.axis_size("tp")

    place = lax.axis_index("tp").astype(jnp.int32)[None]

    inputs = (
        probe_vectors,
        address_vectors,
        content_vectors,
        storage_raw_signal,
        fade_raw_signal,
        extra_fade_amount,
        channel_fade_exponent,
        sequence_label[None, :],
    )
    shapes = [((tokens, heads * DV), F32), ((tokens, heads * DK), F32)]

    def one_step(shape):
        return pl.BlockSpec(shape, lambda i: (0,) * len(shape))

    group = (lax.axis_index("sp").astype(jnp.int32) % heads)[None]
    *ms, local, query = call(
        delta_kernel,
        [((DK + DK + 16, DV), BF16)] * heads + shapes,
        group,
        *inputs,
        grid=(1,),
        in_specs=[smem()] + [one_step(array.shape) for array in inputs[:-2]] + [smem(), one_step(inputs[-1].shape)],
        out_specs=[one_step((DK + DK + 16, DV))] * heads + [one_step(shape) for shape, _ in shapes],
        limit=61,
        flops=2 * 10**9,
    )

    def exchange(blocks):
        moved = []
        for k in range(1, heads):
            moved.append(swap(blocks[k], "sp", k))
        return [blocks[0]] + moved

    _, *others = exchange(ms)
    own = call(
        hold_kernel,
        [((DK + DK + 16, DV), BF16)],
        ms[0],
        in_specs=[pl.BlockSpec(memory_space=pl.ANY)],
        scratch_shapes=[pltpu.SemaphoreType.DMA(())],
    )
    mine = list(own) + others
    states, maps, start, leaving, end = call(
        fold_kernel,
        [
            ((heads, DK, DV), F32),
            ((heads, DK, DK), BF16),
            ((16, DV), BF16),
            ((DK + 16, DV), BF16),
            ((DK + DK, DV), F32),
        ],
        group,
        *mine,
        in_specs=[smem()] + [vmem()] * heads,
        scratch_shapes=[pltpu.VMEM((heads, DK + DK + 16, DV), BF16)],
    )
    onward = [(i, i + heads) for i in range(n_sp - heads)]

    def hop(_, leaving):
        got = lax.ppermute(leaving, "sp", onward)
        return call(leave_kernel, [((DK + 16, DV), BF16)], got, start, leaving, end)[0]

    segments = n_sp // heads
    if segments > 2:
        leaving = lax.fori_loop(0, segments - 2, hop, leaving)
    got = lax.ppermute(leaving, "sp", onward)
    entering = exchange(
        call(
            enter_kernel,
            [((DK, DV), BF16)] * heads,
            group,
            got,
            start,
            states,
            maps,
            in_specs=[smem()] + [vmem()] * 4,
        ),
    )

    partial = call(
        project_kernel,
        [((tokens, width), BF16)] * n_tp,
        place,
        group,
        local,
        query,
        exit_valve_raw_signal,
        final_projection_matrix,
        *entering,
        in_specs=[smem()] * 2 + [vmem()] * (4 + heads),
        scratch_shapes=[pltpu.VMEM((tokens, heads * DV), BF16)],
    )
    keep, got = scatter_sum(partial, "tp")

    top = specialist_picks.shape[1]
    experts = specialist_valve_matrix.shape[0] * n_sp
    capacity = max(2, 9 * tokens * top // (8 * experts))
    slots = (capacity + 10) // 8 * 8
    total = experts * slots
    pick, share = call(
        functools.partial(route_kernel, capacity, slots),
        [((total, tokens), BF16), ((total, 1), F32)],
        lax.axis_index("sp").astype(jnp.int32)[None],
        specialist_picks.T,
        picked_specialist_share.T,
        in_specs=[smem()] + [vmem()] * 2,
    )
    fields = 8
    sent = call(
        functools.partial(pack_kernel, capacity, fields),
        [((slots, width), BF16)] * experts,
        keep,
        got,
        incoming_rows_matrix,
        initial_rescale_factor[None, :],
        pick,
        share,
    )

    def trade(blocks, ks):
        moved = []
        for k in ks:
            moved.append(swap(blocks[k], "sp", k) if k else blocks[k])
        return moved

    parts = [range(experts // 2, experts), range(experts // 2)]
    arrived = []
    for ks in parts:
        moved = trade(sent, ks)
        arrived.append(jnp.concatenate(moved, 0))
    hidden = specialist_valve_matrix.shape[2]
    shared = common_valve_matrix.shape[1]
    step = min(hidden, 256)
    weights = (specialist_valve_matrix, specialist_raising_matrix, common_valve_matrix, common_raising_matrix)
    work = 4 * total * width * (hidden + shared)
    height = total // len(parts)
    common = (step, slots, capacity, fields)
    back = {}
    for i, ks in enumerate(parts):
        far = gather_far(arrived[i], "tp")
        near = gather_near(arrived[i], "tp")
        partial = call(
            functools.partial(near_kernel, *common),
            [((height, hidden), F32)] * 2
            + [((height, shared), F32)] * 2
            + [((8, hidden), F32)] * 2
            + [((8, shared), F32)] * 2
            + [((height, 128), F32)] * 2,
            place,
            *near,
            *weights,
            in_specs=[smem()] + [vmem()] * 6,
            flops=work,
        )
        lowering = (specialist_lowering_matrix, common_lowering_matrix)
        *sends, inner, outer, notes = call(
            functools.partial(far_kernel, n_tp, *common),
            [((height, width), BF16)] * (n_tp // 2)
            + [((height, hidden), BF16), ((height, shared), BF16), ((height, 128), F32)],
            place,
            *far,
            *weights,
            *partial,
            *lowering,
            in_specs=[smem()] + [vmem()] * (n_tp + 14),
            flops=work * n_tp // 2,
        )
        keeps = call(
            functools.partial(tail_kernel, capacity),
            [((height, width), F32)] + [((height, width), BF16)] * (n_tp // 2 - 1),
            place,
            arrived[i],
            inner,
            outer,
            notes,
            *lowering,
            in_specs=[smem()] + [vmem()] * 6,
            flops=work // 2,
        )
        results = [(sends if k % 2 else keeps)[k // 2] for k in range(n_tp)]
        keep, got = scatter_sum(results, "tp")
        blocks = (keep + got.astype(F32)).astype(BF16).reshape(len(ks), slots, width)
        back.update(zip(ks, trade({k: blocks[j] for j, k in enumerate(ks)}, ks)))
    returned = jnp.concatenate([back[k] for k in range(experts)], 0)
    second_sum = lax.dot_general(
        pick, returned, (((0,), (0,)), ((), ())), preferred_element_type=F32
    )
    return feature_norm(second_sum, latter_rescale_factor).astype(BF16)


def solution(mesh):
    placed = (
        P("sp", "tp"),
        P("sp", "tp"),
        P("sp", "tp"),
        P("tp", "sp"),
        P("tp", "sp"),
        P("tp"),
        P("tp", "sp"),
        P("sp"),
        P("sp", "tp"),
        P("tp", None),
        P("sp", "tp"),
        P("tp"),
        P("sp", None),
        P("sp", None),
        P("sp", None, "tp"),
        P("sp", None, "tp"),
        P("sp", "tp", None),
        P(None, "tp"),
        P(None, "tp"),
        P("tp", None),
        P("tp"),
    )

    return jax.shard_map(shards, mesh=mesh, in_specs=placed, out_specs=P("sp", "tp"), check_vma=False)
```

```python
import functools

import jax
import jax.numpy as jnp
from jax import lax
from jax.experimental import pallas as pl
from jax.experimental.pallas import tpu as pltpu
from jax.sharding import PartitionSpec as P


DK = 128
DV = 128
ALPHA = 2.0**0.25
F32 = jnp.float32
BF16 = jnp.bfloat16


def dot(left, right, contract=((1,), (0,))):
    return lax.dot_general(left, right, (contract, ((), ())), preferred_element_type=F32)


def split(array):
    high = array.astype(BF16)
    return high, (array - high.astype(F32)).astype(BF16)


def dot3(left, right):
    left_high, left_low = split(left)
    right_high, right_low = split(right)
    return dot(left_high, right_high) + (dot(left_high, right_low) + dot(left_low, right_high))


def dot_left(left, right):
    high, low = split(left)
    return dot(high, right) + dot(low, right)


def triangular_inverses(lowers, rows, cols):
    size = lowers[0].shape[0]
    identity = jnp.where(rows == cols, 1.0, 0.0)

    def once(left, right):
        return dot(left.astype(BF16), right.astype(BF16))

    def solve(powers, inverses, ratio, block):
        if block == 1:
            inverses = [x - p for p, x in zip(powers, inverses)]
            if ratio > 2:
                powers = [once(p, p) for p in powers]
        elif ratio > 2:
            both = [once(p, jnp.concatenate([p, x], 1)) for p, x in zip(powers, inverses)]
            powers = [pair[:, :size] for pair in both]
            inverses = [x - pair[:, size:] for pair, x in zip(both, inverses)]
        else:
            return [x - once(p, x) for p, x in zip(powers, inverses)]
        if ratio > 2:
            inverses = [x + once(p, x) for p, x in zip(powers, inverses)]
        return inverses

    inverses = [identity for _ in lowers]
    block = 1
    while block < size:
        ratio = min(4, size // block)
        wide = block * ratio
        inside = (rows // wide == cols // wide) & (rows // block != cols // block)
        parts = [jnp.where(inside, lower, 0.0) for lower in lowers]
        if block > 1:
            parts = [once(x, part) for x, part in zip(inverses, parts)]
        inverses = solve(parts, inverses, ratio, block)
        block = wide
    errors = [(identity - x) - dot3(lower, x) for lower, x in zip(lowers, inverses)]
    return [x + once(x, error) for x, error in zip(inverses, errors)]


def delta_kernel(*refs):
    place_ref, q_ref, k_ref, v_ref, store_ref, fade_ref, extra_ref, rate_ref, label_ref = refs[:9]
    ms_refs = refs[9:-2]
    local_ref, query_ref = refs[-2:]
    length = q_ref.shape[0]
    heads = store_ref.shape[0]
    every = range(heads)
    rows = lax.broadcasted_iota(jnp.int32, (length, length), 0)
    cols = lax.broadcasted_iota(jnp.int32, (length, length), 1)
    diagonal = rows == cols
    lower = rows >= cols
    strict = rows > cols
    identity = jnp.where(diagonal, 1.0, 0.0)

    def to_col(row):
        return jnp.sum(jnp.where(diagonal, row, 0.0), 1, keepdims=True)

    def to_row(col):
        return jnp.sum(jnp.where(diagonal, col, 0.0), 0, keepdims=True)

    label_row = label_ref[...].astype(F32)
    label_col = to_col(label_row)
    first = label_col[:1]
    last = label_col[length - 1 :]
    same = lower & (label_col == label_row)
    carried = jnp.where(label_col == first, 1.0, 0.0)
    closing = jnp.where(label_col == last, 1.0, 0.0)
    through = jnp.where(first == last, 1.0, 0.0)
    names = [place_ref[0] ^ k for k in every]
    at = [pl.ds(pl.multiple_of(name * DK, DK), DK) for name in names]
    queries = [q_ref[:, at[h]] for h in every]
    keys = [k_ref[:, at[h]] for h in every]
    values = [v_ref[:, at[h]] for h in every]
    row = [pl.ds(name, 1) for name in names]
    fades = [fade_ref[row[h], :] for h in every]
    softs = [jnp.maximum(fade, 0.0) + jnp.log(1.0 + jnp.exp(-jnp.abs(fade))) for fade in fades]
    rates = [jnp.exp(jnp.full((1, length), rate_ref[names[h]], F32)) for h in every]

    def scale_of(array):
        wide = array.astype(F32)
        return lax.rsqrt(jnp.sum(wide * wide, 1, keepdims=True) + 1e-06)

    key_scales = [scale_of(key) for key in keys]
    query_scales = [scale_of(query) * DK ** (-0.5) for query in queries]
    products = [dot(key, key, ((1,), (1,))) for key in keys]
    scores = [dot(query, key, ((1,), (1,))) for query, key in zip(queries, keys)]
    gate_rows = [1.0 / (1.0 + jnp.exp(-store_ref[row[h], :])) for h in every]
    gate_cols = [to_col(gate_rows[h]) for h in every]
    decays = [extra_ref[row[h], :] - rates[h] * softs[h] for h in every]
    totals = [jnp.sum(jnp.where(lower, decay, 0.0), 1, keepdims=True) for decay in decays]
    ends = [total[length - 1 :] for total in totals]
    reaches = [
        jnp.where(same, jnp.exp(jnp.where(lower, total - to_row(total), 0.0)), 0.0) for total in totals
    ]
    growths = [jnp.exp(total) * carried for total in totals]
    reaches = [reaches[h] * to_row(key_scales[h]) for h in every]
    couplings = [
        jnp.where(strict, products[h] * (key_scales[h] * gate_cols[h]) * reaches[h], 0.0) for h in every
    ]
    scores = [(scores[h] * query_scales[h] * reaches[h]).astype(BF16) for h in every]
    inverses = triangular_inverses(couplings, rows, cols)
    fresh = [dot_left(inverses[h] * gate_rows[h], values[h]) for h in every]
    erase = [
        dot_left(inverses[h] * to_row(gate_cols[h] * key_scales[h] * growths[h]), keys[h]) for h in every
    ]
    both = [jnp.concatenate([fresh[h], erase[h]], 1) for h in every]
    tails = [key_scales[h] * jnp.exp(ends[h] - totals[h]) * closing for h in every]
    carries = [dot(keys[h], (both[h] * tails[h]).astype(BF16), ((0,), (0,))) for h in every]
    seen = [dot(scores[h], both[h].astype(BF16)) for h in every]
    for h in every:
        final = jnp.exp(ends[h]) * through
        ms_refs[h][:DK] = (final * identity[:DK, :DK] - carries[h][:, DV:]).astype(BF16)
        ms_refs[h][DK : DK + DK] = carries[h][:, :DV].astype(BF16)
        ms_refs[h][DK + DK : DK + DK + 8] = jnp.broadcast_to(first, (8, DV)).astype(BF16)
        ms_refs[h][DK + DK + 8 :] = jnp.broadcast_to(last, (8, DV)).astype(BF16)
        local_ref[:, at[h]] = seen[h][:, :DV]
        query_ref[:, at[h]] = queries[h].astype(F32) * (query_scales[h] * growths[h]) - seen[h][:, DV:]


def first_label(ms_ref, j):
    return ms_ref[j, DK + DK : DK + DK + 8].astype(F32)[:1]


def last_label(ms_ref, j):
    return ms_ref[j, DK + DK + 8 :].astype(F32)[:1]


def hold_kernel(array_ref, out_ref, done_ref):
    copy = pltpu.make_async_copy(array_ref, out_ref, done_ref)
    copy.start()
    copy.wait()


def fold_kernel(place_ref, *refs):
    ms_refs = refs[:-6]
    state_ref, map_ref, start_ref, leaving_ref, end_ref, ms_ref = refs[-6:]
    blocks = len(ms_refs)
    for k in range(blocks):
        ms_ref[place_ref[0] ^ k] = ms_refs[k][...]
    state = jnp.zeros((DK, DV), F32)
    reach = jnp.where(
        lax.broadcasted_iota(jnp.int32, (DK, DK), 0) == lax.broadcasted_iota(jnp.int32, (DK, DK), 1), 1.0, 0.0
    )
    for j in range(blocks):
        if j:
            joined = jnp.where(first_label(ms_ref, j) == last_label(ms_ref, j - 1), 1.0, 0.0)
            state = state * joined
            reach = reach * joined
        onto = ms_ref[j, :DK]
        reach = reach.astype(BF16)
        state_ref[j] = state
        map_ref[j] = reach
        add = ms_ref[j, DK : DK + DK].astype(F32)
        if j:
            high, low = split(state)
            moved = dot(onto, jnp.concatenate([high, low, reach], 1))
            state = moved[:, :DV] + moved[:, DV : DV + DV] + add
            reach = moved[:, DV + DV :]
        else:
            state = add
            reach = onto.astype(F32)
    start_ref[...] = ms_ref[0, DK + DK :]
    leaving_ref[:DK] = state.astype(BF16)
    leaving_ref[DK:] = ms_ref[blocks - 1, DK + DK :]
    end_ref[:DK] = state
    end_ref[DK:] = reach


def arriving(got_ref, start_ref):
    last = got_ref[DK + 8 :].astype(F32)[:1]
    joined = jnp.where(start_ref[:8].astype(F32)[:1] == last, 1.0, 0.0)
    return (got_ref[:DK].astype(F32) * joined).astype(BF16)


def enter_kernel(place_ref, got_ref, start_ref, state_ref, map_ref, *entering_refs):
    state = arriving(got_ref, start_ref)
    for k, entering_ref in enumerate(entering_refs):
        j = place_ref[0] ^ k
        entering_ref[...] = (state_ref[j] + dot(map_ref[j], state)).astype(BF16)


def leave_kernel(got_ref, start_ref, leaving_ref, end_ref, out_ref):
    state = arriving(got_ref, start_ref)
    out_ref[:DK] = (end_ref[:DK] + dot(end_ref[DK:].astype(BF16), state)).astype(BF16)
    out_ref[DK:] = leaving_ref[DK:]


def project_kernel(place_ref, group_ref, local_ref, query_ref, valve_ref, weight_ref, *refs):
    heads = local_ref.shape[1] // DV
    state_refs, heads_ref, out_refs = refs[:heads], refs[heads], refs[heads + 1 :]
    for k in range(heads):
        at = pl.ds(pl.multiple_of((group_ref[0] ^ k) * DV, DV), DV)
        mixed = local_ref[:, at] + dot_left(query_ref[:, at], state_refs[k][...])
        scaled = mixed * lax.rsqrt(jnp.mean(mixed * mixed, 1, keepdims=True) + 1e-06)
        heads_ref[:, at] = (scaled * silu(valve_ref[:, at].astype(F32))).astype(BF16)
    project_blocks(1, place_ref, heads_ref, weight_ref, *out_refs)


def project_blocks(odd, place_ref, heads_ref, weight_ref, *out_refs):
    width = out_refs[0].shape[1]
    for i in range(len(out_refs) - 1, -1, -1):
        start = pl.multiple_of((place_ref[0] ^ (2 * i + odd)) * width, width)
        out_refs[i][...] = dot(heads_ref[...], weight_ref[:, pl.ds(start, width)]).astype(out_refs[i].dtype)


def spread(fields, width):
    rows = lax.broadcasted_iota(jnp.int32, (128, width), 0)
    lanes = lax.broadcasted_iota(jnp.int32, (128, width), 1)
    return jnp.where(lanes // (width // fields) == rows, 1.0, 0.0).astype(BF16)


def own_lane(fields, slots, width):
    rows = lax.broadcasted_iota(jnp.int32, (slots, width), 0)
    lanes = lax.broadcasted_iota(jnp.int32, (slots, width), 1)
    return rows == lanes % (width // fields)


def route_kernel(capacity, slots, place_ref, named_ref, share_ref, pick_ref, note_ref):
    top, tokens = named_ref.shape
    experts = pick_ref.shape[0] // slots
    named, share = named_ref[...], share_ref[...].astype(F32)
    taken, signed = [], []
    for k in range(experts):
        hit = jnp.where(named == (place_ref[0] ^ k), 1.0, 0.0)
        taken.append(sum(hit[j : j + 1] for j in range(top)))
        signed.append(sum(hit[j : j + 1] * share[j : j + 1] * (1.0 if j else -1.0) for j in range(top)))
    before = lax.broadcasted_iota(jnp.int32, (tokens, tokens), 0)
    after = lax.broadcasted_iota(jnp.int32, (tokens, tokens), 1)
    earlier = jnp.where(before < after, 1.0, 0.0).astype(BF16)
    rank = dot(jnp.concatenate(taken, 0).astype(BF16), earlier)
    slot = lax.broadcasted_iota(jnp.int32, (slots, tokens), 0).astype(F32)
    for k in range(experts):
        chosen = jnp.where(rank[k : k + 1] == slot, taken[k], 0.0)
        chosen = jnp.where(slot < capacity, chosen, 0.0)
        here = slice(k * slots, (k + 1) * slots)
        pick_ref[here] = chosen.astype(BF16)
        note_ref[here] = jnp.sum(chosen * signed[k], 1, keepdims=True)


def pack_kernel(capacity, fields, keep_ref, got_ref, row_ref, gain_ref, pick_ref, share_ref, *out_refs):
    experts = len(out_refs)
    slots, width = out_refs[0].shape
    summed = ALPHA * row_ref[...].astype(F32) + (keep_ref[...] + got_ref[...].astype(F32))
    tokens = summed.shape[0]
    mean = jnp.mean(summed, 1, keepdims=True)
    centred = summed - mean
    squares = jnp.sum(centred * centred, 1, keepdims=True)
    gain = gain_ref[...]
    lane = lax.broadcasted_iota(jnp.int32, (tokens, 128), 1)
    notes = jnp.zeros((tokens, 128), F32)
    for value, places in ((mean, (1, 2, 3)), (squares, (4, 5))):
        for place in places:
            piece = value.astype(BF16).astype(F32)
            notes = jnp.where(lane == place, piece, notes)
            value = value - piece
    pick = pick_ref[...]
    body = dot(pick, (centred * gain).astype(BF16))
    notes = dot(pick, notes.astype(BF16))
    lane = lax.broadcasted_iota(jnp.int32, (experts * slots, 128), 1)
    notes = jnp.where(lane == 0, share_ref[...], notes).astype(BF16)
    notes = dot(notes, spread(fields, width))
    mine = own_lane(fields, slots, width)
    gain_high, gain_low = split(gain)
    rows = lax.broadcasted_iota(jnp.int32, (slots, width), 0)
    for e in range(experts):
        here = slice(e * slots, (e + 1) * slots)
        info = jnp.sum(jnp.where(mine, notes[here], 0.0), 0, keepdims=True)
        block = jnp.where(rows == capacity, info, body[here])
        block = jnp.where(rows == capacity + 1, gain_high.astype(F32), block)
        block = jnp.where(rows == capacity + 2, gain_low.astype(F32), block)
        out_refs[e][...] = block.astype(BF16)


def silu(array):
    return array / (1.0 + jnp.exp(-array))


def read_notes(piece_ref, capacity, slots, fields):
    width = piece_ref.shape[1]
    mine = own_lane(fields, slots, width)
    base = capacity // 8 * 8
    blocks = []
    for source in range(piece_ref.shape[0] // slots):
        info = piece_ref[source * slots + base : source * slots + base + 8, :].astype(F32)
        blocks.append(jnp.where(mine, info[capacity - base : capacity - base + 1], 0.0))
    return dot(jnp.concatenate(blocks, 0).astype(BF16), spread(fields, width), ((1,), (1,)))


def gain_row(array, capacity):
    return array[capacity + 1 : capacity + 2] + array[capacity + 2 : capacity + 3]


def near_kernel(step, slots, capacity, fields, *refs):
    place_ref, piece_refs = refs[0], refs[1:3]
    weight_refs, sum_refs, gain_refs, note_refs = refs[3:7], refs[7:11], refs[11:15], refs[15:17]
    width = piece_refs[0].shape[1]
    at = [pl.ds(pl.multiple_of((place_ref[0] ^ k) * width, width), width) for k in range(2)]

    def product(weight_ref, sum_ref, gain_ref, cut):
        total = None
        for k in range(2):
            weight = weight_ref[at[k], cut] if len(weight_ref.shape) == 2 else weight_ref[0, at[k], cut]
            term = dot(piece_refs[k][...], weight)
            gain_ref[k : k + 1, cut] = gain_row(term, capacity)
            total = term if total is None else total + term
        sum_ref[:, cut] = total

    for i in (2, 3):
        product(weight_refs[i], sum_refs[i], gain_refs[i], slice(None))

    def chunk(i, _):
        cut = pl.ds(pl.multiple_of(i * step, step), step)
        for j in (0, 1):
            product(weight_refs[j], sum_refs[j], gain_refs[j], cut)
        return 0

    lax.fori_loop(0, weight_refs[0].shape[2] // step, chunk, 0)
    for k in range(2):
        note_refs[k][...] = read_notes(piece_refs[k], capacity, slots, fields)


def far_kernel(count, step, slots, capacity, fields, *refs):
    place_ref, piece_refs = refs[0], refs[1 : count - 1]
    refs = refs[count - 1 :]
    weight_refs, sum_refs, gain_refs, note_refs = refs[:4], refs[4:8], refs[8:12], refs[12:14]
    lower_ref, cl_ref = refs[14:16]
    out_refs = refs[16 : 16 + count // 2]
    hidden_ref, shared_ref, row_ref = refs[16 + count // 2 :]
    height, width = piece_refs[0].shape
    at = [pl.ds(pl.multiple_of((place_ref[0] ^ k) * width, width), width) for k in range(2, count)]
    notes = [note_ref[...] for note_ref in note_refs]
    notes = notes + [read_notes(piece_ref, capacity, slots, fields) for piece_ref in piece_refs]
    means = [note[:, 1:2] + note[:, 2:3] + note[:, 3:4] for note in notes]
    mean = sum(means) / count
    offsets = [own_mean - mean for own_mean in means]
    squares = sum(note[:, 4:5] + note[:, 5:6] + width * offset * offset for note, offset in zip(notes, offsets))
    scale = lax.rsqrt(squares / (count * width) + 1e-05)
    share = notes[0][:, :1]
    flag = jnp.where(share < 0.0, 1.0, 0.0)
    share = jnp.abs(share)

    def product(weight_ref, sum_ref, gain_ref, cut):
        total = sum_ref[:, cut]
        for k in range(2):
            total = total + offsets[k] * gain_ref[k : k + 1, cut]
        for k in range(2, count):
            weight = weight_ref[at[k - 2], cut] if len(weight_ref.shape) == 2 else weight_ref[0, at[k - 2], cut]
            term = dot(piece_refs[k - 2][...], weight)
            total = total + term + offsets[k] * gain_row(term, capacity)
        return total * scale

    every = slice(None)
    gate = product(weight_refs[2], sum_refs[2], gain_refs[2], every)
    lift = product(weight_refs[3], sum_refs[3], gain_refs[3], every)
    shared_ref[...] = (silu(gate) * lift * flag).astype(BF16)

    def chunk(i, _):
        cut = pl.ds(pl.multiple_of(i * step, step), step)
        gate = product(weight_refs[0], sum_refs[0], gain_refs[0], cut)
        lift = product(weight_refs[1], sum_refs[1], gain_refs[1], cut)
        hidden_ref[:, cut] = (silu(gate) * lift * share).astype(BF16)
        return 0

    lax.fori_loop(0, weight_refs[0].shape[2] // step, chunk, 0)
    lane = lax.broadcasted_iota(jnp.int32, (height, 128), 1)
    row_ref[...] = jnp.where(lane == 0, offsets[0], flag * scale * ALPHA)
    for k in range(count - 1, 0, -2):
        out_refs[k // 2][...] = lowered(place_ref, k, width, hidden_ref, shared_ref, lower_ref, cl_ref).astype(BF16)


def lowered(place_ref, k, width, hidden_ref, shared_ref, lower_ref, cl_ref):
    cut = pl.ds(pl.multiple_of((place_ref[0] ^ k) * width, width), width)
    return dot(hidden_ref[...], lower_ref[0, :, cut]) + dot(shared_ref[...], cl_ref[:, cut])


def tail_kernel(capacity, place_ref, own_ref, hidden_ref, shared_ref, row_ref, lower_ref, cl_ref, *out_refs):
    width = own_ref.shape[1]
    for k in range(2 * len(out_refs) - 2, -1, -2):
        term = lowered(place_ref, k, width, hidden_ref, shared_ref, lower_ref, cl_ref)
        if k == 0:
            own = own_ref[...].astype(F32)
            term = term + (own + row_ref[:, :1] * gain_row(own, capacity)) * row_ref[:, 1:2]
        out_refs[k // 2][...] = term.astype(out_refs[k // 2].dtype)


def swap(array, axis, bit):
    size = lax.axis_size(axis)
    return lax.ppermute(array, axis, [(i, i ^ bit) for i in range(size)])


def scatter_sum(blocks, axis):
    bit = 1
    while len(blocks) > 1:
        kept = {}
        final = len(blocks) == 2
        for k in range(len(blocks) - 1, 0, -2):
            got = swap(blocks[k].astype(BF16), axis, bit)
            if final:
                return blocks[0].astype(F32), got
            kept[k // 2] = blocks[k - 1].astype(F32) + got.astype(F32)
        blocks = [kept[k] for k in range(len(blocks) // 2)]
        bit *= 2


def sum_all(array, axis):
    size = lax.axis_size(axis)
    if size <= 4:
        return array + sum(swap(array, axis, k) for k in range(size - 1, 0, -1))
    bit = 1
    while bit < lax.axis_size(axis):
        array = array + swap(array, axis, bit)
        bit *= 2
    return array


def gather_near(array, axis):
    return [array, swap(array, axis, 1)]


def gather_far(array, axis):
    size = lax.axis_size(axis)
    pieces = {0: array}
    bit = size // 2
    while bit:
        for k, piece in list(pieces.items()):
            if k ^ bit != 1:
                pieces[k ^ bit] = swap(piece, axis, bit)
        bit //= 2
    return [pieces[k] for k in range(2, size)]


def feature_norm(summed, gain):
    width = summed.shape[-1] * lax.axis_size("tp")
    sums = sum_all(jnp.stack([jnp.sum(summed, -1), jnp.sum(summed * summed, -1)]), "tp")
    row_mean = sums[0] / width
    row_var = sums[1] / width - row_mean * row_mean
    return (summed - row_mean[:, None]) * lax.rsqrt(row_var[:, None] + 1e-05) * gain


def call(kernel, outs, *args, in_specs=None, out_specs=None, limit=12, flops=4 * 10**9, **kw):
    shapes = [jax.ShapeDtypeStruct(shape, kind) for shape, kind in outs]
    moved = sum(array.size * array.dtype.itemsize for array in args)
    return pl.pallas_call(
        kernel,
        out_shape=shapes,
        in_specs=in_specs or [vmem()] * len(args),
        out_specs=out_specs or [vmem()] * len(outs),
        compiler_params=pltpu.CompilerParams(vmem_limit_bytes=limit * 1024 * 1024),
        cost_estimate=pl.CostEstimate(flops=flops, bytes_accessed=moved, transcendentals=0),
        **kw,
    )(*args)


def smem():
    return pl.BlockSpec(memory_space=pltpu.SMEM)


def vmem():
    return pl.BlockSpec(memory_space=pltpu.VMEM)


def shards(
    probe_vectors,
    address_vectors,
    content_vectors,
    storage_raw_signal,
    fade_raw_signal,
    channel_fade_exponent,
    extra_fade_amount,
    sequence_label,
    exit_valve_raw_signal,
    final_projection_matrix,
    incoming_rows_matrix,
    initial_rescale_factor,
    specialist_picks,
    picked_specialist_share,
    specialist_valve_matrix,
    specialist_raising_matrix,
    specialist_lowering_matrix,
    common_valve_matrix,
    common_raising_matrix,
    common_lowering_matrix,
    latter_rescale_factor,
):
    tokens, width = incoming_rows_matrix.shape
    heads = storage_raw_signal.shape[0]
    n_sp = lax.axis_size("sp")
    n_tp = lax.axis_size("tp")

    place = lax.axis_index("tp").astype(jnp.int32)[None]

    inputs = (
        probe_vectors,
        address_vectors,
        content_vectors,
        storage_raw_signal,
        fade_raw_signal,
        extra_fade_amount,
        channel_fade_exponent,
        sequence_label[None, :],
    )
    shapes = [((tokens, heads * DV), F32), ((tokens, heads * DK), F32)]

    def one_step(shape):
        return pl.BlockSpec(shape, lambda i: (0,) * len(shape))

    group = (lax.axis_index("sp").astype(jnp.int32) % heads)[None]
    *ms, local, query = call(
        delta_kernel,
        [((DK + DK + 16, DV), BF16)] * heads + shapes,
        group,
        *inputs,
        grid=(1,),
        in_specs=[smem()] + [one_step(array.shape) for array in inputs[:-2]] + [smem(), one_step(inputs[-1].shape)],
        out_specs=[one_step((DK + DK + 16, DV))] * heads + [one_step(shape) for shape, _ in shapes],
        limit=61,
        flops=2 * 10**9,
    )

    def exchange(blocks):
        moved = []
        for k in range(1, heads):
            moved.append(swap(blocks[k], "sp", k))
        return [blocks[0]] + moved

    _, *others = exchange(ms)
    own = call(
        hold_kernel,
        [((DK + DK + 16, DV), BF16)],
        ms[0],
        in_specs=[pl.BlockSpec(memory_space=pl.ANY)],
        scratch_shapes=[pltpu.SemaphoreType.DMA(())],
    )
    mine = list(own) + others
    states, maps, start, leaving, end = call(
        fold_kernel,
        [
            ((heads, DK, DV), F32),
            ((heads, DK, DK), BF16),
            ((16, DV), BF16),
            ((DK + 16, DV), BF16),
            ((DK + DK, DV), F32),
        ],
        group,
        *mine,
        in_specs=[smem()] + [vmem()] * heads,
        scratch_shapes=[pltpu.VMEM((heads, DK + DK + 16, DV), BF16)],
    )
    onward = [(i, i + heads) for i in range(n_sp - heads)]

    def hop(_, leaving):
        got = lax.ppermute(leaving, "sp", onward)
        return call(leave_kernel, [((DK + 16, DV), BF16)], got, start, leaving, end)[0]

    segments = n_sp // heads
    if segments > 2:
        leaving = lax.fori_loop(0, segments - 2, hop, leaving)
    got = lax.ppermute(leaving, "sp", onward)
    entering = exchange(
        call(
            enter_kernel,
            [((DK, DV), BF16)] * heads,
            group,
            got,
            start,
            states,
            maps,
            in_specs=[smem()] + [vmem()] * 4,
        ),
    )

    heads_out, *sends = call(
        project_kernel,
        [((tokens, heads * DV), BF16)] + [((tokens, width), BF16)] * (n_tp // 2),
        place,
        group,
        local,
        query,
        exit_valve_raw_signal,
        final_projection_matrix,
        *entering,
        in_specs=[smem()] * 2 + [vmem()] * (4 + heads),
    )
    keeps = call(
        functools.partial(project_blocks, 0),
        [((tokens, width), F32)] * (n_tp // 2),
        place,
        heads_out,
        final_projection_matrix,
        in_specs=[smem()] + [vmem()] * 2,
    )
    partial = [(sends if k % 2 else keeps)[k // 2] for k in range(n_tp)]
    keep, got = scatter_sum(partial, "tp")

    top = specialist_picks.shape[1]
    experts = specialist_valve_matrix.shape[0] * n_sp
    capacity = max(2, 9 * tokens * top // (8 * experts))
    slots = (capacity + 10) // 8 * 8
    total = experts * slots
    pick, share = call(
        functools.partial(route_kernel, capacity, slots),
        [((total, tokens), BF16), ((total, 1), F32)],
        lax.axis_index("sp").astype(jnp.int32)[None],
        specialist_picks.T,
        picked_specialist_share.T,
        in_specs=[smem()] + [vmem()] * 2,
    )
    fields = 8
    sent = call(
        functools.partial(pack_kernel, capacity, fields),
        [((slots, width), BF16)] * experts,
        keep,
        got,
        incoming_rows_matrix,
        initial_rescale_factor[None, :],
        pick,
        share,
    )

    def trade(blocks, ks):
        moved = []
        for k in ks:
            moved.append(swap(blocks[k], "sp", k) if k else blocks[k])
        return moved

    parts = [range(experts // 2, experts), range(experts // 2)]
    arrived = []
    for ks in parts:
        moved = trade(sent, ks)
        arrived.append(jnp.concatenate(moved, 0))
    hidden = specialist_valve_matrix.shape[2]
    shared = common_valve_matrix.shape[1]
    step = min(hidden, 256)
    weights = (specialist_valve_matrix, specialist_raising_matrix, common_valve_matrix, common_raising_matrix)
    work = 4 * total * width * (hidden + shared)
    height = total // len(parts)
    common = (step, slots, capacity, fields)
    back = {}
    for i, ks in enumerate(parts):
        far = gather_far(arrived[i], "tp")
        near = gather_near(arrived[i], "tp")
        partial = call(
            functools.partial(near_kernel, *common),
            [((height, hidden), F32)] * 2
            + [((height, shared), F32)] * 2
            + [((8, hidden), F32)] * 2
            + [((8, shared), F32)] * 2
            + [((height, 128), F32)] * 2,
            place,
            *near,
            *weights,
            in_specs=[smem()] + [vmem()] * 6,
            flops=work,
        )
        lowering = (specialist_lowering_matrix, common_lowering_matrix)
        *sends, inner, outer, notes = call(
            functools.partial(far_kernel, n_tp, *common),
            [((height, width), BF16)] * (n_tp // 2)
            + [((height, hidden), BF16), ((height, shared), BF16), ((height, 128), F32)],
            place,
            *far,
            *weights,
            *partial,
            *lowering,
            in_specs=[smem()] + [vmem()] * (n_tp + 14),
            flops=work * n_tp // 2,
        )
        keeps = call(
            functools.partial(tail_kernel, capacity),
            [((height, width), F32)] + [((height, width), BF16)] * (n_tp // 2 - 1),
            place,
            arrived[i],
            inner,
            outer,
            notes,
            *lowering,
            in_specs=[smem()] + [vmem()] * 6,
            flops=work // 2,
        )
        results = [(sends if k % 2 else keeps)[k // 2] for k in range(n_tp)]
        keep, got = scatter_sum(results, "tp")
        blocks = (keep + got.astype(F32)).astype(BF16).reshape(len(ks), slots, width)
        back.update(zip(ks, trade({k: blocks[j] for j, k in enumerate(ks)}, ks)))
    returned = jnp.concatenate([back[k] for k in range(experts)], 0)
    second_sum = lax.dot_general(
        pick, returned, (((0,), (0,)), ((), ())), preferred_element_type=F32
    )
    return feature_norm(second_sum, latter_rescale_factor).astype(BF16)


def solution(mesh):
    placed = (
        P("sp", "tp"),
        P("sp", "tp"),
        P("sp", "tp"),
        P("tp", "sp"),
        P("tp", "sp"),
        P("tp"),
        P("tp", "sp"),
        P("sp"),
        P("sp", "tp"),
        P("tp", None),
        P("sp", "tp"),
        P("tp"),
        P("sp", None),
        P("sp", None),
        P("sp", None, "tp"),
        P("sp", None, "tp"),
        P("sp", "tp", None),
        P(None, "tp"),
        P(None, "tp"),
        P("tp", None),
        P("tp"),
    )

    return jax.shard_map(shards, mesh=mesh, in_specs=placed, out_specs=P("sp", "tp"), check_vma=False)
```

```python
import functools

import jax
import jax.numpy as jnp
from jax import lax
from jax.experimental import pallas as pl
from jax.experimental.pallas import tpu as pltpu
from jax.sharding import PartitionSpec as P


DK = 128
DV = 128
ALPHA = 2.0**0.25
F32 = jnp.float32
BF16 = jnp.bfloat16


def dot(left, right, contract=((1,), (0,))):
    return lax.dot_general(left, right, (contract, ((), ())), preferred_element_type=F32)


def split(array):
    high = array.astype(BF16)
    return high, (array - high.astype(F32)).astype(BF16)


def dot3(left, right):
    left_high, left_low = split(left)
    right_high, right_low = split(right)
    return dot(left_high, right_high) + (dot(left_high, right_low) + dot(left_low, right_high))


def dot_left(left, right):
    high, low = split(left)
    return dot(high, right) + dot(low, right)


def triangular_inverses(lowers, rows, cols):
    size = lowers[0].shape[0]
    identity = jnp.where(rows == cols, 1.0, 0.0)

    def once(left, right):
        return dot(left.astype(BF16), right.astype(BF16))

    def solve(powers, inverses, ratio, block):
        if block == 1:
            inverses = [x - p for p, x in zip(powers, inverses)]
            if ratio > 2:
                powers = [once(p, p) for p in powers]
        elif ratio > 2:
            both = [once(p, jnp.concatenate([p, x], 1)) for p, x in zip(powers, inverses)]
            powers = [pair[:, :size] for pair in both]
            inverses = [x - pair[:, size:] for pair, x in zip(both, inverses)]
        else:
            return [x - once(p, x) for p, x in zip(powers, inverses)]
        if ratio > 2:
            inverses = [x + once(p, x) for p, x in zip(powers, inverses)]
        return inverses

    inverses = [identity for _ in lowers]
    block = 1
    while block < size:
        ratio = min(4, size // block)
        wide = block * ratio
        inside = (rows // wide == cols // wide) & (rows // block != cols // block)
        parts = [jnp.where(inside, lower, 0.0) for lower in lowers]
        if block > 1:
            parts = [once(x, part) for x, part in zip(inverses, parts)]
        inverses = solve(parts, inverses, ratio, block)
        block = wide
    errors = [(identity - x) - dot3(lower, x) for lower, x in zip(lowers, inverses)]
    return [x + once(x, error) for x, error in zip(inverses, errors)]


def delta_kernel(*refs):
    place_ref, q_ref, k_ref, v_ref, store_ref, fade_ref, extra_ref, rate_ref, label_ref = refs[:9]
    ms_refs = refs[9:-2]
    local_ref, query_ref = refs[-2:]
    length = q_ref.shape[0]
    heads = store_ref.shape[0]
    every = range(heads)
    rows = lax.broadcasted_iota(jnp.int32, (length, length), 0)
    cols = lax.broadcasted_iota(jnp.int32, (length, length), 1)
    diagonal = rows == cols
    lower = rows >= cols
    strict = rows > cols
    identity = jnp.where(diagonal, 1.0, 0.0)

    def to_col(row):
        return jnp.sum(jnp.where(diagonal, row, 0.0), 1, keepdims=True)

    def to_row(col):
        return jnp.sum(jnp.where(diagonal, col, 0.0), 0, keepdims=True)

    label_row = label_ref[...].astype(F32)
    label_col = to_col(label_row)
    first = label_col[:1]
    last = label_col[length - 1 :]
    same = lower & (label_col == label_row)
    carried = jnp.where(label_col == first, 1.0, 0.0)
    closing = jnp.where(label_col == last, 1.0, 0.0)
    through = jnp.where(first == last, 1.0, 0.0)
    names = [place_ref[0] ^ k for k in every]
    at = [pl.ds(pl.multiple_of(name * DK, DK), DK) for name in names]
    queries = [q_ref[:, at[h]] for h in every]
    keys = [k_ref[:, at[h]] for h in every]
    values = [v_ref[:, at[h]] for h in every]
    row = [pl.ds(name, 1) for name in names]
    fades = [fade_ref[row[h], :] for h in every]
    softs = [jnp.maximum(fade, 0.0) + jnp.log(1.0 + jnp.exp(-jnp.abs(fade))) for fade in fades]
    rates = [jnp.exp(jnp.full((1, length), rate_ref[names[h]], F32)) for h in every]

    def scale_of(array):
        wide = array.astype(F32)
        return lax.rsqrt(jnp.sum(wide * wide, 1, keepdims=True) + 1e-06)

    key_scales = [scale_of(key) for key in keys]
    query_scales = [scale_of(query) * DK ** (-0.5) for query in queries]
    products = [dot(key, key, ((1,), (1,))) for key in keys]
    scores = [dot(query, key, ((1,), (1,))) for query, key in zip(queries, keys)]
    gate_rows = [1.0 / (1.0 + jnp.exp(-store_ref[row[h], :])) for h in every]
    gate_cols = [to_col(gate_rows[h]) for h in every]
    decays = [extra_ref[row[h], :] - rates[h] * softs[h] for h in every]
    totals = [jnp.sum(jnp.where(lower, decay, 0.0), 1, keepdims=True) for decay in decays]
    ends = [total[length - 1 :] for total in totals]
    reaches = [
        jnp.where(same, jnp.exp(jnp.where(lower, total - to_row(total), 0.0)), 0.0) for total in totals
    ]
    growths = [jnp.exp(total) * carried for total in totals]
    reaches = [reaches[h] * to_row(key_scales[h]) for h in every]
    couplings = [
        jnp.where(strict, products[h] * (key_scales[h] * gate_cols[h]) * reaches[h], 0.0) for h in every
    ]
    scores = [(scores[h] * query_scales[h] * reaches[h]).astype(BF16) for h in every]
    inverses = triangular_inverses(couplings, rows, cols)
    fresh = [dot_left(inverses[h] * gate_rows[h], values[h]) for h in every]
    erase = [
        dot_left(inverses[h] * to_row(gate_cols[h] * key_scales[h] * growths[h]), keys[h]) for h in every
    ]
    both = [jnp.concatenate([fresh[h], erase[h]], 1) for h in every]
    tails = [key_scales[h] * jnp.exp(ends[h] - totals[h]) * closing for h in every]
    carries = [dot(keys[h], (both[h] * tails[h]).astype(BF16), ((0,), (0,))) for h in every]
    seen = [dot(scores[h], both[h].astype(BF16)) for h in every]
    for h in every:
        final = jnp.exp(ends[h]) * through
        ms_refs[h][:DK] = (final * identity[:DK, :DK] - carries[h][:, DV:]).astype(BF16)
        ms_refs[h][DK : DK + DK] = carries[h][:, :DV].astype(BF16)
        ms_refs[h][DK + DK : DK + DK + 8] = jnp.broadcast_to(first, (8, DV)).astype(BF16)
        ms_refs[h][DK + DK + 8 :] = jnp.broadcast_to(last, (8, DV)).astype(BF16)
        local_ref[:, at[h]] = seen[h][:, :DV]
        query_ref[:, at[h]] = queries[h].astype(F32) * (query_scales[h] * growths[h]) - seen[h][:, DV:]


def first_label(ms_ref, j):
    return ms_ref[j, DK + DK : DK + DK + 8].astype(F32)[:1]


def last_label(ms_ref, j):
    return ms_ref[j, DK + DK + 8 :].astype(F32)[:1]


def hold_kernel(array_ref, out_ref, done_ref):
    copy = pltpu.make_async_copy(array_ref, out_ref, done_ref)
    copy.start()
    copy.wait()


def fold_kernel(place_ref, *refs):
    ms_refs = refs[:-6]
    state_ref, map_ref, start_ref, leaving_ref, end_ref, ms_ref = refs[-6:]
    blocks = len(ms_refs)
    for k in range(blocks):
        ms_ref[place_ref[0] ^ k] = ms_refs[k][...]
    state = jnp.zeros((DK, DV), F32)
    reach = jnp.where(
        lax.broadcasted_iota(jnp.int32, (DK, DK), 0) == lax.broadcasted_iota(jnp.int32, (DK, DK), 1), 1.0, 0.0
    )
    for j in range(blocks):
        if j:
            joined = jnp.where(first_label(ms_ref, j) == last_label(ms_ref, j - 1), 1.0, 0.0)
            state = state * joined
            reach = reach * joined
        onto = ms_ref[j, :DK]
        reach = reach.astype(BF16)
        state_ref[j] = state
        map_ref[j] = reach
        add = ms_ref[j, DK : DK + DK].astype(F32)
        if j:
            high, low = split(state)
            moved = dot(onto, jnp.concatenate([high, low, reach], 1))
            state = moved[:, :DV] + moved[:, DV : DV + DV] + add
            reach = moved[:, DV + DV :]
        else:
            state = add
            reach = onto.astype(F32)
    start_ref[...] = ms_ref[0, DK + DK :]
    leaving_ref[:DK] = state.astype(BF16)
    leaving_ref[DK:] = ms_ref[blocks - 1, DK + DK :]
    end_ref[:DK] = state
    end_ref[DK:] = reach


def arriving(got_ref, start_ref):
    last = got_ref[DK + 8 :].astype(F32)[:1]
    joined = jnp.where(start_ref[:8].astype(F32)[:1] == last, 1.0, 0.0)
    return (got_ref[:DK].astype(F32) * joined).astype(BF16)


def enter_kernel(place_ref, got_ref, start_ref, state_ref, map_ref, *entering_refs):
    state = arriving(got_ref, start_ref)
    for k, entering_ref in enumerate(entering_refs):
        j = place_ref[0] ^ k
        entering_ref[...] = (state_ref[j] + dot(map_ref[j], state)).astype(BF16)


def leave_kernel(got_ref, start_ref, leaving_ref, end_ref, out_ref):
    state = arriving(got_ref, start_ref)
    out_ref[:DK] = (end_ref[:DK] + dot(end_ref[DK:].astype(BF16), state)).astype(BF16)
    out_ref[DK:] = leaving_ref[DK:]


def project_kernel(place_ref, group_ref, local_ref, query_ref, valve_ref, weight_ref, *refs):
    heads = local_ref.shape[1] // DV
    state_refs, heads_ref, out_refs = refs[:heads], refs[heads], refs[heads + 1 :]
    for k in range(heads):
        at = pl.ds(pl.multiple_of((group_ref[0] ^ k) * DV, DV), DV)
        mixed = local_ref[:, at] + dot_left(query_ref[:, at], state_refs[k][...])
        scaled = mixed * lax.rsqrt(jnp.mean(mixed * mixed, 1, keepdims=True) + 1e-06)
        heads_ref[:, at] = (scaled * silu(valve_ref[:, at].astype(F32))).astype(BF16)
    project_blocks(1, place_ref, heads_ref, weight_ref, *out_refs)


def project_blocks(odd, place_ref, heads_ref, weight_ref, *out_refs):
    width = out_refs[0].shape[1]
    for i in range(len(out_refs) - 1, -1, -1):
        start = pl.multiple_of((place_ref[0] ^ (2 * i + odd)) * width, width)
        out_refs[i][...] = dot(heads_ref[...], weight_ref[:, pl.ds(start, width)]).astype(out_refs[i].dtype)


def spread(fields, width):
    rows = lax.broadcasted_iota(jnp.int32, (128, width), 0)
    lanes = lax.broadcasted_iota(jnp.int32, (128, width), 1)
    return jnp.where(lanes // (width // fields) == rows, 1.0, 0.0).astype(BF16)


def own_lane(fields, slots, width):
    rows = lax.broadcasted_iota(jnp.int32, (slots, width), 0)
    lanes = lax.broadcasted_iota(jnp.int32, (slots, width), 1)
    return rows == lanes % (width // fields)


def route_kernel(capacity, slots, place_ref, named_ref, share_ref, pick_ref, note_ref):
    top, tokens = named_ref.shape
    experts = pick_ref.shape[0] // slots
    named, share = named_ref[...], share_ref[...].astype(F32)
    taken, signed = [], []
    for k in range(experts):
        hit = jnp.where(named == (place_ref[0] ^ k), 1.0, 0.0)
        taken.append(sum(hit[j : j + 1] for j in range(top)))
        signed.append(sum(hit[j : j + 1] * share[j : j + 1] * (1.0 if j else -1.0) for j in range(top)))
    before = lax.broadcasted_iota(jnp.int32, (tokens, tokens), 0)
    after = lax.broadcasted_iota(jnp.int32, (tokens, tokens), 1)
    earlier = jnp.where(before < after, 1.0, 0.0).astype(BF16)
    rank = dot(jnp.concatenate(taken, 0).astype(BF16), earlier)
    slot = lax.broadcasted_iota(jnp.int32, (slots, tokens), 0).astype(F32)
    for k in range(experts):
        chosen = jnp.where(rank[k : k + 1] == slot, taken[k], 0.0)
        chosen = jnp.where(slot < capacity, chosen, 0.0)
        here = slice(k * slots, (k + 1) * slots)
        pick_ref[here] = chosen.astype(BF16)
        note_ref[here] = jnp.sum(chosen * signed[k], 1, keepdims=True)


def pack_kernel(capacity, fields, keep_ref, got_ref, row_ref, gain_ref, pick_ref, share_ref, *out_refs):
    experts = len(out_refs)
    slots, width = out_refs[0].shape
    summed = ALPHA * row_ref[...].astype(F32) + (keep_ref[...] + got_ref[...].astype(F32))
    tokens = summed.shape[0]
    mean = jnp.mean(summed, 1, keepdims=True)
    centred = summed - mean
    squares = jnp.sum(centred * centred, 1, keepdims=True)
    gain = gain_ref[...]
    lane = lax.broadcasted_iota(jnp.int32, (tokens, 128), 1)
    notes = jnp.zeros((tokens, 128), F32)
    for value, places in ((mean, (1, 2, 3)), (squares, (4, 5))):
        for place in places:
            piece = value.astype(BF16).astype(F32)
            notes = jnp.where(lane == place, piece, notes)
            value = value - piece
    pick = pick_ref[...]
    body = dot(pick, (centred * gain).astype(BF16))
    notes = dot(pick, notes.astype(BF16))
    lane = lax.broadcasted_iota(jnp.int32, (experts * slots, 128), 1)
    notes = jnp.where(lane == 0, share_ref[...], notes).astype(BF16)
    notes = dot(notes, spread(fields, width))
    mine = own_lane(fields, slots, width)
    gain_high, gain_low = split(gain)
    rows = lax.broadcasted_iota(jnp.int32, (slots, width), 0)
    for e in range(experts):
        here = slice(e * slots, (e + 1) * slots)
        info = jnp.sum(jnp.where(mine, notes[here], 0.0), 0, keepdims=True)
        block = jnp.where(rows == capacity, info, body[here])
        block = jnp.where(rows == capacity + 1, gain_high.astype(F32), block)
        block = jnp.where(rows == capacity + 2, gain_low.astype(F32), block)
        out_refs[e][...] = block.astype(BF16)


def silu(array):
    return array / (1.0 + jnp.exp(-array))


def read_notes(piece_ref, capacity, slots, fields):
    width = piece_ref.shape[1]
    mine = own_lane(fields, slots, width)
    base = capacity // 8 * 8
    blocks = []
    for source in range(piece_ref.shape[0] // slots):
        info = piece_ref[source * slots + base : source * slots + base + 8, :].astype(F32)
        blocks.append(jnp.where(mine, info[capacity - base : capacity - base + 1], 0.0))
    return dot(jnp.concatenate(blocks, 0).astype(BF16), spread(fields, width), ((1,), (1,)))


def gain_row(array, capacity):
    return array[capacity + 1 : capacity + 2] + array[capacity + 2 : capacity + 3]


def near_kernel(step, slots, capacity, fields, *refs):
    place_ref, piece_refs = refs[0], refs[1:3]
    weight_refs, sum_refs, gain_refs, note_refs = refs[3:7], refs[7:11], refs[11:15], refs[15:17]
    width = piece_refs[0].shape[1]
    at = [pl.ds(pl.multiple_of((place_ref[0] ^ k) * width, width), width) for k in range(2)]

    def product(weight_ref, sum_ref, gain_ref, cut):
        total = None
        for k in range(2):
            weight = weight_ref[at[k], cut] if len(weight_ref.shape) == 2 else weight_ref[0, at[k], cut]
            term = dot(piece_refs[k][...], weight)
            gain_ref[k : k + 1, cut] = gain_row(term, capacity)
            total = term if total is None else total + term
        sum_ref[:, cut] = total

    for i in (2, 3):
        product(weight_refs[i], sum_refs[i], gain_refs[i], slice(None))

    def chunk(i, _):
        cut = pl.ds(pl.multiple_of(i * step, step), step)
        for j in (0, 1):
            product(weight_refs[j], sum_refs[j], gain_refs[j], cut)
        return 0

    lax.fori_loop(0, weight_refs[0].shape[2] // step, chunk, 0, unroll=True)
    for k in range(2):
        note_refs[k][...] = read_notes(piece_refs[k], capacity, slots, fields)


def far_kernel(count, step, slots, capacity, fields, *refs):
    place_ref, piece_refs = refs[0], refs[1 : count - 1]
    refs = refs[count - 1 :]
    weight_refs, sum_refs, gain_refs, note_refs = refs[:4], refs[4:8], refs[8:12], refs[12:14]
    lower_ref, cl_ref = refs[14:16]
    out_refs = refs[16 : 16 + count // 2]
    hidden_ref, shared_ref, row_ref = refs[16 + count // 2 :]
    height, width = piece_refs[0].shape
    at = [pl.ds(pl.multiple_of((place_ref[0] ^ k) * width, width), width) for k in range(2, count)]
    notes = [note_ref[...] for note_ref in note_refs]
    notes = notes + [read_notes(piece_ref, capacity, slots, fields) for piece_ref in piece_refs]
    means = [note[:, 1:2] + note[:, 2:3] + note[:, 3:4] for note in notes]
    mean = sum(means) / count
    offsets = [own_mean - mean for own_mean in means]
    squares = sum(note[:, 4:5] + note[:, 5:6] + width * offset * offset for note, offset in zip(notes, offsets))
    scale = lax.rsqrt(squares / (count * width) + 1e-05)
    share = notes[0][:, :1]
    flag = jnp.where(share < 0.0, 1.0, 0.0)
    share = jnp.abs(share)

    def product(weight_ref, sum_ref, gain_ref, cut):
        total = sum_ref[:, cut]
        for k in range(2):
            total = total + offsets[k] * gain_ref[k : k + 1, cut]
        for k in range(2, count):
            weight = weight_ref[at[k - 2], cut] if len(weight_ref.shape) == 2 else weight_ref[0, at[k - 2], cut]
            term = dot(piece_refs[k - 2][...], weight)
            total = total + term + offsets[k] * gain_row(term, capacity)
        return total * scale

    every = slice(None)
    gate = product(weight_refs[2], sum_refs[2], gain_refs[2], every)
    lift = product(weight_refs[3], sum_refs[3], gain_refs[3], every)
    shared_ref[...] = (silu(gate) * lift * flag).astype(BF16)

    def chunk(i, _):
        cut = pl.ds(pl.multiple_of(i * step, step), step)
        gate = product(weight_refs[0], sum_refs[0], gain_refs[0], cut)
        lift = product(weight_refs[1], sum_refs[1], gain_refs[1], cut)
        hidden_ref[:, cut] = (silu(gate) * lift * share).astype(BF16)
        return 0

    lax.fori_loop(0, weight_refs[0].shape[2] // step, chunk, 0, unroll=True)
    lane = lax.broadcasted_iota(jnp.int32, (height, 128), 1)
    row_ref[...] = jnp.where(lane == 0, offsets[0], flag * scale * ALPHA)
    for k in range(count - 1, 0, -2):
        out_refs[k // 2][...] = lowered(place_ref, k, width, hidden_ref, shared_ref, lower_ref, cl_ref).astype(BF16)


def lowered(place_ref, k, width, hidden_ref, shared_ref, lower_ref, cl_ref):
    cut = pl.ds(pl.multiple_of((place_ref[0] ^ k) * width, width), width)
    return dot(hidden_ref[...], lower_ref[0, :, cut]) + dot(shared_ref[...], cl_ref[:, cut])


def tail_kernel(capacity, place_ref, own_ref, hidden_ref, shared_ref, row_ref, lower_ref, cl_ref, *out_refs):
    width = own_ref.shape[1]
    for k in range(2 * len(out_refs) - 2, -1, -2):
        term = lowered(place_ref, k, width, hidden_ref, shared_ref, lower_ref, cl_ref)
        if k == 0:
            own = own_ref[...].astype(F32)
            term = term + (own + row_ref[:, :1] * gain_row(own, capacity)) * row_ref[:, 1:2]
        out_refs[k // 2][...] = term.astype(out_refs[k // 2].dtype)


def swap(array, axis, bit):
    size = lax.axis_size(axis)
    return lax.ppermute(array, axis, [(i, i ^ bit) for i in range(size)])


def scatter_sum(blocks, axis):
    bit = 1
    while len(blocks) > 1:
        kept = {}
        final = len(blocks) == 2
        for k in range(len(blocks) - 1, 0, -2):
            got = swap(blocks[k].astype(BF16), axis, bit)
            if final:
                return blocks[0].astype(F32), got
            kept[k // 2] = blocks[k - 1].astype(F32) + got.astype(F32)
        blocks = [kept[k] for k in range(len(blocks) // 2)]
        bit *= 2


def sum_all(array, axis):
    size = lax.axis_size(axis)
    if size <= 4:
        return array + sum(swap(array, axis, k) for k in range(size - 1, 0, -1))
    bit = 1
    while bit < lax.axis_size(axis):
        array = array + swap(array, axis, bit)
        bit *= 2
    return array


def gather_near(array, axis):
    return [array, swap(array, axis, 1)]


def gather_far(array, axis):
    size = lax.axis_size(axis)
    pieces = {0: array}
    bit = size // 2
    while bit:
        for k, piece in list(pieces.items()):
            if k ^ bit != 1:
                pieces[k ^ bit] = swap(piece, axis, bit)
        bit //= 2
    return [pieces[k] for k in range(2, size)]


def feature_norm(summed, gain):
    width = summed.shape[-1] * lax.axis_size("tp")
    sums = sum_all(jnp.stack([jnp.sum(summed, -1), jnp.sum(summed * summed, -1)]), "tp")
    row_mean = sums[0] / width
    row_var = sums[1] / width - row_mean * row_mean
    return (summed - row_mean[:, None]) * lax.rsqrt(row_var[:, None] + 1e-05) * gain


def call(kernel, outs, *args, in_specs=None, out_specs=None, limit=12, flops=4 * 10**9, **kw):
    shapes = [jax.ShapeDtypeStruct(shape, kind) for shape, kind in outs]
    moved = sum(array.size * array.dtype.itemsize for array in args)
    return pl.pallas_call(
        kernel,
        out_shape=shapes,
        in_specs=in_specs or [vmem()] * len(args),
        out_specs=out_specs or [vmem()] * len(outs),
        compiler_params=pltpu.CompilerParams(vmem_limit_bytes=limit * 1024 * 1024),
        cost_estimate=pl.CostEstimate(flops=flops, bytes_accessed=moved, transcendentals=0),
        **kw,
    )(*args)


def smem():
    return pl.BlockSpec(memory_space=pltpu.SMEM)


def vmem():
    return pl.BlockSpec(memory_space=pltpu.VMEM)


def shards(
    probe_vectors,
    address_vectors,
    content_vectors,
    storage_raw_signal,
    fade_raw_signal,
    channel_fade_exponent,
    extra_fade_amount,
    sequence_label,
    exit_valve_raw_signal,
    final_projection_matrix,
    incoming_rows_matrix,
    initial_rescale_factor,
    specialist_picks,
    picked_specialist_share,
    specialist_valve_matrix,
    specialist_raising_matrix,
    specialist_lowering_matrix,
    common_valve_matrix,
    common_raising_matrix,
    common_lowering_matrix,
    latter_rescale_factor,
):
    tokens, width = incoming_rows_matrix.shape
    heads = storage_raw_signal.shape[0]
    n_sp = lax.axis_size("sp")
    n_tp = lax.axis_size("tp")

    place = lax.axis_index("tp").astype(jnp.int32)[None]

    inputs = (
        probe_vectors,
        address_vectors,
        content_vectors,
        storage_raw_signal,
        fade_raw_signal,
        extra_fade_amount,
        channel_fade_exponent,
        sequence_label[None, :],
    )
    shapes = [((tokens, heads * DV), F32), ((tokens, heads * DK), F32)]

    def one_step(shape):
        return pl.BlockSpec(shape, lambda i: (0,) * len(shape))

    group = (lax.axis_index("sp").astype(jnp.int32) % heads)[None]
    *ms, local, query = call(
        delta_kernel,
        [((DK + DK + 16, DV), BF16)] * heads + shapes,
        group,
        *inputs,
        grid=(1,),
        in_specs=[smem()] + [one_step(array.shape) for array in inputs[:-2]] + [smem(), one_step(inputs[-1].shape)],
        out_specs=[one_step((DK + DK + 16, DV))] * heads + [one_step(shape) for shape, _ in shapes],
        limit=61,
        flops=2 * 10**9,
    )

    def exchange(blocks):
        moved = []
        for k in range(1, heads):
            moved.append(swap(blocks[k], "sp", k))
        return [blocks[0]] + moved

    _, *others = exchange(ms)
    own = call(
        hold_kernel,
        [((DK + DK + 16, DV), BF16)],
        ms[0],
        in_specs=[pl.BlockSpec(memory_space=pl.ANY)],
        scratch_shapes=[pltpu.SemaphoreType.DMA(())],
    )
    mine = list(own) + others
    states, maps, start, leaving, end = call(
        fold_kernel,
        [
            ((heads, DK, DV), F32),
            ((heads, DK, DK), BF16),
            ((16, DV), BF16),
            ((DK + 16, DV), BF16),
            ((DK + DK, DV), F32),
        ],
        group,
        *mine,
        in_specs=[smem()] + [vmem()] * heads,
        scratch_shapes=[pltpu.VMEM((heads, DK + DK + 16, DV), BF16)],
    )
    onward = [(i, i + heads) for i in range(n_sp - heads)]

    def hop(_, leaving):
        got = lax.ppermute(leaving, "sp", onward)
        return call(leave_kernel, [((DK + 16, DV), BF16)], got, start, leaving, end)[0]

    segments = n_sp // heads
    if segments > 2:
        leaving = lax.fori_loop(0, segments - 2, hop, leaving)
    got = lax.ppermute(leaving, "sp", onward)
    entering = exchange(
        call(
            enter_kernel,
            [((DK, DV), BF16)] * heads,
            group,
            got,
            start,
            states,
            maps,
            in_specs=[smem()] + [vmem()] * 4,
        ),
    )

    heads_out, *sends = call(
        project_kernel,
        [((tokens, heads * DV), BF16)] + [((tokens, width), BF16)] * (n_tp // 2),
        place,
        group,
        local,
        query,
        exit_valve_raw_signal,
        final_projection_matrix,
        *entering,
        in_specs=[smem()] * 2 + [vmem()] * (4 + heads),
    )
    keeps = call(
        functools.partial(project_blocks, 0),
        [((tokens, width), F32)] * (n_tp // 2),
        place,
        heads_out,
        final_projection_matrix,
        in_specs=[smem()] + [vmem()] * 2,
    )
    partial = [(sends if k % 2 else keeps)[k // 2] for k in range(n_tp)]
    keep, got = scatter_sum(partial, "tp")

    top = specialist_picks.shape[1]
    experts = specialist_valve_matrix.shape[0] * n_sp
    capacity = max(2, 9 * tokens * top // (8 * experts))
    slots = (capacity + 10) // 8 * 8
    total = experts * slots
    pick, share = call(
        functools.partial(route_kernel, capacity, slots),
        [((total, tokens), BF16), ((total, 1), F32)],
        lax.axis_index("sp").astype(jnp.int32)[None],
        specialist_picks.T,
        picked_specialist_share.T,
        in_specs=[smem()] + [vmem()] * 2,
    )
    fields = 8
    sent = call(
        functools.partial(pack_kernel, capacity, fields),
        [((slots, width), BF16)] * experts,
        keep,
        got,
        incoming_rows_matrix,
        initial_rescale_factor[None, :],
        pick,
        share,
    )

    def trade(blocks, ks):
        moved = []
        for k in ks:
            moved.append(swap(blocks[k], "sp", k) if k else blocks[k])
        return moved

    parts = [range(experts // 2, experts), range(experts // 2)]
    arrived = []
    for ks in parts:
        moved = trade(sent, ks)
        arrived.append(jnp.concatenate(moved, 0))
    hidden = specialist_valve_matrix.shape[2]
    shared = common_valve_matrix.shape[1]
    step = min(hidden, 512)
    weights = (specialist_valve_matrix, specialist_raising_matrix, common_valve_matrix, common_raising_matrix)
    work = 4 * total * width * (hidden + shared)
    height = total // len(parts)
    common = (step, slots, capacity, fields)
    back = {}
    for i, ks in enumerate(parts):
        far = gather_far(arrived[i], "tp")
        near = gather_near(arrived[i], "tp")
        partial = call(
            functools.partial(near_kernel, *common),
            [((height, hidden), F32)] * 2
            + [((height, shared), F32)] * 2
            + [((8, hidden), F32)] * 2
            + [((8, shared), F32)] * 2
            + [((height, 128), F32)] * 2,
            place,
            *near,
            *weights,
            in_specs=[smem()] + [vmem()] * 6,
            flops=work,
        )
        lowering = (specialist_lowering_matrix, common_lowering_matrix)
        *sends, inner, outer, notes = call(
            functools.partial(far_kernel, n_tp, *common),
            [((height, width), BF16)] * (n_tp // 2)
            + [((height, hidden), BF16), ((height, shared), BF16), ((height, 128), F32)],
            place,
            *far,
            *weights,
            *partial,
            *lowering,
            in_specs=[smem()] + [vmem()] * (n_tp + 14),
            flops=work * n_tp // 2,
        )
        keeps = call(
            functools.partial(tail_kernel, capacity),
            [((height, width), F32)] + [((height, width), BF16)] * (n_tp // 2 - 1),
            place,
            arrived[i],
            inner,
            outer,
            notes,
            *lowering,
            in_specs=[smem()] + [vmem()] * 6,
            flops=work // 2,
        )
        results = [(sends if k % 2 else keeps)[k // 2] for k in range(n_tp)]
        keep, got = scatter_sum(results, "tp")
        blocks = (keep + got.astype(F32)).astype(BF16).reshape(len(ks), slots, width)
        back.update(zip(ks, trade({k: blocks[j] for j, k in enumerate(ks)}, ks)))
    returned = jnp.concatenate([back[k] for k in range(experts)], 0)
    second_sum = lax.dot_general(
        pick, returned, (((0,), (0,)), ((), ())), preferred_element_type=F32
    )
    return feature_norm(second_sum, latter_rescale_factor).astype(BF16)


def solution(mesh):
    placed = (
        P("sp", "tp"),
        P("sp", "tp"),
        P("sp", "tp"),
        P("tp", "sp"),
        P("tp", "sp"),
        P("tp"),
        P("tp", "sp"),
        P("sp"),
        P("sp", "tp"),
        P("tp", None),
        P("sp", "tp"),
        P("tp"),
        P("sp", None),
        P("sp", None),
        P("sp", None, "tp"),
        P("sp", None, "tp"),
        P("sp", "tp", None),
        P(None, "tp"),
        P(None, "tp"),
        P("tp", None),
        P("tp"),
    )

    return jax.shard_map(shards, mesh=mesh, in_specs=placed, out_specs=P("sp", "tp"), check_vma=False)
```
